256 devices in a mesh: sp: 64 (over z, x, core), tp: 4 (over y).
Axes of the slice: x: 4, y: 4, z: 8, core: 2. Of those that a mesh axis runs over, the one named last changes fastest.
Arguments:
- queries: bfloat16 [8192, 32, 128], P('sp', 'tp'), may hold values from -6 to 6
- keys: bfloat16 [8192, 8, 128], P('sp', 'tp'), may hold values from -6 to 6
- values: bfloat16 [8192, 8, 128], P('sp', 'tp'), may hold values from -6 to 6
- q_gain: float32 [128], replicated, may hold values from 0.2 to 8
- k_gain: float32 [128], replicated, may hold values from 0.2 to 8
- w_out: bfloat16 [4096, 2048], P('tp'), may hold values from -0.09375 to 0.09375
- residual: bfloat16 [8192, 2048], P(('sp', 'tp')), may hold values from -6 to 6
- gain_mix: float32 [2048], replicated, may hold values from 0.1 to 1.9
- gain_pre: float32 [2048], replicated, may hold values from 0.1 to 1.9
- routes: int32 [8192, 4], P(('sp', 'tp')), may hold values from 0 to 63, all different within a row; in each aligned block of 32 rows (0 to 31, 32 to 63, ...) at most 4 rows name the same one
- route_weights: float32 [8192, 4], P(('sp', 'tp')), may hold values from 0.1 to 1
- w_gate: bfloat16 [64, 2048, 2048], P('sp', None, 'tp'), may hold values from -0.5 to 0.5
- w_up: bfloat16 [64, 2048, 2048], P('sp', None, 'tp'), may hold values from -0.5 to 0.5
- w_down: bfloat16 [64, 2048, 2048], P('sp', 'tp'), may hold values from -0.125 to 0.125
- gain_moe: float32 [2048], replicated, may hold values from 0.1 to 1.9
Outputs:
- layer_out: bfloat16 [8192, 2048], P(('sp', 'tp'))
The draws below stay inside these ranges and needn't reach their ends.
Inputs may be any that keep to these rules, and one draw needn't show every extreme that they name: `routes`: each row names 4 different experts. In each aligned block of 32 rows (the rows of one device) no expert is named by more than 4 rows, a bound that some block reaches.
All inputs are finite; a program needn't handle non-finite values.
Results may differ from the reference program's by a relative error of at most 0.017.
The reference program's roundings to bfloat16 on the way count: a program that leaves them out, or rounds other values in their place, can miss the bound.
Values may be sent and summed in bfloat16 or wider, within the bound.
A program may use at most 128 MiB of HBM per device.

```python
import math
import jax
import jax.numpy as jnp
import numpy as np
from jax import lax

D = 2048
Q_HEADS = 32
KV_HEADS = 8
HD = 128
FF = 2048
TOP = 4
GRID_W = 64
TOKENS = 8192
TOK_TP = 32
EXPERTS = 64
CAP = 4
N_TP = 4


def gain_draw(key):
    return 1.0 + 0.18 * jax.random.truncated_normal(key, -4.0, 4.0, (HD,), jnp.float32)


def draw_q_gain(key, part):
    return gain_draw(jax.random.fold_in(key, 31))


def draw_k_gain(key, part):
    return gain_draw(jax.random.fold_in(key, 57))


def steps_of(own_key, shape, shards, least, high):
    def one(position, blocks):
        draws = jax.random.uniform(jax.random.fold_in(jax.random.fold_in(own_key, 6), position), (blocks,), jnp.float32, least / len(shards), high / len(shards))
        return jnp.repeat(jnp.exp(draws), shape[position] // blocks).reshape((-1,) + (1,) * (len(shape) - position - 1))

    loudness = one(*shards[0])
    for cut in shards[1:]:
        loudness = loudness * one(*cut)
    return loudness


def routed_block(stream_key, own, number, rows, number_of, top, bound, lean):
    order = jax.random.permutation(stream_key, number_of)
    packed, common = shares(number_of, rows * top, bound, lean, True), shares(number_of, rows * top, bound, lean, False)
    places = jnp.arange(number_of)

    def named(lengths, rotation):
        used = int((lengths > 0).sum())
        fixed = max(1, used // 4)
        shifted = fixed + (places - fixed + rotation * (used - fixed)) % max(1, number_of - fixed)
        return jnp.zeros((number_of,), jnp.int32).at[order[jnp.where(places < fixed, places, shifted)]].set(jnp.asarray(lengths, jnp.int32))

    lengths = jnp.where(number % 4 == 0, named(packed, number // 4), named(common, number - number // 4 - 1))
    mixed = jax.random.permutation(jax.random.fold_in(own, 3), number_of)
    donor, taker = mixed[0:number_of // 2 * 2:2], mixed[1:number_of // 2 * 2:2]
    room = jnp.minimum(lengths[donor] - 1, bound - lengths[taker]) // 2
    room = jnp.where((donor == order[0]) | (taker == order[0]) | (lengths[taker] == 0), 0, jnp.maximum(room, 0))
    shifted = jax.random.randint(jax.random.fold_in(own, 4), (number_of // 2,), 0, 1 << 20) % (room + 1)
    lengths = lengths.at[donor].add(-shifted).at[taker].add(shifted)
    members = jnp.searchsorted(jnp.cumsum(lengths), jnp.arange(rows * top), side="right").astype(jnp.int32)
    listing = members.reshape(top, rows).T
    listing = listing[jax.random.permutation(jax.random.fold_in(own, 1), rows)]
    rotation = jax.random.randint(jax.random.fold_in(own, 2), (rows, 1), 0, top)
    return jnp.take_along_axis(listing, (jnp.arange(top)[None, :] + rotation) % top, axis=1)


def shares(amount, total, limit, lean, full):
    portions = [(1 << 20) // math.isqrt(standing ** lean) + 1 for standing in range(1, amount + 1)]
    largest = limit if full else min(limit, max(-(-total // amount), total * portions[0] // sum(portions)))
    least = 1 if total - largest >= amount - 1 else 0
    given, spare = [largest] + [least] * (amount - 1), total - largest - least * (amount - 1)
    while spare > 0:
        free = [i for i in range(1, amount) if given[i] < largest] or [i for i in range(1, amount) if given[i] < limit]
        mass, remaining = sum([portions[i] for i in free]), spare
        for i in free:
            addition = min(limit - given[i], max(1, remaining * portions[i] // mass), spare)
            given[i] = given[i] + addition
            spare = spare - addition
    return np.array(given)


def normal_values(stream_key, dims, spread, limit, shards=(), kind=jnp.bfloat16):
    loudness = steps_of(stream_key, dims, shards, -0.22, 0.18) if shards else 1.0
    values = jax.random.normal(stream_key, dims, jnp.float32) * spread * loudness
    return jnp.minimum(jnp.maximum(values, -limit), limit).astype(kind)


def setup_inputs(seed: int = 0) -> dict:
    key_of = jax.random.split(jax.random.key(seed), 16)
    queries = normal_values(key_of[0], (TOKENS, Q_HEADS, HD), 1.0, 6.0, ((0, 64), (1, 4)))
    keys = normal_values(key_of[1], (TOKENS, KV_HEADS, HD), 1.0, 6.0, ((0, 64), (1, 4)))
    values = normal_values(key_of[2], (TOKENS, KV_HEADS, HD), 1.0, 6.0, ((0, 64), (1, 4)))
    q_gain = draw_q_gain(jax.random.fold_in(key_of[15], 71), 0)
    k_gain = draw_k_gain(jax.random.fold_in(key_of[15], 71), 0)
    w_out = normal_values(key_of[5], (Q_HEADS * HD, D), (Q_HEADS * HD) ** -0.5, 0.09375, ((0, 4),))
    residual = normal_values(key_of[6], (TOKENS, D), 1.0, 6.0, ((0, 256),))
    gain_mix = jnp.clip(1.0 + 0.18 * jax.random.normal(key_of[7], (D,), jnp.float32), 0.1, 1.9)
    gain_pre = jnp.clip(1.0 + 0.18 * jax.random.normal(key_of[8], (D,), jnp.float32), 0.1, 1.9)
    routes_keys = jax.random.split(jax.random.fold_in(key_of[9], 1), TOKENS // TOK_TP)
    routes_turns = jax.random.permutation(jax.random.fold_in(key_of[9], 3), TOKENS // TOK_TP)
    routes = jax.vmap(lambda own, number: routed_block(jax.random.fold_in(key_of[9], 2), own, number, TOK_TP, EXPERTS, TOP, CAP, 1))(routes_keys, routes_turns).reshape((TOKENS, TOP))
    route_weights = jnp.clip(jnp.exp(math.log(1.0) - 2.3025851 * jax.random.uniform(key_of[10], (TOKENS, TOP), jnp.float32) ** steps_of(key_of[10], (TOKENS, TOP), ((0, 256),), -0.2, 0.2)), 0.1, 1.0)
    w_gate = normal_values(key_of[11], (EXPERTS, D, FF), (D // 16) ** -0.5, 0.5, ((0, 64), (2, 4)))
    w_up = normal_values(key_of[12], (EXPERTS, D, FF), (D // 16) ** -0.5, 0.5, ((0, 64), (2, 4)))
    w_down = normal_values(key_of[13], (EXPERTS, FF, D), FF ** -0.5, 0.125, ((0, 64), (1, 4)))
    gain_moe = jnp.clip(1.0 + 0.18 * jax.random.normal(key_of[14], (D,), jnp.float32), 0.1, 1.9)
    return {"queries": queries, "keys": keys, "values": values, "q_gain": q_gain, "k_gain": k_gain, "w_out": w_out, "residual": residual, "gain_mix": gain_mix, "gain_pre": gain_pre, "routes": routes, "route_weights": route_weights, "w_gate": w_gate, "w_up": w_up, "w_down": w_down, "gain_moe": gain_moe}


norm_eps = 1e-06
rope_theta = 10000.0
clamp_limit = 7.0
swish_alpha = 1.702

def rope_tables(positions, head_size):
    row_index = (positions // GRID_W).astype(jnp.float32)
    col_index = (positions % GRID_W).astype(jnp.float32)
    freq_count = head_size // 4
    inverse = rope_theta ** (-jnp.arange(freq_count, dtype=jnp.float32) / freq_count)
    angles = jnp.stack([row_index[:, None] * inverse, col_index[:, None] * inverse], axis=1)
    return (jnp.cos(angles), jnp.sin(angles))

def turn(array_in, cosine_table, sine_table):
    token_count, head_count, head_size = array_in.shape
    split_field = array_in.reshape(token_count, head_count, 2, 2, head_size // 4)
    first_half = split_field[:, :, :, 0, :]
    second_half = split_field[:, :, :, 1, :]
    cos_wide = cosine_table[:, None]
    sin_wide = sine_table[:, None]
    turned = jnp.stack([first_half * cos_wide - second_half * sin_wide, second_half * cos_wide + first_half * sin_wide], axis=3)
    return turned.reshape(token_count, head_count, head_size)

def scale_rows(array_in, gain_vec):
    return array_in * lax.rsqrt(lax.optimization_barrier(jnp.mean(array_in * array_in, axis=-1, keepdims=True)) + norm_eps) * gain_vec

def reference(queries, keys, values, q_gain, k_gain, w_out, residual, gain_mix, gain_pre, routes, route_weights, w_gate, w_up, w_down, gain_moe):
    positions = jnp.arange(TOKENS, dtype=jnp.int32)
    cosine_table, sine_table = rope_tables(positions, HD)
    q_turned = (turn(scale_rows(queries.astype(jnp.float32), q_gain), cosine_table, sine_table) * HD ** (-0.5)).astype(jnp.bfloat16)
    k_turned = turn(scale_rows(keys.astype(jnp.float32), k_gain), cosine_table, sine_table).astype(jnp.bfloat16)
    group_size = Q_HEADS // KV_HEADS
    qblock = math.gcd(TOKENS, 512)
    blocks = q_turned.reshape(TOKENS // qblock, qblock, KV_HEADS, group_size, HD)
    k_wide = k_turned.astype(jnp.float32)
    v_wide = values.astype(jnp.float32)

    def attend(block):
        scores = jnp.einsum('qkgd,skd->kgqs', block.astype(jnp.float32), k_wide)
        unnorm = jnp.exp(scores - lax.optimization_barrier(jnp.max(scores, axis=-1, keepdims=True)))
        totals = lax.optimization_barrier(jnp.sum(unnorm, axis=-1))
        summed = jnp.einsum('kgqs,skd->qkgd', unnorm.astype(jnp.bfloat16).astype(jnp.float32), v_wide)
        return (summed / jnp.moveaxis(totals, 2, 0)[..., None]).astype(jnp.bfloat16)
    mixed_heads = lax.map(attend, blocks).reshape(TOKENS, Q_HEADS * HD)
    projected = jnp.dot(mixed_heads, w_out, preferred_element_type=jnp.float32)
    middle = residual.astype(jnp.float32) + scale_rows(projected, gain_mix)
    normed = scale_rows(middle, gain_pre).astype(jnp.bfloat16)
    block_count = TOKENS // TOK_TP
    assign = TOK_TP * TOP
    flat_routes = routes.reshape(block_count, assign)
    expert_hits = (flat_routes[:, :, None] == jnp.arange(EXPERTS, dtype=jnp.int32)[None, None, :]).astype(jnp.int32)
    slot_index = lax.optimization_barrier(jnp.sum((jnp.cumsum(expert_hits, axis=1) - expert_hits) * expert_hits, axis=2)).astype(jnp.int32)
    block_ids = jnp.broadcast_to(jnp.arange(block_count, dtype=jnp.int32)[:, None], (block_count, assign))
    token_ids = (block_ids * TOK_TP + jnp.arange(assign, dtype=jnp.int32)[None, :] // TOP).astype(jnp.int32)
    slot_tokens = jnp.full((EXPERTS, block_count, CAP), TOKENS, jnp.int32).at[flat_routes, block_ids, slot_index].set(token_ids)
    padded = jnp.concatenate([normed, jnp.zeros((1, D), jnp.bfloat16)], axis=0)
    group_width = FF // N_TP

    def serve_expert(expert_args):
        token_rows, gate_weight, up_weight, down_weight = expert_args
        arrived_rows = padded[token_rows.reshape(-1)]
        gate_pre = jnp.minimum(jnp.dot(arrived_rows, gate_weight, preferred_element_type=jnp.float32), clamp_limit)
        up_pre = jnp.clip(jnp.dot(arrived_rows, up_weight, preferred_element_type=jnp.float32), -clamp_limit, clamp_limit)
        active = (gate_pre * jax.nn.sigmoid(swish_alpha * gate_pre) * (up_pre + 1.0)).astype(jnp.bfloat16)
        group_sums = jnp.einsum('rqf,qfd->rqd', active.reshape(-1, N_TP, group_width).astype(jnp.float32), down_weight.reshape(N_TP, group_width, D).astype(jnp.float32))
        group_sums = lax.optimization_barrier(group_sums.astype(jnp.bfloat16)).astype(jnp.float32)
        return lax.optimization_barrier(jnp.sum(group_sums, axis=1)).astype(jnp.bfloat16)
    expert_out = lax.map(serve_expert, (slot_tokens, w_gate, w_up, w_down))
    picked = expert_out.reshape(EXPERTS, block_count, CAP, D)[flat_routes, block_ids, slot_index]
    picked = picked.reshape(TOKENS, TOP, D).astype(jnp.float32)
    mixture = lax.optimization_barrier(jnp.sum(picked * route_weights[:, :, None], axis=1))
    return (middle + scale_rows(mixture, gain_moe)).astype(jnp.bfloat16)
```

```python
import jax
import jax.numpy as jnp
from jax import lax
from jax.experimental import pallas as pl
from jax.experimental.pallas import tpu as pltpu
from jax.sharding import PartitionSpec as P

TOP = 4
GRID_W = 64


norm_eps = 1e-06
rope_theta = 10000.0
clamp_limit = 7.0
swish_alpha = 1.702


def in_blocks(value, dim, devices):
    lengths = value.shape
    pieces = value.reshape(*lengths[:dim], devices, lengths[dim] // devices, *lengths[dim + 1 :])
    return jnp.moveaxis(pieces, dim, 0)


def sum_at_owner(value, axis, dim):
    pieces = in_blocks(value, dim, lax.axis_size(axis))
    arrived = lax.all_to_all(pieces, axis, split_axis=0, concat_axis=0, tiled=True)
    return arrived.astype(jnp.float32).sum(axis=0)


def rope_tables(positions, head_size):
    row_index = (positions // GRID_W).astype(jnp.float32)
    col_index = (positions % GRID_W).astype(jnp.float32)
    freq_count = head_size // 4
    inverse = rope_theta ** (-jnp.arange(freq_count, dtype=jnp.float32) / freq_count)
    angles = jnp.stack([row_index[:, None] * inverse, col_index[:, None] * inverse], axis=1)
    return (jnp.cos(angles), jnp.sin(angles))


def turn(array_in, cosine_table, sine_table):
    token_count, head_count, head_size = array_in.shape
    split_field = array_in.reshape(token_count, head_count, 2, 2, head_size // 4)
    first_half = split_field[:, :, :, 0, :]
    second_half = split_field[:, :, :, 1, :]
    cos_wide = cosine_table[:, None]
    sin_wide = sine_table[:, None]
    turned = jnp.stack(
        [
            first_half * cos_wide - second_half * sin_wide,
            second_half * cos_wide + first_half * sin_wide,
        ],
        axis=3,
    )
    return turned.reshape(token_count, head_count, head_size)


def scale_rows(array_in, gain_vec):
    return (
        array_in
        * lax.rsqrt(jnp.mean(array_in * array_in, axis=-1, keepdims=True) + norm_eps)
        * gain_vec
    )


def slot_table(route_rows, experts, capacity):
    flat_routes = route_rows.reshape(-1)
    expert_hits = (flat_routes[:, None] == jnp.arange(experts, dtype=jnp.int32)[None, :]).astype(
        jnp.int32
    )
    slot_index = jnp.sum((jnp.cumsum(expert_hits, axis=0) - expert_hits) * expert_hits, axis=1)
    target = flat_routes * capacity + slot_index
    slot_onehot = target[:, None] == jnp.arange(experts * capacity, dtype=jnp.int32)[None, :]
    return slot_onehot.astype(jnp.bfloat16).reshape(
        route_rows.shape[0], route_rows.shape[1], experts * capacity
    )


def expert_apply(arrived_rows, w_gate, w_up, w_down):
    gate_pre = jnp.minimum(
        jnp.einsum("serd,edf->serf", arrived_rows, w_gate, preferred_element_type=jnp.float32),
        clamp_limit,
    )
    up_pre = jnp.clip(
        jnp.einsum("serd,edf->serf", arrived_rows, w_up, preferred_element_type=jnp.float32),
        -clamp_limit,
        clamp_limit,
    )
    active = (gate_pre * jax.nn.sigmoid(swish_alpha * gate_pre) * (up_pre + 1.0)).astype(
        jnp.bfloat16
    )
    partial_value = jnp.einsum("serf,efd->serd", active, w_down, preferred_element_type=jnp.float32)
    return lax.optimization_barrier(partial_value.astype(jnp.bfloat16)).astype(jnp.float32)


def send_back(finished):
    return lax.all_to_all(finished, "sp", split_axis=0, concat_axis=0, tiled=True)


MESH = pl.DeviceIdType.MESH
NZ, NX = 8, 4
PIECE = 128


def attention_kernel(q_ref, kv_ref, out_ref, buf, qbuf, m_ref, l_ref, acc, obuf, rsem, qsem, asem, zup, zdn, bup, bdn, bxp, bxm, bfw, dsem, osem):
    sp = lax.axis_index("sp")
    core = lax.rem(sp, 2)
    chip = lax.div(sp, 2)
    x = lax.rem(chip, NX)
    z = lax.div(chip, NX)

    def dev(zz, xx, cc):
        return {"sp": (lax.rem(zz + 2 * NZ, NZ) * NX + lax.rem(xx + 2 * NX, NX)) * 2 + cc}

    def slot(kind, zz, xx):
        return kind * (NZ * NX) + lax.rem(zz + 2 * NZ, NZ) * NX + lax.rem(xx + 2 * NX, NX)

    partner = dev(z, x, 1 - core)
    z_up, z_dn = dev(z + 1, x, core), dev(z - 1, x, core)
    x_up, x_dn, x_far = dev(z, x + 1, core), dev(z, x - 1, core), dev(z, x + 2, core)

    mine = core * (NZ * NX) + chip
    buf[mine] = kv_ref[core]
    qbuf[pl.ds(pl.multiple_of(core * 512, 512), 512), :] = q_ref[core]
    m_ref[...] = jnp.full(m_ref.shape, -jnp.inf, jnp.float32)
    l_ref[...] = jnp.zeros(l_ref.shape, jnp.float32)
    acc[...] = jnp.zeros(acc.shape, jnp.float32)

    barrier = pltpu.get_barrier_semaphore()
    for peer in (partner, z_up, z_dn, x_up, x_dn, x_far):
        pl.semaphore_signal(barrier, inc=1, device_id=peer, device_id_type=MESH)
    pl.semaphore_wait(barrier, 6)

    def move(at, sem, to):
        return pltpu.make_async_remote_copy(
            src_ref=buf.at[at], dst_ref=buf.at[at], send_sem=sem, recv_sem=rsem.at[at], device_id=to, device_id_type=MESH
        )

    def send(at, sem, to):
        move(at, sem, to).start()

    def arrive(at):
        move(at, dsem.at[0], partner).wait_recv()

    def done(sem):
        move(0, sem, partner).wait_send()

    swap_kv = pltpu.make_async_remote_copy(
        src_ref=kv_ref.at[1 - core], dst_ref=buf.at[(1 - core) * 0 + core * (NZ * NX) + chip], send_sem=dsem.at[0],
        recv_sem=rsem.at[core * (NZ * NX) + chip], device_id=partner, device_id_type=MESH,
    )
    swap_q = pltpu.make_async_remote_copy(
        src_ref=q_ref.at[1 - core], dst_ref=qbuf.at[pl.ds(pl.multiple_of(core * 512, 512), 512), :], send_sem=dsem.at[1],
        recv_sem=qsem, device_id=partner, device_id_type=MESH,
    )
    swap_kv.start()
    swap_q.start()
    arrive((1 - core) * (NZ * NX) + chip)

    def attend(slots):
        keys = jnp.concatenate([buf[s, 0] for s in slots], axis=0)
        vals = jnp.concatenate([buf[s, 1] for s in slots], axis=1)
        for tile in range(4):
            cols = slice(tile * 256, tile * 256 + 256)
            scores = lax.dot_general(keys, qbuf[cols, :], (((1,), (1,)), ((), ())), preferred_element_type=jnp.float32)
            before = m_ref[:, cols]
            now = jnp.maximum(before, jnp.max(scores, axis=0, keepdims=True))
            shrink = jnp.exp(before - now)
            unnorm = jnp.exp(scores - now)
            l_ref[:, cols] = l_ref[:, cols] * shrink + jnp.sum(unnorm, axis=0, keepdims=True)
            acc[:, cols] = acc[:, cols] * shrink + jnp.dot(
                vals, unnorm.astype(jnp.bfloat16), preferred_element_type=jnp.float32
            )
            m_ref[:, cols] = now

    A, B = 0, 1
    own_a, own_b = slot(A, z, x), slot(B, z, x)
    send(own_b, bup.at[0], z_up)
    send(own_b, bdn.at[0], z_dn)
    send(own_a, asem.at[0], x_up)
    send(own_a, asem.at[1], x_dn)
    send(own_a, asem.at[2], x_far)
    send(own_a, zup.at[0], z_up)
    send(own_a, zdn.at[0], z_dn)
    send(own_b, bxp.at[0], x_up)
    send(own_b, bxm.at[0], x_dn)
    for j in (1, 3, 2):
        at = slot(A, z, x + j)
        arrive(at)
        send(at, zup.at[j], z_up)
        send(at, zdn.at[j], z_dn)
    swap_q.wait_recv()
    attend([own_a, own_b, slot(A, z, x + 1), slot(A, z, x + 3)])
    left, right, far = slot(B, z, x - 1), slot(B, z, x + 1), slot(B, z, x + 2)
    arrive(right)
    send(right, bfw.at[0], x_dn)
    arrive(left)

    def step(r, last):
        lo, hi = z - r, z + r
        b_lo, b_hi = slot(B, lo, x), slot(B, hi, x)
        arrive(b_lo)
        send(b_lo, bup.at[r], z_up)
        send(b_lo, bxp.at[2 * r - 1], x_up)
        send(b_lo, bxm.at[2 * r - 1], x_dn)
        arrive(b_hi)

        @pl.when(r < 3)
        def _():
            send(b_hi, bdn.at[r], z_dn)

        send(b_hi, bxp.at[2 * r], x_up)
        send(b_hi, bxm.at[2 * r], x_dn)
        for pair in ((0, 1), (3, 2)):
            group = []
            for j in pair:
                a_lo, a_hi = slot(A, lo, x + j), slot(A, hi, x + j)
                group += [a_lo, a_hi]
                arrive(a_lo)
                if j in (0, 1):
                    send(a_lo, zup.at[r * 4 + j], z_up)
                else:
                    pl.when(r < 3)(lambda a_lo=a_lo, j=j: send(a_lo, zup.at[r * 4 + j], z_up))
                arrive(a_hi)
                if j in (2, 3):
                    send(a_hi, zdn.at[r * 4 + j], z_dn)
                else:
                    pl.when(r < 3)(lambda a_hi=a_hi, j=j: send(a_hi, zdn.at[r * 4 + j], z_dn))
            attend(group)
        lo_left, lo_right, lo_far = slot(B, lo, x - 1), slot(B, lo, x + 1), slot(B, lo, x + 2)
        hi_left, hi_right, hi_far = slot(B, hi, x - 1), slot(B, hi, x + 1), slot(B, hi, x + 2)
        arrive(lo_left)
        send(lo_left, bfw.at[2 * r - 1], x_up)
        arrive(hi_right)
        send(hi_right, bfw.at[2 * r], x_dn)
        attend([b_lo, b_hi, lo_left, hi_right])
        arrive(lo_right)
        arrive(hi_left)
        arrive(lo_far)
        arrive(hi_far)
        attend([lo_right, hi_left, lo_far, hi_far])

    arrive(far)
    attend([slot(A, z, x + 2), left, right, far])

    @pl.loop(1, 4)
    def _(r):
        step(r, False)

    opp = z + 4
    b_op = slot(B, opp, x)
    arrive(b_op)
    send(b_op, bxp.at[7], x_up)
    send(b_op, bxm.at[7], x_dn)
    group = []
    for j in (0, 1, 3, 2):
        at = slot(A, opp, x + j)
        arrive(at)
        group.append(at)
    b_left, b_right, b_far = slot(B, opp, x - 1), slot(B, opp, x + 1), slot(B, opp, x + 2)
    arrive(b_left)
    send(b_left, bfw.at[7], x_up)
    attend(group)
    arrive(b_right)
    arrive(b_far)
    attend([b_op, b_left, b_right, b_far])

    def heads_of(which):
        cols = pl.ds(pl.multiple_of(which * 512, 512), 512)
        return (acc[:, cols] / l_ref[:, cols]).astype(jnp.bfloat16)

    theirs = heads_of(1 - core)
    obuf[2] = theirs
    own = heads_of(core)
    obuf[core] = own
    swap_o = pltpu.make_async_remote_copy(
        src_ref=obuf.at[2], dst_ref=obuf.at[core], send_sem=osem.at[0], recv_sem=osem.at[1], device_id=partner, device_id_type=MESH
    )
    swap_o.start()
    for i in range(3):
        done(asem.at[i])
    for i in range(4):
        done(bup.at[i])
        for j in range(4):
            if i < 3 or j in (0, 1):
                done(zup.at[i * 4 + j])
            if i < 3 or j in (2, 3):
                done(zdn.at[i * 4 + j])
    for i in range(3):
        done(bdn.at[i])
    for i in range(8):
        done(bxp.at[i])
        done(bxm.at[i])
        done(bfw.at[i])
    swap_kv.wait_send()
    swap_q.wait_send()
    swap_o.wait_send()
    swap_o.wait_recv()
    for g in range(2):
        for h in range(4):
            head = obuf[g, :, h * 128 : h * 128 + 128]
            out_ref[:, (g * 4 + h) * 128 : (g * 4 + h) * 128 + 128] = head.T


def attention(q_two, kv_two):
    return pl.pallas_call(
        attention_kernel,
        out_shape=jax.ShapeDtypeStruct((128, 1024), jnp.bfloat16),
        in_specs=[pl.BlockSpec(memory_space=pltpu.VMEM)] * 2,
        out_specs=pl.BlockSpec(memory_space=pltpu.VMEM),
        scratch_shapes=[
            pltpu.VMEM((64, 2, PIECE, 128), jnp.bfloat16),
            pltpu.VMEM((1024, 128), jnp.bfloat16),
            pltpu.VMEM((1, 1024), jnp.float32),
            pltpu.VMEM((1, 1024), jnp.float32),
            pltpu.VMEM((128, 1024), jnp.float32),
            pltpu.VMEM((3, 128, 512), jnp.bfloat16),
            pltpu.SemaphoreType.DMA((64,)),
            pltpu.SemaphoreType.DMA,
            pltpu.SemaphoreType.DMA((3,)),
            pltpu.SemaphoreType.DMA((16,)),
            pltpu.SemaphoreType.DMA((16,)),
            pltpu.SemaphoreType.DMA((4,)),
            pltpu.SemaphoreType.DMA((4,)),
            pltpu.SemaphoreType.DMA((8,)),
            pltpu.SemaphoreType.DMA((8,)),
            pltpu.SemaphoreType.DMA((8,)),
            pltpu.SemaphoreType.DMA((2,)),
            pltpu.SemaphoreType.DMA((2,)),
        ],
        compiler_params=pltpu.CompilerParams(collective_id=0, has_side_effects=True),
        cost_estimate=pl.CostEstimate(flops=4 * 1024 * 8192 * 128, bytes_accessed=1 << 20, transcendentals=1024 * 8192),
        name="gather_attention",
    )(q_two, kv_two)


def on_device(
    queries,
    keys,
    values,
    q_gain,
    k_gain,
    w_out,
    residual,
    gain_mix,
    gain_pre,
    routes,
    route_weights,
    w_gate,
    w_up,
    w_down,
    gain_moe,
):
    tok_rows, head_local, head_size = queries.shape
    kv_local = keys.shape[1]
    group_size = head_local // kv_local
    positions = lax.axis_index("sp") * tok_rows + jnp.arange(tok_rows, dtype=jnp.int32)
    cosine_table, sine_table = rope_tables(positions, head_size)
    q_turned = (
        turn(scale_rows(queries.astype(jnp.float32), q_gain), cosine_table, sine_table)
        * head_size ** (-0.5)
    ).astype(jnp.bfloat16)
    k_turned = turn(scale_rows(keys.astype(jnp.float32), k_gain), cosine_table, sine_table).astype(
        jnp.bfloat16
    )
    q_two = q_turned.transpose(1, 0, 2).reshape(kv_local, group_size * tok_rows, head_size)
    kv_two = jnp.stack([k_turned.transpose(1, 0, 2), values.transpose(1, 2, 0)], axis=1)
    mixed_heads = attention(q_two, kv_two)
    tok_part = residual.shape[0]
    width = residual.shape[1]
    projected = sum_at_owner(
        jnp.dot(mixed_heads, w_out, preferred_element_type=jnp.float32).astype(jnp.bfloat16),
        "tp",
        0,
    )
    middle = residual.astype(jnp.float32) + scale_rows(projected, gain_mix)
    normed = scale_rows(middle, gain_pre).astype(jnp.bfloat16)
    local_experts = w_gate.shape[0]
    experts_all = local_experts * lax.axis_size("sp")
    capacity = max(2, (2 * tok_part * TOP + experts_all - 1) // experts_all)
    tables = slot_table(routes, experts_all, capacity)
    chosen = jnp.sum(tables, axis=1)
    outbound = jnp.einsum("tp,td->pd", chosen, normed, preferred_element_type=jnp.float32)
    outbound = outbound.astype(jnp.bfloat16).reshape(experts_all, capacity, width)
    arrived_rows = lax.all_gather(
        lax.all_to_all(outbound, "sp", split_axis=0, concat_axis=0, tiled=True),
        "tp",
        axis=0,
        tiled=True,
    )
    leading = arrived_rows.shape[0] // local_experts
    partial_value = expert_apply(
        arrived_rows.reshape(leading, local_experts, arrived_rows.shape[1], width),
        w_gate,
        w_up,
        w_down,
    )
    summed = lax.psum_scatter(
        partial_value.reshape(arrived_rows.shape).astype(jnp.bfloat16),
        "tp",
        scatter_dimension=0,
        tiled=True,
    )
    returned = send_back(summed)
    gathered = jnp.einsum(
        "tkp,pd->tkd",
        tables,
        returned.reshape(experts_all * capacity, width),
        preferred_element_type=jnp.float32,
    )
    mixture = jnp.sum(gathered * route_weights[:, :, None], axis=1)
    return (middle + scale_rows(mixture, gain_moe)).astype(jnp.bfloat16)


def solution(mesh):
    placed = (
        P("sp", "tp", None),
        P("sp", "tp", None),
        P("sp", "tp", None),
        P(),
        P(),
        P("tp", None),
        P(("sp", "tp"), None),
        P(),
        P(),
        P(("sp", "tp"), None),
        P(("sp", "tp"), None),
        P("sp", None, "tp"),
        P("sp", None, "tp"),
        P("sp", "tp", None),
        P(),
    )
    return jax.shard_map(
        on_device, mesh=mesh, in_specs=placed, out_specs=P(("sp", "tp"), None), check_vma=False
    )
```

```python
import jax
import jax.numpy as jnp
from jax import lax
from jax.experimental import pallas as pl
from jax.experimental.pallas import tpu as pltpu
from jax.sharding import PartitionSpec as P

TOP = 4
GRID_W = 64


norm_eps = 1e-06
rope_theta = 10000.0
clamp_limit = 7.0
swish_alpha = 1.702


def in_blocks(value, dim, devices):
    lengths = value.shape
    pieces = value.reshape(*lengths[:dim], devices, lengths[dim] // devices, *lengths[dim + 1 :])
    return jnp.moveaxis(pieces, dim, 0)


def sum_at_owner(value, axis, dim):
    pieces = in_blocks(value, dim, lax.axis_size(axis))
    arrived = lax.all_to_all(pieces, axis, split_axis=0, concat_axis=0, tiled=True)
    return arrived.astype(jnp.float32).sum(axis=0)


def rope_tables(positions, head_size):
    row_index = (positions // GRID_W).astype(jnp.float32)
    col_index = (positions % GRID_W).astype(jnp.float32)
    freq_count = head_size // 4
    inverse = rope_theta ** (-jnp.arange(freq_count, dtype=jnp.float32) / freq_count)
    angles = jnp.stack([row_index[:, None] * inverse, col_index[:, None] * inverse], axis=1)
    return (jnp.cos(angles), jnp.sin(angles))


def turn(array_in, cosine_table, sine_table):
    token_count, head_count, head_size = array_in.shape
    split_field = array_in.reshape(token_count, head_count, 2, 2, head_size // 4)
    first_half = split_field[:, :, :, 0, :]
    second_half = split_field[:, :, :, 1, :]
    cos_wide = cosine_table[:, None]
    sin_wide = sine_table[:, None]
    turned = jnp.stack(
        [
            first_half * cos_wide - second_half * sin_wide,
            second_half * cos_wide + first_half * sin_wide,
        ],
        axis=3,
    )
    return turned.reshape(token_count, head_count, head_size)


def scale_rows(array_in, gain_vec):
    return (
        array_in
        * lax.rsqrt(jnp.mean(array_in * array_in, axis=-1, keepdims=True) + norm_eps)
        * gain_vec
    )


def slot_tables(routes, route_weights):
    core = lax.rem(lax.axis_index("sp"), 2)
    swap = [(i, i ^ 1) for i in range(lax.axis_size("sp"))]
    count = routes.shape[0]
    both = jnp.concatenate([routes.astype(jnp.float32), route_weights], axis=1)
    other = lax.ppermute(both, "sp", swap)
    ordered = jnp.where(core == 0, jnp.stack([both, other]), jnp.stack([other, both]))
    chosen, weights = ordered[:, :, :TOP].astype(jnp.int32), ordered[:, :, TOP:]
    flat = chosen.reshape(2, count * TOP)
    same = (flat[:, :, None] == flat[:, None, :]).astype(jnp.int32)
    place = jnp.arange(count * TOP, dtype=jnp.int32)
    earlier = (place[None, :] < place[:, None]).astype(jnp.int32)
    rank = jnp.sum(same * earlier, axis=2).reshape(2, count, TOP)
    side = jnp.arange(2, dtype=jnp.int32)[:, None, None]
    target = jnp.where(chosen % 2 == core, (chosen // 2) * 8 + side * 4 + rank, -1)
    target, weights = target.reshape(2 * count, TOP), weights.reshape(2 * count, TOP)
    spots = jnp.arange(256, dtype=jnp.int32)
    disp = jnp.sum((target[None, :, :] == spots[:, None, None]).astype(jnp.float32), axis=2)
    mixw = jnp.sum(jnp.where(target[:, None, :] == spots[None, :, None], weights[:, None, :], 0.0), axis=2)
    return disp.astype(jnp.bfloat16), mixw


MESH = pl.DeviceIdType.MESH
NZ, NX = 8, 4
PIECE = 128


def attention_kernel(q_ref, kv_ref, out_ref, buf, qbuf, m_ref, l_ref, acc, obuf, rsem, qsem, asem, zup, zdn, bup, bdn, bxp, bxm, bfw, dsem, osem):
    sp = lax.axis_index("sp")
    core = lax.rem(sp, 2)
    chip = lax.div(sp, 2)
    x = lax.rem(chip, NX)
    z = lax.div(chip, NX)

    def dev(zz, xx, cc):
        return {"sp": (lax.rem(zz + 2 * NZ, NZ) * NX + lax.rem(xx + 2 * NX, NX)) * 2 + cc}

    def slot(kind, zz, xx):
        return kind * (NZ * NX) + lax.rem(zz + 2 * NZ, NZ) * NX + lax.rem(xx + 2 * NX, NX)

    partner = dev(z, x, 1 - core)
    z_up, z_dn = dev(z + 1, x, core), dev(z - 1, x, core)
    x_up, x_dn, x_far = dev(z, x + 1, core), dev(z, x - 1, core), dev(z, x + 2, core)

    mine = core * (NZ * NX) + chip
    buf[mine] = kv_ref[core]
    qbuf[pl.ds(pl.multiple_of(core * 512, 512), 512), :] = q_ref[core]
    m_ref[...] = jnp.full(m_ref.shape, -jnp.inf, jnp.float32)
    l_ref[...] = jnp.zeros(l_ref.shape, jnp.float32)
    acc[...] = jnp.zeros(acc.shape, jnp.float32)

    barrier = pltpu.get_barrier_semaphore()
    for peer in (partner, z_up, z_dn, x_up, x_dn, x_far):
        pl.semaphore_signal(barrier, inc=1, device_id=peer, device_id_type=MESH)
    pl.semaphore_wait(barrier, 6)

    def move(at, sem, to):
        return pltpu.make_async_remote_copy(
            src_ref=buf.at[at], dst_ref=buf.at[at], send_sem=sem, recv_sem=rsem.at[at], device_id=to, device_id_type=MESH
        )

    def send(at, sem, to):
        move(at, sem, to).start()

    def arrive(at):
        move(at, dsem.at[0], partner).wait_recv()

    def done(sem):
        move(0, sem, partner).wait_send()

    swap_kv = pltpu.make_async_remote_copy(
        src_ref=kv_ref.at[1 - core], dst_ref=buf.at[(1 - core) * 0 + core * (NZ * NX) + chip], send_sem=dsem.at[0],
        recv_sem=rsem.at[core * (NZ * NX) + chip], device_id=partner, device_id_type=MESH,
    )
    swap_q = pltpu.make_async_remote_copy(
        src_ref=q_ref.at[1 - core], dst_ref=qbuf.at[pl.ds(pl.multiple_of(core * 512, 512), 512), :], send_sem=dsem.at[1],
        recv_sem=qsem, device_id=partner, device_id_type=MESH,
    )
    swap_kv.start()
    swap_q.start()
    arrive((1 - core) * (NZ * NX) + chip)

    def attend(slots):
        keys = jnp.concatenate([buf[s, 0] for s in slots], axis=0)
        vals = jnp.concatenate([buf[s, 1] for s in slots], axis=1)
        for tile in range(4):
            cols = slice(tile * 256, tile * 256 + 256)
            scores = lax.dot_general(keys, qbuf[cols, :], (((1,), (1,)), ((), ())), preferred_element_type=jnp.float32)
            before = m_ref[:, cols]
            now = jnp.maximum(before, jnp.max(scores, axis=0, keepdims=True))
            shrink = jnp.exp(before - now)
            unnorm = jnp.exp(scores - now)
            l_ref[:, cols] = l_ref[:, cols] * shrink + jnp.sum(unnorm, axis=0, keepdims=True)
            acc[:, cols] = acc[:, cols] * shrink + jnp.dot(
                vals, unnorm.astype(jnp.bfloat16), preferred_element_type=jnp.float32
            )
            m_ref[:, cols] = now

    A, B = 0, 1
    own_a, own_b = slot(A, z, x), slot(B, z, x)
    send(own_b, bup.at[0], z_up)
    send(own_b, bdn.at[0], z_dn)
    send(own_a, asem.at[0], x_up)
    send(own_a, asem.at[1], x_dn)
    send(own_a, asem.at[2], x_far)
    send(own_a, zup.at[0], z_up)
    send(own_a, zdn.at[0], z_dn)
    send(own_b, bxp.at[0], x_up)
    send(own_b, bxm.at[0], x_dn)
    for j in (1, 3, 2):
        at = slot(A, z, x + j)
        arrive(at)
        send(at, zup.at[j], z_up)
        send(at, zdn.at[j], z_dn)
    swap_q.wait_recv()
    attend([own_a, own_b, slot(A, z, x + 1), slot(A, z, x + 3)])
    left, right, far = slot(B, z, x - 1), slot(B, z, x + 1), slot(B, z, x + 2)
    arrive(right)
    send(right, bfw.at[0], x_dn)
    arrive(left)

    def step(r, last):
        lo, hi = z - r, z + r
        b_lo, b_hi = slot(B, lo, x), slot(B, hi, x)
        arrive(b_lo)
        send(b_lo, bup.at[r], z_up)
        send(b_lo, bxp.at[2 * r - 1], x_up)
        send(b_lo, bxm.at[2 * r - 1], x_dn)
        arrive(b_hi)

        @pl.when(r < 3)
        def _():
            send(b_hi, bdn.at[r], z_dn)

        send(b_hi, bxp.at[2 * r], x_up)
        send(b_hi, bxm.at[2 * r], x_dn)
        for pair in ((0, 1), (3, 2)):
            group = []
            for j in pair:
                a_lo, a_hi = slot(A, lo, x + j), slot(A, hi, x + j)
                group += [a_lo, a_hi]
                arrive(a_lo)
                if j in (0, 1):
                    send(a_lo, zup.at[r * 4 + j], z_up)
                else:
                    pl.when(r < 3)(lambda a_lo=a_lo, j=j: send(a_lo, zup.at[r * 4 + j], z_up))
                arrive(a_hi)
                if j in (2, 3):
                    send(a_hi, zdn.at[r * 4 + j], z_dn)
                else:
                    pl.when(r < 3)(lambda a_hi=a_hi, j=j: send(a_hi, zdn.at[r * 4 + j], z_dn))
            attend(group)
        lo_left, lo_right, lo_far = slot(B, lo, x - 1), slot(B, lo, x + 1), slot(B, lo, x + 2)
        hi_left, hi_right, hi_far = slot(B, hi, x - 1), slot(B, hi, x + 1), slot(B, hi, x + 2)
        arrive(lo_left)
        send(lo_left, bfw.at[2 * r - 1], x_up)
        arrive(hi_right)
        send(hi_right, bfw.at[2 * r], x_dn)
        attend([b_lo, b_hi, lo_left, hi_right])
        arrive(lo_right)
        arrive(hi_left)
        arrive(lo_far)
        arrive(hi_far)
        attend([lo_right, hi_left, lo_far, hi_far])

    arrive(far)
    attend([slot(A, z, x + 2), left, right, far])

    @pl.loop(1, 4)
    def _(r):
        step(r, False)

    opp = z + 4
    b_op = slot(B, opp, x)
    arrive(b_op)
    send(b_op, bxp.at[7], x_up)
    send(b_op, bxm.at[7], x_dn)
    group = []
    for j in (0, 1, 3, 2):
        at = slot(A, opp, x + j)
        arrive(at)
        group.append(at)
    b_left, b_right, b_far = slot(B, opp, x - 1), slot(B, opp, x + 1), slot(B, opp, x + 2)
    arrive(b_left)
    send(b_left, bfw.at[7], x_up)
    attend(group)
    arrive(b_right)
    arrive(b_far)
    attend([b_op, b_left, b_right, b_far])

    def heads_of(which):
        cols = pl.ds(pl.multiple_of(which * 512, 512), 512)
        return (acc[:, cols] / l_ref[:, cols]).astype(jnp.bfloat16)

    theirs = heads_of(1 - core)
    obuf[2] = theirs
    own = heads_of(core)
    obuf[core] = own
    swap_o = pltpu.make_async_remote_copy(
        src_ref=obuf.at[2], dst_ref=obuf.at[core], send_sem=osem.at[0], recv_sem=osem.at[1], device_id=partner, device_id_type=MESH
    )
    swap_o.start()
    for i in range(3):
        done(asem.at[i])
    for i in range(4):
        done(bup.at[i])
        for j in range(4):
            if i < 3 or j in (0, 1):
                done(zup.at[i * 4 + j])
            if i < 3 or j in (2, 3):
                done(zdn.at[i * 4 + j])
    for i in range(3):
        done(bdn.at[i])
    for i in range(8):
        done(bxp.at[i])
        done(bxm.at[i])
        done(bfw.at[i])
    swap_kv.wait_send()
    swap_q.wait_send()
    swap_o.wait_send()
    swap_o.wait_recv()
    for g in range(2):
        for h in range(4):
            head = obuf[g, :, h * 128 : h * 128 + 128]
            out_ref[:, (g * 4 + h) * 128 : (g * 4 + h) * 128 + 128] = head.T


def attention(q_two, kv_two):
    return pl.pallas_call(
        attention_kernel,
        out_shape=jax.ShapeDtypeStruct((128, 1024), jnp.bfloat16),
        in_specs=[pl.BlockSpec(memory_space=pltpu.VMEM)] * 2,
        out_specs=pl.BlockSpec(memory_space=pltpu.VMEM),
        scratch_shapes=[
            pltpu.VMEM((64, 2, PIECE, 128), jnp.bfloat16),
            pltpu.VMEM((1024, 128), jnp.bfloat16),
            pltpu.VMEM((1, 1024), jnp.float32),
            pltpu.VMEM((1, 1024), jnp.float32),
            pltpu.VMEM((128, 1024), jnp.float32),
            pltpu.VMEM((3, 128, 512), jnp.bfloat16),
            pltpu.SemaphoreType.DMA((64,)),
            pltpu.SemaphoreType.DMA,
            pltpu.SemaphoreType.DMA((3,)),
            pltpu.SemaphoreType.DMA((16,)),
            pltpu.SemaphoreType.DMA((16,)),
            pltpu.SemaphoreType.DMA((4,)),
            pltpu.SemaphoreType.DMA((4,)),
            pltpu.SemaphoreType.DMA((8,)),
            pltpu.SemaphoreType.DMA((8,)),
            pltpu.SemaphoreType.DMA((8,)),
            pltpu.SemaphoreType.DMA((2,)),
            pltpu.SemaphoreType.DMA((2,)),
        ],
        compiler_params=pltpu.CompilerParams(collective_id=0, has_side_effects=True),
        cost_estimate=pl.CostEstimate(flops=4 * 1024 * 8192 * 128, bytes_accessed=1 << 20, transcendentals=1024 * 8192),
        name="gather_attention",
    )(q_two, kv_two)


GROUP_ORDER = (0, 1, 7, 2, 6, 3, 5, 4)
VIA_UP = (3, 6, 1, 0)
VIA_DN = (4, 5, 2, 7)


def experts_kernel(normed_ref, disp_ref, mixw_ref, middle_ref, gain_ref, wg_hbm, wu_hbm, wd_hbm, out_ref,
                   both, msgs, rows, act, part, mid, fin, ret, mixs, wg, wu, wd,
                   wsem, msend, mrecv, gup, gdn, gfw, grecv, s_first, s_direct, s_mid, midrecv, finrecv, rsend, rrecv, nsem, xsem):
    sp = lax.axis_index("sp")
    t = lax.axis_index("tp")
    core = lax.rem(sp, 2)
    chip = lax.div(sp, 2)
    x = lax.rem(chip, NX)
    z = lax.div(chip, NX)
    t_up, t_dn, t_far = lax.rem(t + 1, 4), lax.rem(t + 3, 4), lax.rem(t + 2, 4)

    def chip_at(dz, dx):
        return lax.rem(z + dz, NZ) * NX + lax.rem(x + dx, NX)

    def plane(which):
        return {"sp": which * 2 + core}

    partner = {"sp": chip * 2 + 1 - core}
    up, dn = {"tp": t_up}, {"tp": t_dn}

    loads = [
        pltpu.make_async_copy(wg_hbm, wg, wsem.at[0]),
        pltpu.make_async_copy(wu_hbm, wu, wsem.at[1]),
        pltpu.make_async_copy(wd_hbm, wd, wsem.at[2]),
    ]
    for load in loads:
        load.start()
    both[core] = normed_ref[...]

    barrier = pltpu.get_barrier_semaphore()
    for peer in (partner, up, dn):
        pl.semaphore_signal(barrier, inc=1, device_id=peer, device_id_type=MESH)
    others = [(dz, dx) for dz in GROUP_ORDER for dx in (0, 1, 3, 2) if (dz, dx) != (0, 0)]
    for dz, dx in others:
        pl.semaphore_signal(barrier, inc=1, device_id=plane(chip_at(dz, dx)), device_id_type=MESH)
    pl.semaphore_wait(barrier, 3 + len(others))

    def remote(src, dst, send_sem, recv_sem, to):
        return pltpu.make_async_remote_copy(
            src_ref=src, dst_ref=dst, send_sem=send_sem, recv_sem=recv_sem, device_id=to, device_id_type=MESH
        )

    swap = remote(normed_ref, both.at[core], nsem.at[0], nsem.at[1], partner)
    swap.start()
    swap.wait()
    tokens = jnp.concatenate([both[0], both[1]], axis=0)
    for cut in range(4):
        cols = slice(cut * 512, cut * 512 + 512)
        msgs[:, :, cols] = (
            jnp.dot(disp_ref[...], tokens[:, cols], preferred_element_type=jnp.float32)
            .astype(jnp.bfloat16)
            .reshape(32, 8, 512)
        )

    for dz, dx in others:
        to = chip_at(dz, dx)
        remote(msgs.at[to], rows.at[t, chip], msend.at[to], mrecv.at[chip], plane(to)).start()
    rows[t, chip] = msgs[chip]

    def chunk_at(which, dz):
        first = lax.rem(z + NZ - dz, NZ) * NX
        return rows.at[which, pl.ds(first, NX)]

    def give(dz, sem, to):
        ref = chunk_at(t, dz)
        return remote(ref, ref, sem, grecv.at[t * 8 + dz], to)

    def take(which, dz):
        ref = chunk_at(which, dz)
        remote(ref, ref, gup.at[0], grecv.at[which * 8 + dz], up).wait_recv()

    def hand(which, dz, to):
        ref = chunk_at(which, dz)
        return remote(ref, ref, gfw.at[dz], grecv.at[which * 8 + dz], to)

    def relay(dz):
        take(t_dn, dz)
        if dz in VIA_UP:
            hand(t_dn, dz, up).start()
        take(t_up, dz)
        if dz in VIA_DN:
            hand(t_up, dz, dn).start()

    for i, dz in enumerate(GROUP_ORDER):
        for dx in (0, 1, 3, 2):
            if (dz, dx) != (0, 0):
                source = chip_at(NZ - dz, dx)
                remote(msgs.at[0], rows.at[t, source], msend.at[0], mrecv.at[source], partner).wait_recv()
        give(dz, gup.at[dz], up).start()
        give(dz, gdn.at[dz], dn).start()
        if i > 0:
            relay(GROUP_ORDER[i - 1])
    for load in loads:
        load.wait()

    def serve(which):
        data = rows[which].reshape(256, 2048)
        for f in range(2):
            cols = slice(f * 256, f * 256 + 256)
            gate = jnp.minimum(jnp.dot(data, wg[:, cols], preferred_element_type=jnp.float32), clamp_limit)
            lift = jnp.clip(jnp.dot(data, wu[:, cols], preferred_element_type=jnp.float32), -clamp_limit, clamp_limit)
            act[:, cols] = (gate * jax.nn.sigmoid(swish_alpha * gate) * (lift + 1.0)).astype(jnp.bfloat16)
        for cut in range(8):
            cols = slice(cut * 256, cut * 256 + 256)
            part[which, :, :, cols] = (
                jnp.dot(act[...], wd[:, cols], preferred_element_type=jnp.float32).astype(jnp.bfloat16).reshape(32, 8, 256)
            )

    def group(dz):
        return pl.ds(lax.rem(z + NZ - dz, NZ) * NX, NX)

    serve(t)
    relay(GROUP_ORDER[-1])
    serve(t_up)
    for k, dz in enumerate(VIA_DN):
        remote(part.at[t_up, group(dz)], fin.at[0, group(dz)], s_direct.at[k], finrecv.at[dz], up).start()
    serve(t_dn)
    for k, dz in enumerate(VIA_UP):
        remote(part.at[t_dn, group(dz)], fin.at[1, group(dz)], s_direct.at[4 + k], finrecv.at[8 + dz], dn).start()
    for dz in GROUP_ORDER:
        take(t_far, dz)
    serve(t_far)
    for k in range(4):
        remote(part.at[t_far, group(VIA_UP[k])], mid.at[0, k], s_first.at[k], midrecv.at[k], up).start()
        remote(part.at[t_far, group(VIA_DN[k])], mid.at[1, k], s_first.at[4 + k], midrecv.at[4 + k], dn).start()
    for k in range(4):
        for way, (dzs, owner, to) in enumerate(((VIA_UP, t_up, up), (VIA_DN, t_dn, dn))):
            where = group(dzs[k])
            remote(part.at[owner, where], mid.at[way, k], s_first.at[0], midrecv.at[way * 4 + k], up).wait_recv()
            total = part[owner, where].astype(jnp.float32) + mid[way, k].astype(jnp.float32)
            part[owner, where] = total.astype(jnp.bfloat16)
            remote(part.at[owner, where], fin.at[way, where], s_mid.at[way * 4 + k], finrecv.at[way * 8 + dzs[k]], to).start()
    for k in range(4):
        for dz in (VIA_UP[k], VIA_DN[k]):
            where = group(dz)
            for way in range(2):
                remote(part.at[t, where], fin.at[way, where], s_first.at[0], finrecv.at[way * 8 + dz], up).wait_recv()
            total = part[t, where].astype(jnp.float32) + fin[0, where].astype(jnp.float32) + fin[1, where].astype(jnp.float32)
            part[t, where] = total.astype(jnp.bfloat16)
            for dx in (2, 1, 3, 0):
                to = chip_at(NZ - dz, dx)
                if (dz, dx) != (0, 0):
                    remote(part.at[t, to], ret.at[chip], rsend.at[to], rrecv.at[chip], plane(to)).start()
    ret[chip] = part[t, chip]
    for dz, dx in others:
        source = chip_at(dz, dx)
        remote(part.at[t, 0], ret.at[source], rsend.at[0], rrecv.at[source], partner).wait_recv()
    weight = mixw_ref[...]
    coarse = weight.astype(jnp.bfloat16)
    fine = (weight - coarse.astype(jnp.float32)).astype(jnp.bfloat16)
    for cut in range(4):
        cols = slice(cut * 512, cut * 512 + 512)
        came = ret[:, :, cols].reshape(256, 512)
        mixed = jnp.dot(coarse, came, preferred_element_type=jnp.float32) + jnp.dot(
            fine, came, preferred_element_type=jnp.float32
        )
        mixs[0, :, cols] = mixed[:32]
        mixs[1, :, cols] = mixed[32:]
    swap_mix = remote(mixs.at[1 - core], mixs.at[2], xsem.at[0], xsem.at[1], partner)
    swap_mix.start()

    def sent(src, sem):
        remote(src, src, sem, nsem.at[1], partner).wait_send()

    for dz, dx in others:
        to = chip_at(dz, dx)
        sent(msgs.at[0], msend.at[to])
        sent(msgs.at[0], rsend.at[to])
    for i in range(8):
        for sems in (gup, gdn, gfw, s_first, s_direct, s_mid):
            sent(mid.at[0, 0], sems.at[i])
    swap_mix.wait()
    mixture = mixs[core] + mixs[2]
    scale = lax.rsqrt(jnp.mean(mixture * mixture, axis=-1, keepdims=True) + norm_eps)
    out_ref[...] = (middle_ref[...] + mixture * scale * gain_ref[...]).astype(jnp.bfloat16)


def experts(normed, disp, mixw, middle, gain, w_gate, w_up, w_down):
    whole, remote = pl.BlockSpec(memory_space=pltpu.VMEM), pl.BlockSpec(memory_space=pl.ANY)
    dma = pltpu.SemaphoreType.DMA
    return pl.pallas_call(
        experts_kernel,
        out_shape=jax.ShapeDtypeStruct((32, 2048), jnp.bfloat16),
        in_specs=[whole] * 5 + [remote] * 3,
        out_specs=whole,
        scratch_shapes=[
            pltpu.VMEM((2, 32, 2048), jnp.bfloat16),
            pltpu.VMEM((32, 8, 2048), jnp.bfloat16),
            pltpu.VMEM((4, 32, 8, 2048), jnp.bfloat16),
            pltpu.VMEM((256, 512), jnp.bfloat16),
            pltpu.VMEM((4, 32, 8, 2048), jnp.bfloat16),
            pltpu.VMEM((2, 4, 4, 8, 2048), jnp.bfloat16),
            pltpu.VMEM((2, 32, 8, 2048), jnp.bfloat16),
            pltpu.VMEM((32, 8, 2048), jnp.bfloat16),
            pltpu.VMEM((3, 32, 2048), jnp.float32),
            pltpu.VMEM((2048, 512), jnp.bfloat16),
            pltpu.VMEM((2048, 512), jnp.bfloat16),
            pltpu.VMEM((512, 2048), jnp.bfloat16),
            dma((3,)),
            dma((32,)),
            dma((32,)),
            dma((8,)),
            dma((8,)),
            dma((8,)),
            dma((32,)),
            dma((8,)),
            dma((8,)),
            dma((8,)),
            dma((8,)),
            dma((16,)),
            dma((32,)),
            dma((32,)),
            dma((2,)),
            dma((2,)),
        ],
        compiler_params=pltpu.CompilerParams(collective_id=1, has_side_effects=True, vmem_limit_bytes=48 << 20),
        cost_estimate=pl.CostEstimate(flops=6 * 1024 * 2048 * 512, bytes_accessed=8 << 20, transcendentals=1024 * 512),
        name="experts",
    )(normed, disp, mixw, middle, gain, w_gate, w_up, w_down)


def on_device(
    queries,
    keys,
    values,
    q_gain,
    k_gain,
    w_out,
    residual,
    gain_mix,
    gain_pre,
    routes,
    route_weights,
    w_gate,
    w_up,
    w_down,
    gain_moe,
):
    tok_rows, head_local, head_size = queries.shape
    kv_local = keys.shape[1]
    group_size = head_local // kv_local
    positions = lax.axis_index("sp") * tok_rows + jnp.arange(tok_rows, dtype=jnp.int32)
    cosine_table, sine_table = rope_tables(positions, head_size)
    q_turned = (
        turn(scale_rows(queries.astype(jnp.float32), q_gain), cosine_table, sine_table)
        * head_size ** (-0.5)
    ).astype(jnp.bfloat16)
    k_turned = turn(scale_rows(keys.astype(jnp.float32), k_gain), cosine_table, sine_table).astype(
        jnp.bfloat16
    )
    q_two = q_turned.transpose(1, 0, 2).reshape(kv_local, group_size * tok_rows, head_size)
    kv_two = jnp.stack([k_turned.transpose(1, 0, 2), values.transpose(1, 2, 0)], axis=1)
    mixed_heads = attention(q_two, kv_two)
    tok_part = residual.shape[0]
    width = residual.shape[1]
    projected = sum_at_owner(
        jnp.dot(mixed_heads, w_out, preferred_element_type=jnp.float32).astype(jnp.bfloat16),
        "tp",
        0,
    )
    middle = residual.astype(jnp.float32) + scale_rows(projected, gain_mix)
    normed = scale_rows(middle, gain_pre).astype(jnp.bfloat16)
    disp, mixw = slot_tables(routes, route_weights)
    return experts(
        normed, disp, mixw, middle, gain_moe.reshape(1, width), w_gate[0], w_up[0], w_down[0]
    )


def solution(mesh):
    placed = (
        P("sp", "tp", None),
        P("sp", "tp", None),
        P("sp", "tp", None),
        P(),
        P(),
        P("tp", None),
        P(("sp", "tp"), None),
        P(),
        P(),
        P(("sp", "tp"), None),
        P(("sp", "tp"), None),
        P("sp", None, "tp"),
        P("sp", None, "tp"),
        P("sp", "tp", None),
        P(),
    )
    return jax.shard_map(
        on_device, mesh=mesh, in_specs=placed, out_specs=P(("sp", "tp"), None), check_vma=False
    )
```

```python
import jax
import jax.numpy as jnp
from jax import lax
from jax.experimental import pallas as pl
from jax.experimental.pallas import tpu as pltpu
from jax.sharding import PartitionSpec as P

TOP = 4
GRID_W = 64


norm_eps = 1e-06
rope_theta = 10000.0
clamp_limit = 7.0
swish_alpha = 1.702


def rope_tables(positions, head_size):
    row_index = (positions // GRID_W).astype(jnp.float32)
    col_index = (positions % GRID_W).astype(jnp.float32)
    freq_count = head_size // 4
    inverse = rope_theta ** (-jnp.arange(freq_count, dtype=jnp.float32) / freq_count)
    angles = jnp.stack([row_index[:, None] * inverse, col_index[:, None] * inverse], axis=1)
    return (jnp.cos(angles), jnp.sin(angles))


def turn(array_in, cosine_table, sine_table):
    token_count, head_count, head_size = array_in.shape
    split_field = array_in.reshape(token_count, head_count, 2, 2, head_size // 4)
    first_half = split_field[:, :, :, 0, :]
    second_half = split_field[:, :, :, 1, :]
    cos_wide = cosine_table[:, None]
    sin_wide = sine_table[:, None]
    turned = jnp.stack(
        [
            first_half * cos_wide - second_half * sin_wide,
            second_half * cos_wide + first_half * sin_wide,
        ],
        axis=3,
    )
    return turned.reshape(token_count, head_count, head_size)


def scale_rows(array_in, gain_vec):
    return (
        array_in
        * lax.rsqrt(jnp.mean(array_in * array_in, axis=-1, keepdims=True) + norm_eps)
        * gain_vec
    )


def slot_tables(routes, route_weights):
    core = lax.rem(lax.axis_index("sp"), 2)
    swap = [(i, i ^ 1) for i in range(lax.axis_size("sp"))]
    count = routes.shape[0]
    both = jnp.concatenate([routes.astype(jnp.float32), route_weights], axis=1)
    other = lax.ppermute(both, "sp", swap)
    ordered = jnp.where(core == 0, jnp.stack([both, other]), jnp.stack([other, both]))
    chosen, weights = ordered[:, :, :TOP].astype(jnp.int32), ordered[:, :, TOP:]
    flat = chosen.reshape(2, count * TOP)
    same = (flat[:, :, None] == flat[:, None, :]).astype(jnp.int32)
    place = jnp.arange(count * TOP, dtype=jnp.int32)
    earlier = (place[None, :] < place[:, None]).astype(jnp.int32)
    rank = jnp.sum(same * earlier, axis=2).reshape(2, count, TOP)
    side = jnp.arange(2, dtype=jnp.int32)[:, None, None]
    target = jnp.where(chosen % 2 == core, (chosen // 2) * 8 + side * 4 + rank, -1)
    target, weights = target.reshape(2 * count, TOP), weights.reshape(2 * count, TOP)
    spots = jnp.arange(256, dtype=jnp.int32)
    disp = jnp.sum((target[None, :, :] == spots[:, None, None]).astype(jnp.float32), axis=2)
    mixw = jnp.sum(jnp.where(target[:, None, :] == spots[None, :, None], weights[:, None, :], 0.0), axis=2)
    return disp.astype(jnp.bfloat16), mixw


MESH = pl.DeviceIdType.MESH
NZ, NX = 8, 4
PIECE = 128


def attention_kernel(q_ref, kv_ref, wo_hbm, residual_ref, mix_ref, pre_ref, middle_ref, normed_ref,
                     buf, qbuf, m_ref, l_ref, acc, obuf, heads, wo, pbuf, pin,
                     rsem, qsem, asem, zup, zdn, bup, bdn, bxp, bxm, bfw, dsem, osem, psend, precv, wsem):
    sp = lax.axis_index("sp")
    t = lax.axis_index("tp")
    load = pltpu.make_async_copy(wo_hbm, wo, wsem)
    load.start()
    core = lax.rem(sp, 2)
    chip = lax.div(sp, 2)
    x = lax.rem(chip, NX)
    z = lax.div(chip, NX)

    def dev(zz, xx, cc):
        return {"sp": (lax.rem(zz + 2 * NZ, NZ) * NX + lax.rem(xx + 2 * NX, NX)) * 2 + cc}

    def slot(kind, zz, xx):
        return kind * (NZ * NX) + lax.rem(zz + 2 * NZ, NZ) * NX + lax.rem(xx + 2 * NX, NX)

    partner = dev(z, x, 1 - core)
    z_up, z_dn = dev(z + 1, x, core), dev(z - 1, x, core)
    x_up, x_dn, x_far = dev(z, x + 1, core), dev(z, x - 1, core), dev(z, x + 2, core)

    mine = core * (NZ * NX) + chip
    buf[mine] = kv_ref[core]
    qbuf[pl.ds(pl.multiple_of(core * 512, 512), 512), :] = q_ref[core]
    m_ref[...] = jnp.full(m_ref.shape, -jnp.inf, jnp.float32)
    l_ref[...] = jnp.zeros(l_ref.shape, jnp.float32)
    acc[...] = jnp.zeros(acc.shape, jnp.float32)

    barrier = pltpu.get_barrier_semaphore()
    tp_peers = [lax.rem(t + d, 4) for d in (2, 1, 3)]
    for peer in (partner, z_up, z_dn, x_up, x_dn, x_far, *({"tp": p} for p in tp_peers)):
        pl.semaphore_signal(barrier, inc=1, device_id=peer, device_id_type=MESH)
    pl.semaphore_wait(barrier, 9)

    def move(at, sem, to):
        return pltpu.make_async_remote_copy(
            src_ref=buf.at[at], dst_ref=buf.at[at], send_sem=sem, recv_sem=rsem.at[at], device_id=to, device_id_type=MESH
        )

    def send(at, sem, to):
        move(at, sem, to).start()

    def arrive(at):
        move(at, dsem.at[0], partner).wait_recv()

    def done(sem):
        move(0, sem, partner).wait_send()

    swap_kv = pltpu.make_async_remote_copy(
        src_ref=kv_ref.at[1 - core], dst_ref=buf.at[(1 - core) * 0 + core * (NZ * NX) + chip], send_sem=dsem.at[0],
        recv_sem=rsem.at[core * (NZ * NX) + chip], device_id=partner, device_id_type=MESH,
    )
    swap_q = pltpu.make_async_remote_copy(
        src_ref=q_ref.at[1 - core], dst_ref=qbuf.at[pl.ds(pl.multiple_of(core * 512, 512), 512), :], send_sem=dsem.at[1],
        recv_sem=qsem, device_id=partner, device_id_type=MESH,
    )
    swap_kv.start()
    swap_q.start()
    arrive((1 - core) * (NZ * NX) + chip)

    def attend(slots):
        keys = jnp.concatenate([buf[s, 0] for s in slots], axis=0)
        vals = jnp.concatenate([buf[s, 1] for s in slots], axis=1)
        for tile in range(4):
            cols = slice(tile * 256, tile * 256 + 256)
            scores = lax.dot_general(keys, qbuf[cols, :], (((1,), (1,)), ((), ())), preferred_element_type=jnp.float32)
            before = m_ref[:, cols]
            now = jnp.maximum(before, jnp.max(scores, axis=0, keepdims=True))
            shrink = jnp.exp(before - now)
            unnorm = jnp.exp(scores - now)
            l_ref[:, cols] = l_ref[:, cols] * shrink + jnp.sum(unnorm, axis=0, keepdims=True)
            acc[:, cols] = acc[:, cols] * shrink + jnp.dot(
                vals, unnorm.astype(jnp.bfloat16), preferred_element_type=jnp.float32
            )
            m_ref[:, cols] = now

    A, B = 0, 1
    own_a, own_b = slot(A, z, x), slot(B, z, x)
    send(own_b, bup.at[0], z_up)
    send(own_b, bdn.at[0], z_dn)
    send(own_a, asem.at[0], x_up)
    send(own_a, asem.at[1], x_dn)
    send(own_a, zup.at[0], z_up)
    send(own_a, zdn.at[0], z_dn)
    send(own_a, asem.at[2], x_far)
    send(own_b, bxp.at[0], x_up)
    send(own_b, bxm.at[0], x_dn)
    ready = [own_a, own_b]

    def work(least=4):
        if len(ready) >= least:
            group = ready[:4]
            del ready[:4]
            attend(group)

    def lines_b(r):
        lo, hi = slot(B, z - r, x), slot(B, z + r, x)
        arrive(lo)
        if r < 4:
            send(lo, bup.at[r], z_up)
        send(lo, bxp.at[2 * r - 1], x_up)
        send(lo, bxm.at[2 * r - 1], x_dn)
        ready.append(lo)
        if r < 4:
            arrive(hi)
            if r < 3:
                send(hi, bdn.at[r], z_dn)
            send(hi, bxp.at[2 * r], x_up)
            send(hi, bxm.at[2 * r], x_dn)
            ready.append(hi)

    def lines_a(r, j):
        lo, hi = slot(A, z - r, x + j), slot(A, z + r, x + j)
        arrive(lo)
        if r < 3 or (r == 3 and j in (0, 1)):
            send(lo, zup.at[r * 4 + j], z_up)
        if 0 < r < 4:
            ready.append(lo)
            arrive(hi)
        if r < 3 or (r == 3 and j in (2, 3)):
            send(hi, zdn.at[r * 4 + j], z_dn)
        ready.append(hi)

    def across(r):
        if r > 0:
            at = slot(B, z - r, x - 1)
            arrive(at)
            send(at, bfw.at[2 * r - 1], x_up)
            ready.append(at)
        if r < 4:
            at = slot(B, z + r, x + 1)
            arrive(at)
            send(at, bfw.at[2 * r], x_dn)
            ready.append(at)
        if r > 0:
            at = slot(B, z - r, x + 1)
            arrive(at)
            ready.append(at)
        if r < 4:
            at = slot(B, z + r, x - 1)
            arrive(at)
            ready.append(at)

    def far(r):
        for at in {0: [slot(B, z, x + 2)], 4: [slot(B, z + 4, x + 2)]}.get(r, [slot(B, z - r, x + 2), slot(B, z + r, x + 2)]):
            arrive(at)
            ready.append(at)

    lines_a(0, 1)
    lines_a(0, 3)
    lines_a(0, 2)
    swap_q.wait_recv()
    for r in range(1, 5):
        lines_b(r)
        work()
        lines_a(r, 0)
        work()
        lines_a(r, 1)
        work()
        across(r - 1)
        work()
        lines_a(r, 3)
        work()
        lines_a(r, 2)
        work()
        if r > 1:
            far(r - 2)
        work()
    across(4)
    work()
    far(3)
    work()
    far(4)
    while ready:
        work(1)

    def heads_of(which):
        cols = pl.ds(pl.multiple_of(which * 512, 512), 512)
        return (acc[:, cols] / l_ref[:, cols]).astype(jnp.bfloat16)

    theirs = heads_of(1 - core)
    obuf[2] = theirs
    own = heads_of(core)
    obuf[core] = own
    swap_o = pltpu.make_async_remote_copy(
        src_ref=obuf.at[2], dst_ref=obuf.at[core], send_sem=osem.at[0], recv_sem=osem.at[1], device_id=partner, device_id_type=MESH
    )
    swap_o.start()

    def stack_heads(g):
        for h in range(4):
            cols = pl.ds(pl.multiple_of(g * 512 + h * 128, 128), 128)
            heads[:, cols] = obuf[g, :, h * 128 : h * 128 + 128].T

    stack_heads(core)
    load.wait()
    swap_o.wait()
    stack_heads(1 - core)
    for cut in range(4):
        cols = slice(cut * 512, cut * 512 + 512)
        part = jnp.dot(heads[...], wo[:, cols], preferred_element_type=jnp.float32).astype(jnp.bfloat16)
        for owner in range(4):
            pbuf[owner, :, cols] = part[owner * 32 : owner * 32 + 32]
    gives = [
        pltpu.make_async_remote_copy(
            src_ref=pbuf.at[peer], dst_ref=pin.at[i], send_sem=psend.at[i], recv_sem=precv.at[i], device_id={"tp": peer},
            device_id_type=MESH,
        )
        for i, peer in enumerate(tp_peers)
    ]
    for give in gives:
        give.start()
    for i in range(3):
        done(asem.at[i])
    for i in range(4):
        done(bup.at[i])
        for j in range(4):
            if i < 3 or j in (0, 1):
                done(zup.at[i * 4 + j])
            if i < 3 or j in (2, 3):
                done(zdn.at[i * 4 + j])
    for i in range(3):
        done(bdn.at[i])
    for i in range(8):
        done(bxp.at[i])
        done(bxm.at[i])
        done(bfw.at[i])
    swap_kv.wait_send()
    swap_q.wait_send()
    for give in gives:
        give.wait()
    projected = pbuf[t].astype(jnp.float32)
    for i in range(3):
        projected = projected + pin[i].astype(jnp.float32)
    middle = residual_ref[...].astype(jnp.float32) + scale_rows(projected, mix_ref[...])
    middle_ref[...] = middle
    normed_ref[...] = scale_rows(middle, pre_ref[...]).astype(jnp.bfloat16)


def attention(q_two, kv_two, w_out, residual, gain_mix, gain_pre):
    whole, apart = pl.BlockSpec(memory_space=pltpu.VMEM), pl.BlockSpec(memory_space=pl.ANY)
    return pl.pallas_call(
        attention_kernel,
        out_shape=[jax.ShapeDtypeStruct((32, 2048), jnp.float32), jax.ShapeDtypeStruct((32, 2048), jnp.bfloat16)],
        in_specs=[whole, whole, apart, whole, whole, whole],
        out_specs=[whole, whole],
        scratch_shapes=[
            pltpu.VMEM((64, 2, PIECE, 128), jnp.bfloat16),
            pltpu.VMEM((1024, 128), jnp.bfloat16),
            pltpu.VMEM((1, 1024), jnp.float32),
            pltpu.VMEM((1, 1024), jnp.float32),
            pltpu.VMEM((128, 1024), jnp.float32),
            pltpu.VMEM((3, 128, 512), jnp.bfloat16),
            pltpu.VMEM((128, 1024), jnp.bfloat16),
            pltpu.VMEM((1024, 2048), jnp.bfloat16),
            pltpu.VMEM((4, 32, 2048), jnp.bfloat16),
            pltpu.VMEM((3, 32, 2048), jnp.bfloat16),
            pltpu.SemaphoreType.DMA((64,)),
            pltpu.SemaphoreType.DMA,
            pltpu.SemaphoreType.DMA((3,)),
            pltpu.SemaphoreType.DMA((16,)),
            pltpu.SemaphoreType.DMA((16,)),
            pltpu.SemaphoreType.DMA((4,)),
            pltpu.SemaphoreType.DMA((4,)),
            pltpu.SemaphoreType.DMA((8,)),
            pltpu.SemaphoreType.DMA((8,)),
            pltpu.SemaphoreType.DMA((8,)),
            pltpu.SemaphoreType.DMA((2,)),
            pltpu.SemaphoreType.DMA((2,)),
            pltpu.SemaphoreType.DMA((3,)),
            pltpu.SemaphoreType.DMA((3,)),
            pltpu.SemaphoreType.DMA,
        ],
        compiler_params=pltpu.CompilerParams(collective_id=0, has_side_effects=True, vmem_limit_bytes=40 << 20),
        cost_estimate=pl.CostEstimate(flops=4 * 1024 * 8192 * 128, bytes_accessed=1 << 20, transcendentals=1024 * 8192),
        name="gather_attention",
    )(q_two, kv_two, w_out, residual, gain_mix, gain_pre)


GROUP_ORDER = (0, 1, 7, 2, 6, 3, 5, 4)
VIA_UP = (3, 6, 1, 0)
VIA_DN = (4, 5, 2, 7)


def experts_kernel(normed_ref, disp_ref, mixw_ref, middle_ref, gain_ref, wg_hbm, wu_hbm, wd_hbm, out_ref,
                   both, msgs, rows, act, part, mid, fin, ret, mixs, wg, wu, wd,
                   wsem, msend, mrecv, gup, gdn, gfw, grecv, s_first, s_direct, s_mid, midrecv, finrecv, rsend, rrecv, nsem, xsem):
    sp = lax.axis_index("sp")
    t = lax.axis_index("tp")
    core = lax.rem(sp, 2)
    chip = lax.div(sp, 2)
    x = lax.rem(chip, NX)
    z = lax.div(chip, NX)
    t_up, t_dn, t_far = lax.rem(t + 1, 4), lax.rem(t + 3, 4), lax.rem(t + 2, 4)

    def chip_at(dz, dx):
        return lax.rem(z + dz, NZ) * NX + lax.rem(x + dx, NX)

    def plane(which):
        return {"sp": which * 2 + core}

    partner = {"sp": chip * 2 + 1 - core}
    up, dn = {"tp": t_up}, {"tp": t_dn}

    loads = [
        pltpu.make_async_copy(wg_hbm, wg, wsem.at[0]),
        pltpu.make_async_copy(wu_hbm, wu, wsem.at[1]),
        pltpu.make_async_copy(wd_hbm, wd, wsem.at[2]),
    ]
    for load in loads:
        load.start()
    both[core] = normed_ref[...]

    barrier = pltpu.get_barrier_semaphore()
    for peer in (partner, up, dn):
        pl.semaphore_signal(barrier, inc=1, device_id=peer, device_id_type=MESH)
    others = [(dz, dx) for dz in GROUP_ORDER for dx in (0, 1, 3, 2) if (dz, dx) != (0, 0)]
    for dz, dx in others:
        pl.semaphore_signal(barrier, inc=1, device_id=plane(chip_at(dz, dx)), device_id_type=MESH)
    pl.semaphore_wait(barrier, 3 + len(others))

    def remote(src, dst, send_sem, recv_sem, to):
        return pltpu.make_async_remote_copy(
            src_ref=src, dst_ref=dst, send_sem=send_sem, recv_sem=recv_sem, device_id=to, device_id_type=MESH
        )

    swap = remote(normed_ref, both.at[core], nsem.at[0], nsem.at[1], partner)
    swap.start()
    swap.wait()
    tokens = jnp.concatenate([both[0], both[1]], axis=0)
    for cut in range(4):
        cols = slice(cut * 512, cut * 512 + 512)
        msgs[:, :, cols] = (
            jnp.dot(disp_ref[...], tokens[:, cols], preferred_element_type=jnp.float32)
            .astype(jnp.bfloat16)
            .reshape(32, 8, 512)
        )

    for dz, dx in others:
        to = chip_at(dz, dx)
        remote(msgs.at[to], rows.at[t, chip], msend.at[to], mrecv.at[chip], plane(to)).start()
    rows[t, chip] = msgs[chip]

    def chunk_at(which, dz):
        first = lax.rem(z + NZ - dz, NZ) * NX
        return rows.at[which, pl.ds(first, NX)]

    def give(dz, sem, to):
        ref = chunk_at(t, dz)
        return remote(ref, ref, sem, grecv.at[t * 8 + dz], to)

    def take(which, dz):
        ref = chunk_at(which, dz)
        remote(ref, ref, gup.at[0], grecv.at[which * 8 + dz], up).wait_recv()

    def hand(which, dz, to):
        ref = chunk_at(which, dz)
        return remote(ref, ref, gfw.at[dz], grecv.at[which * 8 + dz], to)

    def relay(dz):
        take(t_dn, dz)
        if dz in VIA_UP:
            hand(t_dn, dz, up).start()
        take(t_up, dz)
        if dz in VIA_DN:
            hand(t_up, dz, dn).start()

    for i, dz in enumerate(GROUP_ORDER):
        for dx in (0, 1, 3, 2):
            if (dz, dx) != (0, 0):
                source = chip_at(NZ - dz, dx)
                remote(msgs.at[0], rows.at[t, source], msend.at[0], mrecv.at[source], partner).wait_recv()
        give(dz, gup.at[dz], up).start()
        give(dz, gdn.at[dz], dn).start()
        if i > 0:
            relay(GROUP_ORDER[i - 1])
    for load in loads:
        load.wait()

    def serve(which):
        data = rows[which].reshape(256, 2048)
        for f in range(2):
            cols = slice(f * 256, f * 256 + 256)
            gate = jnp.minimum(jnp.dot(data, wg[:, cols], preferred_element_type=jnp.float32), clamp_limit)
            lift = jnp.clip(jnp.dot(data, wu[:, cols], preferred_element_type=jnp.float32), -clamp_limit, clamp_limit)
            act[:, cols] = (gate * jax.nn.sigmoid(swish_alpha * gate) * (lift + 1.0)).astype(jnp.bfloat16)
        for cut in range(8):
            cols = slice(cut * 256, cut * 256 + 256)
            part[which, :, :, cols] = (
                jnp.dot(act[...], wd[:, cols], preferred_element_type=jnp.float32).astype(jnp.bfloat16).reshape(32, 8, 256)
            )

    def group(dz):
        return pl.ds(lax.rem(z + NZ - dz, NZ) * NX, NX)

    serve(t)
    relay(GROUP_ORDER[-1])

    def direct(k):
        a, b = group(VIA_DN[k]), group(VIA_UP[k])
        remote(part.at[t_up, a], fin.at[0, a], s_direct.at[k], finrecv.at[VIA_DN[k]], up).start()
        remote(part.at[t_dn, b], fin.at[1, b], s_direct.at[4 + k], finrecv.at[8 + VIA_UP[k]], dn).start()

    def first(k):
        a, b = group(VIA_UP[k]), group(VIA_DN[k])
        remote(part.at[t_far, a], mid.at[0, k], s_first.at[k], midrecv.at[k], up).start()
        remote(part.at[t_far, b], mid.at[1, k], s_first.at[4 + k], midrecv.at[4 + k], dn).start()

    def middle_sum(k):
        for way, (dzs, owner, to) in enumerate(((VIA_UP, t_up, up), (VIA_DN, t_dn, dn))):
            where = group(dzs[k])
            remote(part.at[owner, where], mid.at[way, k], s_first.at[0], midrecv.at[way * 4 + k], up).wait_recv()
            total = part[owner, where].astype(jnp.float32) + mid[way, k].astype(jnp.float32)
            part[owner, where] = total.astype(jnp.bfloat16)
            remote(part.at[owner, where], fin.at[way, where], s_mid.at[way * 4 + k], finrecv.at[way * 8 + dzs[k]], to).start()

    def settle(k):
        for dz in (VIA_UP[k], VIA_DN[k]):
            where = group(dz)
            for way in range(2):
                remote(part.at[t, where], fin.at[way, where], s_first.at[0], finrecv.at[way * 8 + dz], up).wait_recv()
            total = part[t, where].astype(jnp.float32) + fin[0, where].astype(jnp.float32) + fin[1, where].astype(jnp.float32)
            part[t, where] = total.astype(jnp.bfloat16)
            for dx in (2, 1, 3, 0):
                to = chip_at(NZ - dz, dx)
                if (dz, dx) != (0, 0):
                    remote(part.at[t, to], ret.at[chip], rsend.at[to], rrecv.at[chip], plane(to)).start()

    serve(t_up)
    serve(t_dn)
    direct(0)
    for dz in GROUP_ORDER:
        take(t_far, dz)
    serve(t_far)
    first(0)
    first(1)
    middle_sum(0)
    direct(1)
    first(2)
    middle_sum(1)
    settle(0)
    direct(2)
    first(3)
    middle_sum(2)
    settle(1)
    direct(3)
    middle_sum(3)
    settle(2)
    settle(3)
    ret[chip] = part[t, chip]
    for dz, dx in others:
        source = chip_at(dz, dx)
        remote(part.at[t, 0], ret.at[source], rsend.at[0], rrecv.at[source], partner).wait_recv()
    weight = mixw_ref[...]
    coarse = weight.astype(jnp.bfloat16)
    fine = (weight - coarse.astype(jnp.float32)).astype(jnp.bfloat16)
    for cut in range(4):
        cols = slice(cut * 512, cut * 512 + 512)
        came = ret[:, :, cols].reshape(256, 512)
        mixed = jnp.dot(coarse, came, preferred_element_type=jnp.float32) + jnp.dot(
            fine, came, preferred_element_type=jnp.float32
        )
        mixs[0, :, cols] = mixed[:32]
        mixs[1, :, cols] = mixed[32:]
    swap_mix = remote(mixs.at[1 - core], mixs.at[2], xsem.at[0], xsem.at[1], partner)
    swap_mix.start()

    def sent(src, sem):
        remote(src, src, sem, nsem.at[1], partner).wait_send()

    for dz, dx in others:
        to = chip_at(dz, dx)
        sent(msgs.at[0], msend.at[to])
        sent(msgs.at[0], rsend.at[to])
    for i in range(8):
        for sems in (gup, gdn, gfw, s_first, s_direct, s_mid):
            sent(mid.at[0, 0], sems.at[i])
    swap_mix.wait()
    mixture = mixs[core] + mixs[2]
    scale = lax.rsqrt(jnp.mean(mixture * mixture, axis=-1, keepdims=True) + norm_eps)
    out_ref[...] = (middle_ref[...] + mixture * scale * gain_ref[...]).astype(jnp.bfloat16)


def experts(normed, disp, mixw, middle, gain, w_gate, w_up, w_down):
    whole, remote = pl.BlockSpec(memory_space=pltpu.VMEM), pl.BlockSpec(memory_space=pl.ANY)
    dma = pltpu.SemaphoreType.DMA
    return pl.pallas_call(
        experts_kernel,
        out_shape=jax.ShapeDtypeStruct((32, 2048), jnp.bfloat16),
        in_specs=[whole] * 5 + [remote] * 3,
        out_specs=whole,
        scratch_shapes=[
            pltpu.VMEM((2, 32, 2048), jnp.bfloat16),
            pltpu.VMEM((32, 8, 2048), jnp.bfloat16),
            pltpu.VMEM((4, 32, 8, 2048), jnp.bfloat16),
            pltpu.VMEM((256, 512), jnp.bfloat16),
            pltpu.VMEM((4, 32, 8, 2048), jnp.bfloat16),
            pltpu.VMEM((2, 4, 4, 8, 2048), jnp.bfloat16),
            pltpu.VMEM((2, 32, 8, 2048), jnp.bfloat16),
            pltpu.VMEM((32, 8, 2048), jnp.bfloat16),
            pltpu.VMEM((3, 32, 2048), jnp.float32),
            pltpu.VMEM((2048, 512), jnp.bfloat16),
            pltpu.VMEM((2048, 512), jnp.bfloat16),
            pltpu.VMEM((512, 2048), jnp.bfloat16),
            dma((3,)),
            dma((32,)),
            dma((32,)),
            dma((8,)),
            dma((8,)),
            dma((8,)),
            dma((32,)),
            dma((8,)),
            dma((8,)),
            dma((8,)),
            dma((8,)),
            dma((16,)),
            dma((32,)),
            dma((32,)),
            dma((2,)),
            dma((2,)),
        ],
        compiler_params=pltpu.CompilerParams(collective_id=1, has_side_effects=True, vmem_limit_bytes=48 << 20),
        cost_estimate=pl.CostEstimate(flops=6 * 1024 * 2048 * 512, bytes_accessed=8 << 20, transcendentals=1024 * 512),
        name="experts",
    )(normed, disp, mixw, middle, gain, w_gate, w_up, w_down)


def on_device(
    queries,
    keys,
    values,
    q_gain,
    k_gain,
    w_out,
    residual,
    gain_mix,
    gain_pre,
    routes,
    route_weights,
    w_gate,
    w_up,
    w_down,
    gain_moe,
):
    tok_rows, head_local, head_size = queries.shape
    kv_local = keys.shape[1]
    group_size = head_local // kv_local
    positions = lax.axis_index("sp") * tok_rows + jnp.arange(tok_rows, dtype=jnp.int32)
    cosine_table, sine_table = rope_tables(positions, head_size)
    q_turned = (
        turn(scale_rows(queries.astype(jnp.float32), q_gain), cosine_table, sine_table)
        * head_size ** (-0.5)
    ).astype(jnp.bfloat16)
    k_turned = turn(scale_rows(keys.astype(jnp.float32), k_gain), cosine_table, sine_table).astype(
        jnp.bfloat16
    )
    q_two = q_turned.transpose(1, 0, 2).reshape(kv_local, group_size * tok_rows, head_size)
    kv_two = jnp.stack([k_turned.transpose(1, 0, 2), values.transpose(1, 2, 0)], axis=1)
    width = residual.shape[1]
    middle, normed = attention(
        q_two, kv_two, w_out, residual, gain_mix.reshape(1, width), gain_pre.reshape(1, width)
    )
    disp, mixw = slot_tables(routes, route_weights)
    return experts(
        normed, disp, mixw, middle, gain_moe.reshape(1, width), w_gate[0], w_up[0], w_down[0]
    )


def solution(mesh):
    placed = (
        P("sp", "tp", None),
        P("sp", "tp", None),
        P("sp", "tp", None),
        P(),
        P(),
        P("tp", None),
        P(("sp", "tp"), None),
        P(),
        P(),
        P(("sp", "tp"), None),
        P(("sp", "tp"), None),
        P("sp", None, "tp"),
        P("sp", None, "tp"),
        P("sp", "tp", None),
        P(),
    )
    return jax.shard_map(
        on_device, mesh=mesh, in_specs=placed, out_specs=P(("sp", "tp"), None), check_vma=False
    )
```

```python
import jax
import jax.numpy as jnp
from jax import lax
from jax.experimental import pallas as pl
from jax.experimental.pallas import tpu as pltpu
from jax.sharding import PartitionSpec as P

TOP = 4
GRID_W = 64


norm_eps = 1e-06
rope_theta = 10000.0
clamp_limit = 7.0
swish_alpha = 1.702


def rope_tables(positions, head_size):
    row_index = (positions // GRID_W).astype(jnp.float32)
    col_index = (positions % GRID_W).astype(jnp.float32)
    freq_count = head_size // 4
    inverse = rope_theta ** (-jnp.arange(freq_count, dtype=jnp.float32) / freq_count)
    angles = jnp.stack([row_index[:, None] * inverse, col_index[:, None] * inverse], axis=1)
    return (jnp.cos(angles), jnp.sin(angles))


def turn(array_in, cosine_table, sine_table):
    token_count, head_count, head_size = array_in.shape
    split_field = array_in.reshape(token_count, head_count, 2, 2, head_size // 4)
    first_half = split_field[:, :, :, 0, :]
    second_half = split_field[:, :, :, 1, :]
    cos_wide = cosine_table[:, None]
    sin_wide = sine_table[:, None]
    turned = jnp.stack(
        [
            first_half * cos_wide - second_half * sin_wide,
            second_half * cos_wide + first_half * sin_wide,
        ],
        axis=3,
    )
    return turned.reshape(token_count, head_count, head_size)


def scale_rows(array_in, gain_vec):
    return (
        array_in
        * lax.rsqrt(jnp.mean(array_in * array_in, axis=-1, keepdims=True) + norm_eps)
        * gain_vec
    )


def route_info(routes, route_weights):
    core = lax.rem(lax.axis_index("sp"), 2)
    count = routes.shape[0]
    flat = routes.reshape(-1)
    place = jnp.arange(count * TOP, dtype=jnp.int32)
    earlier = (flat[:, None] == flat[None, :]) & (place[None, :] < place[:, None])
    rank = jnp.sum(earlier.astype(jnp.int32), axis=1)
    slots = (flat * 4 + rank).reshape(count, TOP).astype(jnp.float32)
    info = jnp.concatenate([slots.T, route_weights.T], axis=0)
    side = jnp.arange(128 // count, dtype=jnp.int32)[None, :, None]
    return jnp.where(side == core, info[:, None, :], 0.0).reshape(2 * TOP, 128)


MESH = pl.DeviceIdType.MESH
NZ, NX = 8, 4
PIECE = 128


def attention_part(q_ref, kv_ref, wo_hbm, residual_ref, mix_ref, pre_ref, middle_ref, normed_ref, meet,
                     buf, qbuf, m_ref, l_ref, acc, obuf, heads, wo, pbuf, pin,
                     rsem, qsem, asem, zup, zdn, bup, bdn, bxp, bxm, bfw, dsem, osem, psend, precv, wsem):
    sp = lax.axis_index("sp")
    t = lax.axis_index("tp")
    load = pltpu.make_async_copy(wo_hbm, wo, wsem)
    load.start()
    core = lax.rem(sp, 2)
    chip = lax.div(sp, 2)
    x = lax.rem(chip, NX)
    z = lax.div(chip, NX)

    def dev(zz, xx, cc):
        return {"sp": (lax.rem(zz + 2 * NZ, NZ) * NX + lax.rem(xx + 2 * NX, NX)) * 2 + cc}

    def slot(kind, zz, xx):
        return kind * (NZ * NX) + lax.rem(zz + 2 * NZ, NZ) * NX + lax.rem(xx + 2 * NX, NX)

    partner = dev(z, x, 1 - core)
    z_up, z_dn = dev(z + 1, x, core), dev(z - 1, x, core)
    x_up, x_dn, x_far = dev(z, x + 1, core), dev(z, x - 1, core), dev(z, x + 2, core)

    mine = core * (NZ * NX) + chip
    buf[mine] = kv_ref[core]
    qbuf[pl.ds(pl.multiple_of(core * 512, 512), 512), :] = q_ref[core]
    m_ref[...] = jnp.full(m_ref.shape, -jnp.inf, jnp.float32)
    l_ref[...] = jnp.zeros(l_ref.shape, jnp.float32)
    acc[...] = jnp.zeros(acc.shape, jnp.float32)

    tp_peers = [lax.rem(t + d, 4) for d in (2, 1, 3)]
    meet()

    def move(at, sem, to):
        return pltpu.make_async_remote_copy(
            src_ref=buf.at[at], dst_ref=buf.at[at], send_sem=sem, recv_sem=rsem.at[at], device_id=to, device_id_type=MESH
        )

    def send(at, sem, to):
        move(at, sem, to).start()

    def arrive(at):
        move(at, dsem.at[0], partner).wait_recv()

    def done(sem):
        move(0, sem, partner).wait_send()

    swap_kv = pltpu.make_async_remote_copy(
        src_ref=kv_ref.at[1 - core], dst_ref=buf.at[(1 - core) * 0 + core * (NZ * NX) + chip], send_sem=dsem.at[0],
        recv_sem=rsem.at[core * (NZ * NX) + chip], device_id=partner, device_id_type=MESH,
    )
    swap_q = pltpu.make_async_remote_copy(
        src_ref=q_ref.at[1 - core], dst_ref=qbuf.at[pl.ds(pl.multiple_of(core * 512, 512), 512), :], send_sem=dsem.at[1],
        recv_sem=qsem, device_id=partner, device_id_type=MESH,
    )
    swap_kv.start()
    swap_q.start()
    arrive((1 - core) * (NZ * NX) + chip)

    def attend(slots):
        keys = jnp.concatenate([buf[s, 0] for s in slots], axis=0)
        vals = jnp.concatenate([buf[s, 1] for s in slots], axis=1)
        for tile in range(4):
            cols = slice(tile * 256, tile * 256 + 256)
            scores = lax.dot_general(keys, qbuf[cols, :], (((1,), (1,)), ((), ())), preferred_element_type=jnp.float32)
            before = m_ref[:, cols]
            now = jnp.maximum(before, jnp.max(scores, axis=0, keepdims=True))
            shrink = jnp.exp(before - now)
            unnorm = jnp.exp(scores - now)
            l_ref[:, cols] = l_ref[:, cols] * shrink + jnp.sum(unnorm, axis=0, keepdims=True)
            acc[:, cols] = acc[:, cols] * shrink + jnp.dot(
                vals, unnorm.astype(jnp.bfloat16), preferred_element_type=jnp.float32
            )
            m_ref[:, cols] = now

    A, B = 0, 1
    own_a, own_b = slot(A, z, x), slot(B, z, x)
    send(own_b, bup.at[0], z_up)
    send(own_b, bdn.at[0], z_dn)
    send(own_a, asem.at[0], x_up)
    send(own_a, asem.at[1], x_dn)
    send(own_a, zup.at[0], z_up)
    send(own_a, zdn.at[0], z_dn)
    send(own_a, asem.at[2], x_far)
    send(own_b, bxp.at[0], x_up)
    send(own_b, bxm.at[0], x_dn)
    ready = [own_a, own_b]

    def work(least=4):
        if len(ready) >= least:
            group = ready[:4]
            del ready[:4]
            attend(group)

    def lines_b(r):
        lo, hi = slot(B, z - r, x), slot(B, z + r, x)
        arrive(lo)
        if r < 4:
            send(lo, bup.at[r], z_up)
        send(lo, bxp.at[2 * r - 1], x_up)
        send(lo, bxm.at[2 * r - 1], x_dn)
        ready.append(lo)
        if r < 4:
            arrive(hi)
            if r < 3:
                send(hi, bdn.at[r], z_dn)
            send(hi, bxp.at[2 * r], x_up)
            send(hi, bxm.at[2 * r], x_dn)
            ready.append(hi)

    def lines_a(r, j):
        lo, hi = slot(A, z - r, x + j), slot(A, z + r, x + j)
        arrive(lo)
        if r < 3 or (r == 3 and j in (0, 1)):
            send(lo, zup.at[r * 4 + j], z_up)
        if 0 < r < 4:
            ready.append(lo)
            arrive(hi)
        if r < 3 or (r == 3 and j in (2, 3)):
            send(hi, zdn.at[r * 4 + j], z_dn)
        ready.append(hi)

    def across(r):
        if r > 0:
            at = slot(B, z - r, x - 1)
            arrive(at)
            send(at, bfw.at[2 * r - 1], x_up)
            ready.append(at)
        if r < 4:
            at = slot(B, z + r, x + 1)
            arrive(at)
            send(at, bfw.at[2 * r], x_dn)
            ready.append(at)
        if r > 0:
            at = slot(B, z - r, x + 1)
            arrive(at)
            ready.append(at)
        if r < 4:
            at = slot(B, z + r, x - 1)
            arrive(at)
            ready.append(at)

    def far(r):
        for at in {0: [slot(B, z, x + 2)], 4: [slot(B, z + 4, x + 2)]}.get(r, [slot(B, z - r, x + 2), slot(B, z + r, x + 2)]):
            arrive(at)
            ready.append(at)

    lines_a(0, 1)
    lines_a(0, 3)
    lines_a(0, 2)
    swap_q.wait_recv()
    for r in range(1, 5):
        lines_b(r)
        work()
        lines_a(r, 0)
        work()
        lines_a(r, 1)
        work()
        across(r - 1)
        work()
        lines_a(r, 3)
        work()
        lines_a(r, 2)
        work()
        if r > 1:
            far(r - 2)
        work()
    across(4)
    work()
    far(3)
    work()
    far(4)
    while ready:
        work(1)

    def heads_of(which):
        cols = pl.ds(pl.multiple_of(which * 512, 512), 512)
        return (acc[:, cols] / l_ref[:, cols]).astype(jnp.bfloat16)

    theirs = heads_of(1 - core)
    obuf[2] = theirs
    own = heads_of(core)
    obuf[core] = own
    swap_o = pltpu.make_async_remote_copy(
        src_ref=obuf.at[2], dst_ref=obuf.at[core], send_sem=osem.at[0], recv_sem=osem.at[1], device_id=partner, device_id_type=MESH
    )
    swap_o.start()

    def stack_heads(g):
        for h in range(4):
            cols = pl.ds(pl.multiple_of(g * 512 + h * 128, 128), 128)
            heads[:, cols] = obuf[g, :, h * 128 : h * 128 + 128].T

    stack_heads(core)
    load.wait()
    swap_o.wait()
    stack_heads(1 - core)
    for cut in range(4):
        cols = slice(cut * 512, cut * 512 + 512)
        part = jnp.dot(heads[...], wo[:, cols], preferred_element_type=jnp.float32).astype(jnp.bfloat16)
        for owner in range(4):
            pbuf[owner, :, cols] = part[owner * 32 : owner * 32 + 32]
    gives = [
        pltpu.make_async_remote_copy(
            src_ref=pbuf.at[peer], dst_ref=pin.at[i], send_sem=psend.at[i], recv_sem=precv.at[i], device_id={"tp": peer},
            device_id_type=MESH,
        )
        for i, peer in enumerate(tp_peers)
    ]
    for give in gives:
        give.start()
    for i in range(3):
        done(asem.at[i])
    for i in range(4):
        done(bup.at[i])
        for j in range(4):
            if i < 3 or j in (0, 1):
                done(zup.at[i * 4 + j])
            if i < 3 or j in (2, 3):
                done(zdn.at[i * 4 + j])
    for i in range(3):
        done(bdn.at[i])
    for i in range(8):
        done(bxp.at[i])
        done(bxm.at[i])
        done(bfw.at[i])
    swap_kv.wait_send()
    swap_q.wait_send()
    for give in gives:
        give.wait()
    projected = pbuf[t].astype(jnp.float32)
    for i in range(3):
        projected = projected + pin[i].astype(jnp.float32)
    middle = residual_ref[...].astype(jnp.float32) + scale_rows(projected, mix_ref[...])
    middle_ref[...] = middle
    normed_ref[...] = scale_rows(middle, pre_ref[...]).astype(jnp.bfloat16)


GROUP_ORDER = (0, 1, 7, 2, 6, 3, 5, 4)
VIA_UP = (3, 6, 1, 0)
VIA_DN = (4, 5, 2, 7)


def experts_part(normed_ref, info_ref, middle_ref, gain_ref, loads, out_ref, others, column,
                 toks, infos, msgs, rows, act, part, mid, fin, ret, mixs, wg, wu, wd,
                   isend, irecv, tsend, trecv, msend, mrecv, gup, gdn, gfw, grecv, s_first, s_direct, s_mid, midrecv, finrecv,
                   rsend, rrecv, xsem):
    sp = lax.axis_index("sp")
    t = lax.axis_index("tp")
    core = lax.rem(sp, 2)
    chip = lax.div(sp, 2)
    x = lax.rem(chip, NX)
    z = lax.div(chip, NX)
    t_up, t_dn, t_far = lax.rem(t + 1, 4), lax.rem(t + 3, 4), lax.rem(t + 2, 4)

    def chip_at(dz, dx):
        return lax.rem(z + dz, NZ) * NX + lax.rem(x + dx, NX)

    def plane(which):
        return {"sp": which * 2 + core}

    partner = {"sp": chip * 2 + 1 - core}
    up, dn = {"tp": t_up}, {"tp": t_dn}

    toks[z, core] = normed_ref[...]
    infos[z, core] = info_ref[...]

    column = [{"sp": to} for to in column]

    def remote(src, dst, send_sem, recv_sem, to):
        return pltpu.make_async_remote_copy(
            src_ref=src, dst_ref=dst, send_sem=send_sem, recv_sem=recv_sem, device_id=to, device_id_type=MESH
        )

    z_up, z_dn = plane(chip_at(1, 0)), plane(chip_at(NZ - 1, 0))
    for i, to in enumerate((partner, z_up, z_dn)):
        remote(normed_ref, toks.at[z, core], tsend.at[i], trecv.at[z * 2 + core], to).start()
        if i == 0:
            remote(info_ref, infos.at[z, core], isend.at[0], irecv.at[z * 2 + core], partner).start()
    column += [plane(chip_at(dz, 0)) for dz in range(1, NZ)]
    for i, to in enumerate(column):
        remote(info_ref, infos.at[z, core], isend.at[1 + i], irecv.at[z * 2 + core], to).start()

    def wanted(count, first):
        row = lax.broadcasted_iota(jnp.int32, (count, 128), 0)
        lane = lax.broadcasted_iota(jnp.int32, (count, 128), 1)
        expert = (first + row // 8) * 2 + core
        slot_id = expert * 4 + row % 4
        return jnp.where((row // 4) % 2 == lane // 32, slot_id, -1).astype(jnp.float32)

    here = wanted(32, z * NX)

    def hop(dz, i, to):
        zz = lax.rem(z + NZ - dz, NZ)
        remote(toks.at[zz, core], toks.at[zz, core], tsend.at[i], trecv.at[zz * 2 + core], to).start()

    def tokens_of(dz):
        zz = lax.rem(z + NZ - dz, NZ)
        if dz:
            remote(normed_ref, toks.at[zz, core], tsend.at[0], trecv.at[zz * 2 + core], partner).wait_recv()
            if dz in (1, 2, 3):
                hop(dz, 2 + dz, z_up)
            if dz in (7, 6):
                hop(dz, dz, z_dn)
            hop(dz, 7 + dz, partner)
            remote(info_ref, infos.at[zz, core], isend.at[0], irecv.at[zz * 2 + core], partner).wait_recv()
        remote(info_ref, infos.at[zz, 1 - core], isend.at[0], irecv.at[zz * 2 + 1 - core], partner).wait_recv()
        remote(normed_ref, toks.at[zz, 1 - core], tsend.at[0], trecv.at[zz * 2 + 1 - core], partner).wait_recv()
        info = infos[zz, 0] + infos[zz, 1]
        disp = jnp.zeros((32, 128), jnp.float32)
        for k in range(4):
            disp = disp + jnp.where(info[k : k + 1] == here, 1.0, 0.0)
        disp = disp[:, :64].astype(jnp.bfloat16)
        data = jnp.concatenate([toks[zz, 0], toks[zz, 1]], axis=0)
        for cut in range(2):
            cols = slice(cut * 1024, cut * 1024 + 1024)
            msgs[zz, :, :, cols] = (
                jnp.dot(disp, data[:, cols], preferred_element_type=jnp.float32).astype(jnp.bfloat16).reshape(4, 8, 1024)
            )
        rows[t, zz * NX + x] = msgs[zz, x]
        for i, dx in enumerate((1, 3, 2)):
            to = lax.rem(x + dx, NX)
            remote(
                msgs.at[zz, to], rows.at[t, zz * NX + x], msend.at[dz * 3 + i], mrecv.at[zz * NX + x], plane(chip_at(0, dx))
            ).start()

    def chunk_at(which, dz):
        first = lax.rem(z + NZ - dz, NZ) * NX
        return rows.at[which, pl.ds(first, NX)]

    def give(dz, sem, to):
        ref = chunk_at(t, dz)
        return remote(ref, ref, sem, grecv.at[t * 8 + dz], to)

    def take(which, dz):
        ref = chunk_at(which, dz)
        remote(ref, ref, gup.at[0], grecv.at[which * 8 + dz], up).wait_recv()

    def hand(which, dz, to):
        ref = chunk_at(which, dz)
        return remote(ref, ref, gfw.at[dz], grecv.at[which * 8 + dz], to)

    def relay(dz):
        take(t_dn, dz)
        if dz in VIA_UP:
            hand(t_dn, dz, up).start()
        take(t_up, dz)
        if dz in VIA_DN:
            hand(t_up, dz, dn).start()

    def spread(dz):
        zz = lax.rem(z + NZ - dz, NZ)
        for dx in (1, 3, 2):
            source = zz * NX + lax.rem(x + dx, NX)
            remote(msgs.at[0, 0], rows.at[t, source], msend.at[0], mrecv.at[source], partner).wait_recv()
        give(dz, gup.at[dz], up).start()
        give(dz, gdn.at[dz], dn).start()

    for i, dz in enumerate(GROUP_ORDER):
        tokens_of(dz)
        if i > 0:
            spread(GROUP_ORDER[i - 1])
        if i > 1:
            relay(GROUP_ORDER[i - 2])
    spread(GROUP_ORDER[7])
    relay(GROUP_ORDER[6])
    for load in loads:
        load.wait()

    def serve(which):
        data = rows[which].reshape(256, 2048)
        for f in range(2):
            cols = slice(f * 256, f * 256 + 256)
            gate = jnp.minimum(jnp.dot(data, wg[:, cols], preferred_element_type=jnp.float32), clamp_limit)
            lift = jnp.clip(jnp.dot(data, wu[:, cols], preferred_element_type=jnp.float32), -clamp_limit, clamp_limit)
            act[:, cols] = (gate * jax.nn.sigmoid(swish_alpha * gate) * (lift + 1.0)).astype(jnp.bfloat16)
        for cut in range(8):
            cols = slice(cut * 256, cut * 256 + 256)
            part[which, :, :, cols] = (
                jnp.dot(act[...], wd[:, cols], preferred_element_type=jnp.float32).astype(jnp.bfloat16).reshape(32, 8, 256)
            )

    def group(dz):
        return pl.ds(lax.rem(z + NZ - dz, NZ) * NX, NX)

    serve(t)
    relay(GROUP_ORDER[-1])

    def direct(k):
        a, b = group(VIA_DN[k]), group(VIA_UP[k])
        remote(part.at[t_up, a], fin.at[0, a], s_direct.at[k], finrecv.at[VIA_DN[k]], up).start()
        remote(part.at[t_dn, b], fin.at[1, b], s_direct.at[4 + k], finrecv.at[8 + VIA_UP[k]], dn).start()

    def first(k):
        a, b = group(VIA_UP[k]), group(VIA_DN[k])
        remote(part.at[t_far, a], mid.at[0, k], s_first.at[k], midrecv.at[k], up).start()
        remote(part.at[t_far, b], mid.at[1, k], s_first.at[4 + k], midrecv.at[4 + k], dn).start()

    def middle_sum(k):
        for way, (dzs, owner, to) in enumerate(((VIA_UP, t_up, up), (VIA_DN, t_dn, dn))):
            where = group(dzs[k])
            remote(part.at[owner, where], mid.at[way, k], s_first.at[0], midrecv.at[way * 4 + k], up).wait_recv()
            total = part[owner, where].astype(jnp.float32) + mid[way, k].astype(jnp.float32)
            part[owner, where] = total.astype(jnp.bfloat16)
            remote(part.at[owner, where], fin.at[way, where], s_mid.at[way * 4 + k], finrecv.at[way * 8 + dzs[k]], to).start()

    def settle(k):
        for dz in (VIA_UP[k], VIA_DN[k]):
            where = group(dz)
            for way in range(2):
                remote(part.at[t, where], fin.at[way, where], s_first.at[0], finrecv.at[way * 8 + dz], up).wait_recv()
            total = part[t, where].astype(jnp.float32) + fin[0, where].astype(jnp.float32) + fin[1, where].astype(jnp.float32)
            part[t, where] = total.astype(jnp.bfloat16)
            for dx in (2, 1, 3, 0):
                to = chip_at(NZ - dz, dx)
                if (dz, dx) != (0, 0):
                    remote(part.at[t, to], ret.at[chip], rsend.at[to], rrecv.at[chip], plane(to)).start()

    serve(t_up)
    serve(t_dn)
    direct(0)
    for dz in GROUP_ORDER:
        take(t_far, dz)
    serve(t_far)
    first(0)
    first(1)
    middle_sum(0)
    direct(1)
    first(2)
    middle_sum(1)
    settle(0)
    direct(2)
    first(3)
    middle_sum(2)
    settle(1)
    direct(3)
    middle_sum(3)
    settle(2)
    settle(3)
    ret[chip] = part[t, chip]
    for dz, dx in others:
        source = chip_at(dz, dx)
        remote(part.at[t, 0], ret.at[source], rsend.at[0], rrecv.at[source], partner).wait_recv()
    info = infos[z, 0] + infos[z, 1]
    everywhere = wanted(256, 0)
    weight = jnp.zeros((256, 128), jnp.float32)
    for k in range(4):
        weight = weight + jnp.where(info[k : k + 1] == everywhere, info[4 + k : 5 + k], 0.0)
    weight = weight.T[:64]
    coarse = weight.astype(jnp.bfloat16)
    fine = (weight - coarse.astype(jnp.float32)).astype(jnp.bfloat16)
    for cut in range(4):
        cols = slice(cut * 512, cut * 512 + 512)
        came = ret[:, :, cols].reshape(256, 512)
        mixed = jnp.dot(coarse, came, preferred_element_type=jnp.float32) + jnp.dot(
            fine, came, preferred_element_type=jnp.float32
        )
        mixs[0, :, cols] = mixed[:32]
        mixs[1, :, cols] = mixed[32:]
    swap_mix = remote(mixs.at[1 - core], mixs.at[2], xsem.at[0], xsem.at[1], partner)
    swap_mix.start()

    def sent(src, sem):
        remote(src, src, sem, xsem.at[1], partner).wait_send()

    for i in range(15):
        sent(toks.at[0, 0], tsend.at[i])
        sent(infos.at[0, 0], isend.at[i])
    for i in range(24):
        sent(msgs.at[0, 0], msend.at[i])

    for dz, dx in others:
        to = chip_at(dz, dx)
        sent(msgs.at[0, 0], rsend.at[to])
    for i in range(8):
        for sems in (gup, gdn, gfw, s_first, s_direct, s_mid):
            sent(mid.at[0, 0], sems.at[i])
    swap_mix.wait()
    mixture = mixs[core] + mixs[2]
    scale = lax.rsqrt(jnp.mean(mixture * mixture, axis=-1, keepdims=True) + norm_eps)
    out_ref[...] = (middle_ref[...] + mixture * scale * gain_ref[...]).astype(jnp.bfloat16)


ATTENTION_ITEMS = 25


def layer_kernel(q_ref, kv_ref, wo_hbm, residual_ref, mix_ref, pre_ref, info_ref, gain_ref, wg_hbm, wu_hbm, wd_hbm, out_ref, *rest):
    middle, normed, wsem = rest[:3]
    attention_items = rest[3 : 3 + ATTENTION_ITEMS]
    expert_items = rest[3 + ATTENTION_ITEMS :]
    wg, wu, wd = expert_items[10:13]
    sp = lax.axis_index("sp")
    t = lax.axis_index("tp")
    core = lax.rem(sp, 2)
    chip = lax.div(sp, 2)
    x = lax.rem(chip, NX)
    z = lax.div(chip, NX)

    def chip_at(dz, dx):
        return lax.rem(z + dz, NZ) * NX + lax.rem(x + dx, NX)

    others = [(dz, dx) for dz in GROUP_ORDER for dx in (0, 1, 3, 2) if (dz, dx) != (0, 0)]
    column = [chip_at(dz, 0) * 2 + 1 - core for dz in range(1, NZ)]
    loads = [pltpu.make_async_copy(src, dst, wsem.at[i]) for i, (src, dst) in enumerate(((wg_hbm, wg), (wu_hbm, wu), (wd_hbm, wd)))]

    def meet():
        barrier = pltpu.get_barrier_semaphore()
        peers = [{"sp": chip * 2 + 1 - core}] + [{"tp": lax.rem(t + d, 4)} for d in (1, 2, 3)]
        peers += [{"sp": chip_at(dz, dx) * 2 + core} for dz, dx in others] + [{"sp": to} for to in column]
        for peer in peers:
            pl.semaphore_signal(barrier, inc=1, device_id=peer, device_id_type=MESH)
        pl.semaphore_wait(barrier, len(peers))

    for load in loads:
        load.start()
    attention_part(q_ref, kv_ref, wo_hbm, residual_ref, mix_ref, pre_ref, middle, normed, meet, *attention_items)
    experts_part(normed, info_ref, middle, gain_ref, loads, out_ref, others, column, *expert_items)


def layer(q_two, kv_two, w_out, residual, gain_mix, gain_pre, info, gain_moe, w_gate, w_up, w_down):
    whole, apart = pl.BlockSpec(memory_space=pltpu.VMEM), pl.BlockSpec(memory_space=pltpu.MemorySpace.HBM)
    dma, bf16, f32 = pltpu.SemaphoreType.DMA, jnp.bfloat16, jnp.float32
    attention_scratch = [
        pltpu.VMEM((64, 2, PIECE, 128), bf16),
        pltpu.VMEM((1024, 128), bf16),
        pltpu.VMEM((1, 1024), f32),
        pltpu.VMEM((1, 1024), f32),
        pltpu.VMEM((128, 1024), f32),
        pltpu.VMEM((3, 128, 512), bf16),
        pltpu.VMEM((128, 1024), bf16),
        pltpu.VMEM((1024, 2048), bf16),
        pltpu.VMEM((4, 32, 2048), bf16),
        pltpu.VMEM((3, 32, 2048), bf16),
    ] + [dma((n,)) if n else dma for n in (64, 0, 3, 16, 16, 4, 4, 8, 8, 8, 2, 2, 3, 3, 0)]
    expert_scratch = [
        pltpu.VMEM((8, 2, 32, 2048), bf16),
        pltpu.VMEM((8, 2, 8, 128), f32),
        pltpu.VMEM((8, 4, 8, 2048), bf16),
        pltpu.VMEM((4, 32, 8, 2048), bf16),
        pltpu.VMEM((256, 512), bf16),
        pltpu.VMEM((4, 32, 8, 2048), bf16),
        pltpu.VMEM((2, 4, 4, 8, 2048), bf16),
        pltpu.VMEM((2, 32, 8, 2048), bf16),
        pltpu.VMEM((32, 8, 2048), bf16),
        pltpu.VMEM((3, 32, 2048), f32),
        pltpu.VMEM((2048, 512), bf16),
        pltpu.VMEM((2048, 512), bf16),
        pltpu.VMEM((512, 2048), bf16),
    ] + [dma((n,)) for n in (15, 16, 15, 16, 24, 32, 8, 8, 8, 32, 8, 8, 8, 8, 16, 32, 32, 2)]
    return pl.pallas_call(
        layer_kernel,
        out_shape=jax.ShapeDtypeStruct((32, 2048), bf16),
        in_specs=[whole, whole, apart, whole, whole, whole, whole, whole, apart, apart, apart],
        out_specs=whole,
        scratch_shapes=[pltpu.VMEM((32, 2048), f32), pltpu.VMEM((32, 2048), bf16), dma((3,))] + attention_scratch + expert_scratch,
        compiler_params=pltpu.CompilerParams(collective_id=0, has_side_effects=True, vmem_limit_bytes=58 << 20),
        name="layer",
    )(q_two, kv_two, w_out, residual, gain_mix, gain_pre, info, gain_moe, w_gate, w_up, w_down)


def on_device(
    queries,
    keys,
    values,
    q_gain,
    k_gain,
    w_out,
    residual,
    gain_mix,
    gain_pre,
    routes,
    route_weights,
    w_gate,
    w_up,
    w_down,
    gain_moe,
):
    tok_rows, head_local, head_size = queries.shape
    kv_local = keys.shape[1]
    group_size = head_local // kv_local
    positions = lax.axis_index("sp") * tok_rows + jnp.arange(tok_rows, dtype=jnp.int32)
    cosine_table, sine_table = rope_tables(positions, head_size)
    q_turned = (
        turn(scale_rows(queries.astype(jnp.float32), q_gain), cosine_table, sine_table)
        * head_size ** (-0.5)
    ).astype(jnp.bfloat16)
    k_turned = turn(scale_rows(keys.astype(jnp.float32), k_gain), cosine_table, sine_table).astype(
        jnp.bfloat16
    )
    q_two = q_turned.transpose(1, 0, 2).reshape(kv_local, group_size * tok_rows, head_size)
    kv_two = jnp.stack([k_turned.transpose(1, 0, 2), values.transpose(1, 2, 0)], axis=1)
    width = residual.shape[1]
    info = route_info(routes, route_weights)
    return layer(
        q_two,
        kv_two,
        w_out,
        residual,
        gain_mix.reshape(1, width),
        gain_pre.reshape(1, width),
        info,
        gain_moe.reshape(1, width),
        w_gate[0],
        w_up[0],
        w_down[0],
    )


def solution(mesh):
    placed = (
        P("sp", "tp", None),
        P("sp", "tp", None),
        P("sp", "tp", None),
        P(),
        P(),
        P("tp", None),
        P(("sp", "tp"), None),
        P(),
        P(),
        P(("sp", "tp"), None),
        P(("sp", "tp"), None),
        P("sp", None, "tp"),
        P("sp", None, "tp"),
        P("sp", "tp", None),
        P(),
    )
    return jax.shard_map(
        on_device, mesh=mesh, in_specs=placed, out_specs=P(("sp", "tp"), None), check_vma=False
    )
```

```python
import jax
import jax.numpy as jnp
from jax import lax
from jax.experimental import pallas as pl
from jax.experimental.pallas import tpu as pltpu
from jax.sharding import PartitionSpec as P

TOP = 4
GRID_W = 64


norm_eps = 1e-06
rope_theta = 10000.0
clamp_limit = 7.0
swish_alpha = 1.702


def rope_tables(positions, head_size):
    row_index = (positions // GRID_W).astype(jnp.float32)
    col_index = (positions % GRID_W).astype(jnp.float32)
    freq_count = head_size // 4
    inverse = rope_theta ** (-jnp.arange(freq_count, dtype=jnp.float32) / freq_count)
    angles = jnp.stack([row_index[:, None] * inverse, col_index[:, None] * inverse], axis=1)
    return (jnp.cos(angles), jnp.sin(angles))


def turn(array_in, cosine_table, sine_table):
    token_count, head_count, head_size = array_in.shape
    split_field = array_in.reshape(token_count, head_count, 2, 2, head_size // 4)
    first_half = split_field[:, :, :, 0, :]
    second_half = split_field[:, :, :, 1, :]
    cos_wide = cosine_table[:, None]
    sin_wide = sine_table[:, None]
    turned = jnp.stack(
        [
            first_half * cos_wide - second_half * sin_wide,
            second_half * cos_wide + first_half * sin_wide,
        ],
        axis=3,
    )
    return turned.reshape(token_count, head_count, head_size)


def scale_rows(array_in, gain_vec):
    return (
        array_in
        * lax.rsqrt(jnp.mean(array_in * array_in, axis=-1, keepdims=True) + norm_eps)
        * gain_vec
    )


def route_info(routes, route_weights):
    core = lax.rem(lax.axis_index("sp"), 2)
    count = routes.shape[0]
    flat = routes.reshape(-1)
    place = jnp.arange(count * TOP, dtype=jnp.int32)
    earlier = (flat[:, None] == flat[None, :]) & (place[None, :] < place[:, None])
    rank = jnp.sum(earlier.astype(jnp.int32), axis=1)
    slots = (flat * 4 + rank).reshape(count, TOP).astype(jnp.float32)
    info = jnp.concatenate([slots.T, route_weights.T], axis=0)
    side = jnp.arange(128 // count, dtype=jnp.int32)[None, :, None]
    return jnp.where(side == core, info[:, None, :], 0.0).reshape(2 * TOP, 128)


MESH = pl.DeviceIdType.MESH
NZ, NX = 8, 4
PIECE = 128


def attention_part(q_ref, kv_ref, wo_hbm, residual_ref, mix_ref, pre_ref, middle_ref, normed_ref, meet,
                     buf, qbuf, m_ref, l_ref, acc, obuf, heads, wo, pbuf, pin,
                     rsem, qsem, asem, zup, zdn, bup, bdn, bxp, bxm, bfw, dsem, osem, psend, precv, wsem):
    sp = lax.axis_index("sp")
    t = lax.axis_index("tp")
    load = pltpu.make_async_copy(wo_hbm, wo, wsem)
    load.start()
    core = lax.rem(sp, 2)
    chip = lax.div(sp, 2)
    x = lax.rem(chip, NX)
    z = lax.div(chip, NX)

    def dev(zz, xx, cc):
        return {"sp": (lax.rem(zz + 2 * NZ, NZ) * NX + lax.rem(xx + 2 * NX, NX)) * 2 + cc}

    def slot(kind, zz, xx):
        return kind * (NZ * NX) + lax.rem(zz + 2 * NZ, NZ) * NX + lax.rem(xx + 2 * NX, NX)

    partner = dev(z, x, 1 - core)
    z_up, z_dn = dev(z + 1, x, core), dev(z - 1, x, core)
    x_up, x_dn, x_far = dev(z, x + 1, core), dev(z, x - 1, core), dev(z, x + 2, core)

    mine = core * (NZ * NX) + chip
    buf[mine] = kv_ref[core]
    qbuf[pl.ds(pl.multiple_of(core * 512, 512), 512), :] = q_ref[core]
    m_ref[...] = jnp.full(m_ref.shape, -jnp.inf, jnp.float32)
    l_ref[...] = jnp.zeros(l_ref.shape, jnp.float32)
    acc[...] = jnp.zeros(acc.shape, jnp.float32)

    tp_peers = [lax.rem(t + d, 4) for d in (2, 1, 3)]
    meet()

    def move(at, sem, to):
        return pltpu.make_async_remote_copy(
            src_ref=buf.at[at], dst_ref=buf.at[at], send_sem=sem, recv_sem=rsem.at[at], device_id=to, device_id_type=MESH
        )

    def send(at, sem, to):
        move(at, sem, to).start()

    def arrive(at):
        move(at, dsem.at[0], partner).wait_recv()

    def done(sem):
        move(0, sem, partner).wait_send()

    swap_kv = pltpu.make_async_remote_copy(
        src_ref=kv_ref.at[1 - core], dst_ref=buf.at[(1 - core) * 0 + core * (NZ * NX) + chip], send_sem=dsem.at[0],
        recv_sem=rsem.at[core * (NZ * NX) + chip], device_id=partner, device_id_type=MESH,
    )
    swap_q = pltpu.make_async_remote_copy(
        src_ref=q_ref.at[1 - core], dst_ref=qbuf.at[pl.ds(pl.multiple_of(core * 512, 512), 512), :], send_sem=dsem.at[1],
        recv_sem=qsem, device_id=partner, device_id_type=MESH,
    )
    swap_kv.start()
    swap_q.start()
    arrive((1 - core) * (NZ * NX) + chip)

    def attend(slots):
        keys = jnp.concatenate([buf[s, 0] for s in slots], axis=0)
        vals = jnp.concatenate([buf[s, 1] for s in slots], axis=1)
        for tile in range(4):
            cols = slice(tile * 256, tile * 256 + 256)
            scores = lax.dot_general(keys, qbuf[cols, :], (((1,), (1,)), ((), ())), preferred_element_type=jnp.float32)
            before = m_ref[:, cols]
            now = jnp.maximum(before, jnp.max(scores, axis=0, keepdims=True))
            shrink = jnp.exp(before - now)
            unnorm = jnp.exp(scores - now)
            l_ref[:, cols] = l_ref[:, cols] * shrink + jnp.sum(unnorm, axis=0, keepdims=True)
            acc[:, cols] = acc[:, cols] * shrink + jnp.dot(
                vals, unnorm.astype(jnp.bfloat16), preferred_element_type=jnp.float32
            )
            m_ref[:, cols] = now

    A, B = 0, 1
    own_a, own_b = slot(A, z, x), slot(B, z, x)
    send(own_b, bup.at[0], z_up)
    send(own_b, bdn.at[0], z_dn)
    send(own_a, asem.at[0], x_up)
    send(own_a, asem.at[1], x_dn)
    send(own_a, zup.at[0], z_up)
    send(own_a, zdn.at[0], z_dn)
    send(own_a, asem.at[2], x_far)
    send(own_b, bxp.at[0], x_up)
    send(own_b, bxm.at[0], x_dn)
    ready = [own_a, own_b]

    def work(least=4):
        if len(ready) >= least:
            group = ready[:4]
            del ready[:4]
            attend(group)

    def lines_b(r):
        lo, hi = slot(B, z - r, x), slot(B, z + r, x)
        arrive(lo)
        if r < 4:
            send(lo, bup.at[r], z_up)
        send(lo, bxp.at[2 * r - 1], x_up)
        send(lo, bxm.at[2 * r - 1], x_dn)
        ready.append(lo)
        if r < 4:
            arrive(hi)
            if r < 3:
                send(hi, bdn.at[r], z_dn)
            send(hi, bxp.at[2 * r], x_up)
            send(hi, bxm.at[2 * r], x_dn)
            ready.append(hi)

    def lines_a(r, j):
        lo, hi = slot(A, z - r, x + j), slot(A, z + r, x + j)
        arrive(lo)
        if r < 3 or (r == 3 and j in (0, 1)):
            send(lo, zup.at[r * 4 + j], z_up)
        if 0 < r < 4:
            ready.append(lo)
            arrive(hi)
        if r < 3 or (r == 3 and j in (2, 3)):
            send(hi, zdn.at[r * 4 + j], z_dn)
        ready.append(hi)

    def across(r):
        if r > 0:
            at = slot(B, z - r, x - 1)
            arrive(at)
            send(at, bfw.at[2 * r - 1], x_up)
            ready.append(at)
        if r < 4:
            at = slot(B, z + r, x + 1)
            arrive(at)
            send(at, bfw.at[2 * r], x_dn)
            ready.append(at)
        if r > 0:
            at = slot(B, z - r, x + 1)
            arrive(at)
            ready.append(at)
        if r < 4:
            at = slot(B, z + r, x - 1)
            arrive(at)
            ready.append(at)

    def far(r):
        for at in {0: [slot(B, z, x + 2)], 4: [slot(B, z + 4, x + 2)]}.get(r, [slot(B, z - r, x + 2), slot(B, z + r, x + 2)]):
            arrive(at)
            ready.append(at)

    swap_q.wait_recv()
    lines_a(0, 1)
    work()
    lines_a(0, 3)
    work()
    lines_a(0, 2)
    work()
    lines_b(1)
    work()
    lines_a(1, 0)
    work()
    lines_a(1, 1)
    work()
    across(0)
    work()
    lines_b(2)
    work()
    lines_a(1, 3)
    work()
    lines_a(1, 2)
    work()
    across(1)
    work()
    far(0)
    work()
    lines_a(2, 0)
    work()
    lines_a(2, 1)
    work()
    lines_b(3)
    work()
    across(2)
    work()
    far(1)
    work()
    lines_a(2, 3)
    work()
    lines_a(2, 2)
    work()
    lines_b(4)
    work()
    lines_a(3, 0)
    work()
    lines_a(3, 1)
    work()
    across(3)
    work()
    far(2)
    work()
    lines_a(3, 3)
    work()
    lines_a(3, 2)
    work()
    across(4)
    work()
    far(3)
    work()
    lines_a(4, 0)
    work()
    lines_a(4, 1)
    work()
    far(4)
    work()
    lines_a(4, 3)
    work()
    lines_a(4, 2)
    work()
    while ready:
        work(1)

    def heads_of(which):
        cols = pl.ds(pl.multiple_of(which * 512, 512), 512)
        return (acc[:, cols] / l_ref[:, cols]).astype(jnp.bfloat16)

    theirs = heads_of(1 - core)
    obuf[2] = theirs
    own = heads_of(core)
    obuf[core] = own
    swap_o = pltpu.make_async_remote_copy(
        src_ref=obuf.at[2], dst_ref=obuf.at[core], send_sem=osem.at[0], recv_sem=osem.at[1], device_id=partner, device_id_type=MESH
    )
    swap_o.start()

    def stack_heads(g):
        for h in range(4):
            cols = pl.ds(pl.multiple_of(g * 512 + h * 128, 128), 128)
            heads[:, cols] = obuf[g, :, h * 128 : h * 128 + 128].T

    stack_heads(core)
    load.wait()
    swap_o.wait()
    stack_heads(1 - core)
    for cut in range(4):
        cols = slice(cut * 512, cut * 512 + 512)
        part = jnp.dot(heads[...], wo[:, cols], preferred_element_type=jnp.float32).astype(jnp.bfloat16)
        for owner in range(4):
            pbuf[owner, :, cols] = part[owner * 32 : owner * 32 + 32]
    gives = [
        pltpu.make_async_remote_copy(
            src_ref=pbuf.at[peer], dst_ref=pin.at[i], send_sem=psend.at[i], recv_sem=precv.at[i], device_id={"tp": peer},
            device_id_type=MESH,
        )
        for i, peer in enumerate(tp_peers)
    ]
    for give in gives:
        give.start()
    for i in range(3):
        done(asem.at[i])
    for i in range(4):
        done(bup.at[i])
        for j in range(4):
            if i < 3 or j in (0, 1):
                done(zup.at[i * 4 + j])
            if i < 3 or j in (2, 3):
                done(zdn.at[i * 4 + j])
    for i in range(3):
        done(bdn.at[i])
    for i in range(8):
        done(bxp.at[i])
        done(bxm.at[i])
        done(bfw.at[i])
    swap_kv.wait_send()
    swap_q.wait_send()
    for give in gives:
        give.wait()
    projected = pbuf[t].astype(jnp.float32)
    for i in range(3):
        projected = projected + pin[i].astype(jnp.float32)
    middle = residual_ref[...].astype(jnp.float32) + scale_rows(projected, mix_ref[...])
    middle_ref[...] = middle
    normed_ref[...] = scale_rows(middle, pre_ref[...]).astype(jnp.bfloat16)


GROUP_ORDER = (0, 1, 7, 2, 6, 3, 5, 4)
VIA_UP = (3, 6, 1, 0)
VIA_DN = (4, 5, 2, 7)


def experts_part(normed_ref, info_ref, middle_ref, gain_ref, loads, out_ref, others, column,
                 toks, infos, msgs, rows, act, part, mid, fin, ret, mixs, wg, wu, wd,
                   isend, irecv, tsend, trecv, msend, mrecv, gup, gdn, gfw, grecv, s_first, s_direct, s_mid, midrecv, finrecv,
                   rsend, rrecv, xsem):
    sp = lax.axis_index("sp")
    t = lax.axis_index("tp")
    core = lax.rem(sp, 2)
    chip = lax.div(sp, 2)
    x = lax.rem(chip, NX)
    z = lax.div(chip, NX)
    t_up, t_dn, t_far = lax.rem(t + 1, 4), lax.rem(t + 3, 4), lax.rem(t + 2, 4)

    def chip_at(dz, dx):
        return lax.rem(z + dz, NZ) * NX + lax.rem(x + dx, NX)

    def plane(which):
        return {"sp": which * 2 + core}

    partner = {"sp": chip * 2 + 1 - core}
    up, dn = {"tp": t_up}, {"tp": t_dn}

    toks[z, core] = normed_ref[...]
    infos[z, core] = info_ref[...]

    column = [{"sp": to} for to in column]

    def remote(src, dst, send_sem, recv_sem, to):
        return pltpu.make_async_remote_copy(
            src_ref=src, dst_ref=dst, send_sem=send_sem, recv_sem=recv_sem, device_id=to, device_id_type=MESH
        )

    z_up, z_dn = plane(chip_at(1, 0)), plane(chip_at(NZ - 1, 0))
    for i, to in enumerate((partner, z_up, z_dn)):
        remote(normed_ref, toks.at[z, core], tsend.at[i], trecv.at[z * 2 + core], to).start()
        if i == 0:
            remote(info_ref, infos.at[z, core], isend.at[0], irecv.at[z * 2 + core], partner).start()
    column += [plane(chip_at(dz, 0)) for dz in range(1, NZ)]
    for i, to in enumerate(column):
        remote(info_ref, infos.at[z, core], isend.at[1 + i], irecv.at[z * 2 + core], to).start()

    def wanted(count, first):
        row = lax.broadcasted_iota(jnp.int32, (count, 128), 0)
        lane = lax.broadcasted_iota(jnp.int32, (count, 128), 1)
        expert = (first + row // 8) * 2 + core
        slot_id = expert * 4 + row % 4
        return jnp.where((row // 4) % 2 == lane // 32, slot_id, -1).astype(jnp.float32)

    here = wanted(32, z * NX)

    def hop(dz, i, to):
        zz = lax.rem(z + NZ - dz, NZ)
        remote(toks.at[zz, core], toks.at[zz, core], tsend.at[i], trecv.at[zz * 2 + core], to).start()

    def tokens_of(dz):
        zz = lax.rem(z + NZ - dz, NZ)
        if dz:
            remote(normed_ref, toks.at[zz, core], tsend.at[0], trecv.at[zz * 2 + core], partner).wait_recv()
            if dz in (1, 2, 3):
                hop(dz, 2 + dz, z_up)
            if dz in (7, 6):
                hop(dz, dz, z_dn)
            hop(dz, 7 + dz, partner)
            remote(info_ref, infos.at[zz, core], isend.at[0], irecv.at[zz * 2 + core], partner).wait_recv()
        remote(info_ref, infos.at[zz, 1 - core], isend.at[0], irecv.at[zz * 2 + 1 - core], partner).wait_recv()
        remote(normed_ref, toks.at[zz, 1 - core], tsend.at[0], trecv.at[zz * 2 + 1 - core], partner).wait_recv()
        info = infos[zz, 0] + infos[zz, 1]
        disp = jnp.zeros((32, 128), jnp.float32)
        for k in range(4):
            disp = disp + jnp.where(info[k : k + 1] == here, 1.0, 0.0)
        disp = disp[:, :64].astype(jnp.bfloat16)
        data = jnp.concatenate([toks[zz, 0], toks[zz, 1]], axis=0)
        for cut in range(2):
            cols = slice(cut * 1024, cut * 1024 + 1024)
            msgs[zz, :, :, cols] = (
                jnp.dot(disp, data[:, cols], preferred_element_type=jnp.float32).astype(jnp.bfloat16).reshape(4, 8, 1024)
            )
        rows[t, zz * NX + x] = msgs[zz, x]
        for i, dx in enumerate((1, 3, 2)):
            to = lax.rem(x + dx, NX)
            remote(
                msgs.at[zz, to], rows.at[t, zz * NX + x], msend.at[dz * 3 + i], mrecv.at[zz * NX + x], plane(chip_at(0, dx))
            ).start()

    def chunk_at(which, dz):
        first = lax.rem(z + NZ - dz, NZ) * NX
        return rows.at[which, pl.ds(first, NX)]

    def give(dz, sem, to):
        ref = chunk_at(t, dz)
        return remote(ref, ref, sem, grecv.at[t * 8 + dz], to)

    def take(which, dz):
        ref = chunk_at(which, dz)
        remote(ref, ref, gup.at[0], grecv.at[which * 8 + dz], up).wait_recv()

    def hand(which, dz, to):
        ref = chunk_at(which, dz)
        return remote(ref, ref, gfw.at[dz], grecv.at[which * 8 + dz], to)

    def relay(dz):
        take(t_dn, dz)
        if dz in VIA_UP:
            hand(t_dn, dz, up).start()
        take(t_up, dz)
        if dz in VIA_DN:
            hand(t_up, dz, dn).start()

    def spread(dz):
        zz = lax.rem(z + NZ - dz, NZ)
        for dx in (1, 3, 2):
            source = zz * NX + lax.rem(x + dx, NX)
            remote(msgs.at[0, 0], rows.at[t, source], msend.at[0], mrecv.at[source], partner).wait_recv()
        give(dz, gup.at[dz], up).start()
        give(dz, gdn.at[dz], dn).start()

    for i in range(11):
        if i < 8:
            tokens_of(GROUP_ORDER[i])
        if 1 <= i < 9:
            spread(GROUP_ORDER[i - 1])
        if i >= 4:
            relay(GROUP_ORDER[i - 4])
    for load in loads:
        load.wait()

    def serve(which):
        data = rows[which].reshape(256, 2048)
        for f in range(2):
            cols = slice(f * 256, f * 256 + 256)
            gate = jnp.minimum(jnp.dot(data, wg[:, cols], preferred_element_type=jnp.float32), clamp_limit)
            lift = jnp.clip(jnp.dot(data, wu[:, cols], preferred_element_type=jnp.float32), -clamp_limit, clamp_limit)
            act[:, cols] = (gate * jax.nn.sigmoid(swish_alpha * gate) * (lift + 1.0)).astype(jnp.bfloat16)
        for cut in range(8):
            cols = slice(cut * 256, cut * 256 + 256)
            part[which, :, :, cols] = (
                jnp.dot(act[...], wd[:, cols], preferred_element_type=jnp.float32).astype(jnp.bfloat16).reshape(32, 8, 256)
            )

    def group(dz):
        return pl.ds(lax.rem(z + NZ - dz, NZ) * NX, NX)

    serve(t)
    relay(GROUP_ORDER[-1])

    def direct(k):
        a, b = group(VIA_DN[k]), group(VIA_UP[k])
        remote(part.at[t_up, a], fin.at[0, a], s_direct.at[k], finrecv.at[VIA_DN[k]], up).start()
        remote(part.at[t_dn, b], fin.at[1, b], s_direct.at[4 + k], finrecv.at[8 + VIA_UP[k]], dn).start()

    def first(k):
        a, b = group(VIA_UP[k]), group(VIA_DN[k])
        remote(part.at[t_far, a], mid.at[0, k], s_first.at[k], midrecv.at[k], up).start()
        remote(part.at[t_far, b], mid.at[1, k], s_first.at[4 + k], midrecv.at[4 + k], dn).start()

    def middle_sum(k):
        for way, (dzs, owner, to) in enumerate(((VIA_UP, t_up, up), (VIA_DN, t_dn, dn))):
            where = group(dzs[k])
            remote(part.at[owner, where], mid.at[way, k], s_first.at[0], midrecv.at[way * 4 + k], up).wait_recv()
            total = part[owner, where].astype(jnp.float32) + mid[way, k].astype(jnp.float32)
            part[owner, where] = total.astype(jnp.bfloat16)
            remote(part.at[owner, where], fin.at[way, where], s_mid.at[way * 4 + k], finrecv.at[way * 8 + dzs[k]], to).start()

    def settle(k):
        for dz in (VIA_UP[k], VIA_DN[k]):
            where = group(dz)
            for way in range(2):
                remote(part.at[t, where], fin.at[way, where], s_first.at[0], finrecv.at[way * 8 + dz], up).wait_recv()
            total = part[t, where].astype(jnp.float32) + fin[0, where].astype(jnp.float32) + fin[1, where].astype(jnp.float32)
            part[t, where] = total.astype(jnp.bfloat16)
            for dx in (2, 1, 3, 0):
                to = chip_at(NZ - dz, dx)
                if (dz, dx) != (0, 0):
                    remote(part.at[t, to], ret.at[chip], rsend.at[to], rrecv.at[chip], plane(to)).start()

    serve(t_up)
    serve(t_dn)
    direct(0)
    direct(1)
    for dz in GROUP_ORDER:
        take(t_far, dz)
    serve(t_far)
    first(0)
    first(1)
    middle_sum(0)
    first(2)
    middle_sum(1)
    direct(2)
    settle(0)
    first(3)
    middle_sum(2)
    direct(3)
    settle(1)
    middle_sum(3)
    settle(2)
    settle(3)
    ret[chip] = part[t, chip]
    for dz, dx in others:
        source = chip_at(dz, dx)
        remote(part.at[t, 0], ret.at[source], rsend.at[0], rrecv.at[source], partner).wait_recv()
    info = infos[z, 0] + infos[z, 1]
    everywhere = wanted(256, 0)
    weight = jnp.zeros((256, 128), jnp.float32)
    for k in range(4):
        weight = weight + jnp.where(info[k : k + 1] == everywhere, info[4 + k : 5 + k], 0.0)
    weight = weight.T[:64]
    coarse = weight.astype(jnp.bfloat16)
    fine = (weight - coarse.astype(jnp.float32)).astype(jnp.bfloat16)
    for cut in range(4):
        cols = slice(cut * 512, cut * 512 + 512)
        came = ret[:, :, cols].reshape(256, 512)
        mixed = jnp.dot(coarse, came, preferred_element_type=jnp.float32) + jnp.dot(
            fine, came, preferred_element_type=jnp.float32
        )
        mixs[0, :, cols] = mixed[:32]
        mixs[1, :, cols] = mixed[32:]
    swap_mix = remote(mixs.at[1 - core], mixs.at[2], xsem.at[0], xsem.at[1], partner)
    swap_mix.start()

    def sent(src, sem):
        remote(src, src, sem, xsem.at[1], partner).wait_send()

    for i in range(15):
        sent(toks.at[0, 0], tsend.at[i])
        sent(infos.at[0, 0], isend.at[i])
    for i in range(24):
        sent(msgs.at[0, 0], msend.at[i])

    for dz, dx in others:
        to = chip_at(dz, dx)
        sent(msgs.at[0, 0], rsend.at[to])
    for i in range(8):
        for sems in (gup, gdn, gfw, s_first, s_direct, s_mid):
            sent(mid.at[0, 0], sems.at[i])
    swap_mix.wait()
    mixture = mixs[core] + mixs[2]
    scale = lax.rsqrt(jnp.mean(mixture * mixture, axis=-1, keepdims=True) + norm_eps)
    out_ref[...] = (middle_ref[...] + mixture * scale * gain_ref[...]).astype(jnp.bfloat16)


ATTENTION_ITEMS = 25


def layer_kernel(q_ref, kv_ref, wo_hbm, residual_ref, mix_ref, pre_ref, info_ref, gain_ref, wg_hbm, wu_hbm, wd_hbm, out_ref, *rest):
    middle, normed, wsem = rest[:3]
    attention_items = rest[3 : 3 + ATTENTION_ITEMS]
    expert_items = rest[3 + ATTENTION_ITEMS :]
    wg, wu, wd = expert_items[10:13]
    sp = lax.axis_index("sp")
    t = lax.axis_index("tp")
    core = lax.rem(sp, 2)
    chip = lax.div(sp, 2)
    x = lax.rem(chip, NX)
    z = lax.div(chip, NX)

    def chip_at(dz, dx):
        return lax.rem(z + dz, NZ) * NX + lax.rem(x + dx, NX)

    others = [(dz, dx) for dz in GROUP_ORDER for dx in (0, 1, 3, 2) if (dz, dx) != (0, 0)]
    column = [chip_at(dz, 0) * 2 + 1 - core for dz in range(1, NZ)]
    loads = [pltpu.make_async_copy(src, dst, wsem.at[i]) for i, (src, dst) in enumerate(((wg_hbm, wg), (wu_hbm, wu), (wd_hbm, wd)))]

    def meet():
        barrier = pltpu.get_barrier_semaphore()
        peers = [{"sp": chip * 2 + 1 - core}] + [{"tp": lax.rem(t + d, 4)} for d in (1, 2, 3)]
        peers += [{"sp": chip_at(dz, dx) * 2 + core} for dz, dx in others] + [{"sp": to} for to in column]
        for peer in peers:
            pl.semaphore_signal(barrier, inc=1, device_id=peer, device_id_type=MESH)
        pl.semaphore_wait(barrier, len(peers))

    for load in loads:
        load.start()
    attention_part(q_ref, kv_ref, wo_hbm, residual_ref, mix_ref, pre_ref, middle, normed, meet, *attention_items)
    experts_part(normed, info_ref, middle, gain_ref, loads, out_ref, others, column, *expert_items)


def layer(q_two, kv_two, w_out, residual, gain_mix, gain_pre, info, gain_moe, w_gate, w_up, w_down):
    whole, apart = pl.BlockSpec(memory_space=pltpu.VMEM), pl.BlockSpec(memory_space=pltpu.MemorySpace.HBM)
    dma, bf16, f32 = pltpu.SemaphoreType.DMA, jnp.bfloat16, jnp.float32
    attention_scratch = [
        pltpu.VMEM((64, 2, PIECE, 128), bf16),
        pltpu.VMEM((1024, 128), bf16),
        pltpu.VMEM((1, 1024), f32),
        pltpu.VMEM((1, 1024), f32),
        pltpu.VMEM((128, 1024), f32),
        pltpu.VMEM((3, 128, 512), bf16),
        pltpu.VMEM((128, 1024), bf16),
        pltpu.VMEM((1024, 2048), bf16),
        pltpu.VMEM((4, 32, 2048), bf16),
        pltpu.VMEM((3, 32, 2048), bf16),
    ] + [dma((n,)) if n else dma for n in (64, 0, 3, 16, 16, 4, 4, 8, 8, 8, 2, 2, 3, 3, 0)]
    expert_scratch = [
        pltpu.VMEM((8, 2, 32, 2048), bf16),
        pltpu.VMEM((8, 2, 8, 128), f32),
        pltpu.VMEM((8, 4, 8, 2048), bf16),
        pltpu.VMEM((4, 32, 8, 2048), bf16),
        pltpu.VMEM((256, 512), bf16),
        pltpu.VMEM((4, 32, 8, 2048), bf16),
        pltpu.VMEM((2, 4, 4, 8, 2048), bf16),
        pltpu.VMEM((2, 32, 8, 2048), bf16),
        pltpu.VMEM((32, 8, 2048), bf16),
        pltpu.VMEM((3, 32, 2048), f32),
        pltpu.VMEM((2048, 512), bf16),
        pltpu.VMEM((2048, 512), bf16),
        pltpu.VMEM((512, 2048), bf16),
    ] + [dma((n,)) for n in (15, 16, 15, 16, 24, 32, 8, 8, 8, 32, 8, 8, 8, 8, 16, 32, 32, 2)]
    return pl.pallas_call(
        layer_kernel,
        out_shape=jax.ShapeDtypeStruct((32, 2048), bf16),
        in_specs=[whole, whole, apart, whole, whole, whole, whole, whole, apart, apart, apart],
        out_specs=whole,
        scratch_shapes=[pltpu.VMEM((32, 2048), f32), pltpu.VMEM((32, 2048), bf16), dma((3,))] + attention_scratch + expert_scratch,
        compiler_params=pltpu.CompilerParams(collective_id=0, has_side_effects=True, vmem_limit_bytes=40 << 20),
        name="layer",
    )(q_two, kv_two, w_out, residual, gain_mix, gain_pre, info, gain_moe, w_gate, w_up, w_down)


def on_device(
    queries,
    keys,
    values,
    q_gain,
    k_gain,
    w_out,
    residual,
    gain_mix,
    gain_pre,
    routes,
    route_weights,
    w_gate,
    w_up,
    w_down,
    gain_moe,
):
    tok_rows, head_local, head_size = queries.shape
    kv_local = keys.shape[1]
    group_size = head_local // kv_local
    positions = lax.axis_index("sp") * tok_rows + jnp.arange(tok_rows, dtype=jnp.int32)
    cosine_table, sine_table = rope_tables(positions, head_size)
    q_turned = (
        turn(scale_rows(queries.astype(jnp.float32), q_gain), cosine_table, sine_table)
        * head_size ** (-0.5)
    ).astype(jnp.bfloat16)
    k_turned = turn(scale_rows(keys.astype(jnp.float32), k_gain), cosine_table, sine_table).astype(
        jnp.bfloat16
    )
    q_two = q_turned.transpose(1, 0, 2).reshape(kv_local, group_size * tok_rows, head_size)
    kv_two = jnp.stack([k_turned.transpose(1, 0, 2), values.transpose(1, 2, 0)], axis=1)
    width = residual.shape[1]
    info = route_info(routes, route_weights)
    return layer(
        q_two,
        kv_two,
        w_out,
        residual,
        gain_mix.reshape(1, width),
        gain_pre.reshape(1, width),
        info,
        gain_moe.reshape(1, width),
        w_gate[0],
        w_up[0],
        w_down[0],
    )


def solution(mesh):
    placed = (
        P("sp", "tp", None),
        P("sp", "tp", None),
        P("sp", "tp", None),
        P(),
        P(),
        P("tp", None),
        P(("sp", "tp"), None),
        P(),
        P(),
        P(("sp", "tp"), None),
        P(("sp", "tp"), None),
        P("sp", None, "tp"),
        P("sp", None, "tp"),
        P("sp", "tp", None),
        P(),
    )
    return jax.shard_map(
        on_device, mesh=mesh, in_specs=placed, out_specs=P(("sp", "tp"), None), check_vma=False
    )
```

```python
import jax
import jax.numpy as jnp
from jax import lax
from jax.experimental import pallas as pl
from jax.experimental.pallas import tpu as pltpu
from jax.sharding import PartitionSpec as P

TOP = 4
GRID_W = 64


norm_eps = 1e-06
rope_theta = 10000.0
clamp_limit = 7.0
swish_alpha = 1.702


def rope_tables(positions, head_size):
    row_index = (positions // GRID_W).astype(jnp.float32)
    col_index = (positions % GRID_W).astype(jnp.float32)
    freq_count = head_size // 4
    inverse = rope_theta ** (-jnp.arange(freq_count, dtype=jnp.float32) / freq_count)
    angles = jnp.stack([row_index[:, None] * inverse, col_index[:, None] * inverse], axis=1)
    return (jnp.cos(angles), jnp.sin(angles))


def scale_rows(array_in, gain_vec):
    return (
        array_in
        * lax.rsqrt(jnp.mean(array_in * array_in, axis=-1, keepdims=True) + norm_eps)
        * gain_vec
    )


MESH = pl.DeviceIdType.MESH
NZ, NX = 8, 4
PIECE = 128


def attention_part(q_ref, kv_ref, wo_hbm, residual_ref, mix_ref, pre_ref, middle_ref, normed_ref, meet,
                     buf, qbuf, m_ref, l_ref, acc, obuf, heads, wo, pbuf, pin,
                     rsem, qsem, asem, zup, zdn, bup, bdn, bxp, bxm, bfw, dsem, osem, psend, precv, wsem):
    sp = lax.axis_index("sp")
    t = lax.axis_index("tp")
    load = pltpu.make_async_copy(wo_hbm, wo, wsem)
    load.start()
    core = lax.rem(sp, 2)
    chip = lax.div(sp, 2)
    x = lax.rem(chip, NX)
    z = lax.div(chip, NX)

    def dev(zz, xx, cc):
        return {"sp": (lax.rem(zz + 2 * NZ, NZ) * NX + lax.rem(xx + 2 * NX, NX)) * 2 + cc}

    def slot(kind, zz, xx):
        return kind * (NZ * NX) + lax.rem(zz + 2 * NZ, NZ) * NX + lax.rem(xx + 2 * NX, NX)

    partner = dev(z, x, 1 - core)
    z_up, z_dn = dev(z + 1, x, core), dev(z - 1, x, core)
    x_up, x_dn, x_far = dev(z, x + 1, core), dev(z, x - 1, core), dev(z, x + 2, core)

    mine = core * (NZ * NX) + chip
    buf[mine] = kv_ref[core]
    qbuf[pl.ds(pl.multiple_of(core * 512, 512), 512), :] = q_ref[core]
    m_ref[...] = jnp.full(m_ref.shape, -jnp.inf, jnp.float32)
    l_ref[...] = jnp.zeros(l_ref.shape, jnp.float32)
    acc[...] = jnp.zeros(acc.shape, jnp.float32)

    tp_peers = [lax.rem(t + d, 4) for d in (2, 1, 3)]
    meet()

    def move(at, sem, to):
        return pltpu.make_async_remote_copy(
            src_ref=buf.at[at], dst_ref=buf.at[at], send_sem=sem, recv_sem=rsem.at[at], device_id=to, device_id_type=MESH
        )

    def send(at, sem, to):
        move(at, sem, to).start()

    def arrive(at):
        move(at, dsem.at[0], partner).wait_recv()

    def done(sem):
        move(0, sem, partner).wait_send()

    swap_kv = pltpu.make_async_remote_copy(
        src_ref=kv_ref.at[1 - core], dst_ref=buf.at[(1 - core) * 0 + core * (NZ * NX) + chip], send_sem=dsem.at[0],
        recv_sem=rsem.at[core * (NZ * NX) + chip], device_id=partner, device_id_type=MESH,
    )
    swap_q = pltpu.make_async_remote_copy(
        src_ref=q_ref.at[1 - core], dst_ref=qbuf.at[pl.ds(pl.multiple_of(core * 512, 512), 512), :], send_sem=dsem.at[1],
        recv_sem=qsem, device_id=partner, device_id_type=MESH,
    )
    swap_kv.start()
    swap_q.start()
    arrive((1 - core) * (NZ * NX) + chip)

    def attend(slots):
        keys = jnp.concatenate([buf[s, 0] for s in slots], axis=0)
        vals = jnp.concatenate([buf[s, 1] for s in slots], axis=1)
        for tile in range(4):
            cols = slice(tile * 256, tile * 256 + 256)
            scores = lax.dot_general(keys, qbuf[cols, :], (((1,), (1,)), ((), ())), preferred_element_type=jnp.float32)
            before = m_ref[:, cols]
            now = jnp.maximum(before, jnp.max(scores, axis=0, keepdims=True))
            shrink = jnp.exp(before - now)
            unnorm = jnp.exp(scores - now)
            l_ref[:, cols] = l_ref[:, cols] * shrink + jnp.sum(unnorm, axis=0, keepdims=True)
            acc[:, cols] = acc[:, cols] * shrink + jnp.dot(
                vals, unnorm.astype(jnp.bfloat16), preferred_element_type=jnp.float32
            )
            m_ref[:, cols] = now

    A, B = 0, 1
    own_a, own_b = slot(A, z, x), slot(B, z, x)
    send(own_b, bup.at[0], z_up)
    send(own_b, bdn.at[0], z_dn)
    send(own_a, asem.at[0], x_up)
    send(own_a, asem.at[1], x_dn)
    send(own_a, zup.at[0], z_up)
    send(own_a, zdn.at[0], z_dn)
    send(own_a, asem.at[2], x_far)
    send(own_b, bxp.at[0], x_up)
    send(own_b, bxm.at[0], x_dn)
    ready = [own_a, own_b]

    def work(least=4):
        if len(ready) >= least:
            group = ready[:4]
            del ready[:4]
            attend(group)

    def lines_b(r):
        lo, hi = slot(B, z - r, x), slot(B, z + r, x)
        arrive(lo)
        if r < 4:
            send(lo, bup.at[r], z_up)
        send(lo, bxp.at[2 * r - 1], x_up)
        send(lo, bxm.at[2 * r - 1], x_dn)
        ready.append(lo)
        if r < 4:
            arrive(hi)
            if r < 3:
                send(hi, bdn.at[r], z_dn)
            send(hi, bxp.at[2 * r], x_up)
            send(hi, bxm.at[2 * r], x_dn)
            ready.append(hi)

    def lines_a(r, j):
        lo, hi = slot(A, z - r, x + j), slot(A, z + r, x + j)
        arrive(lo)
        if r < 3 or (r == 3 and j in (0, 1)):
            send(lo, zup.at[r * 4 + j], z_up)
        if 0 < r < 4:
            ready.append(lo)
            arrive(hi)
        if r < 3 or (r == 3 and j in (2, 3)):
            send(hi, zdn.at[r * 4 + j], z_dn)
        ready.append(hi)

    def across(r):
        if r > 0:
            at = slot(B, z - r, x - 1)
            arrive(at)
            send(at, bfw.at[2 * r - 1], x_up)
            ready.append(at)
        if r < 4:
            at = slot(B, z + r, x + 1)
            arrive(at)
            send(at, bfw.at[2 * r], x_dn)
            ready.append(at)
        if r > 0:
            at = slot(B, z - r, x + 1)
            arrive(at)
            ready.append(at)
        if r < 4:
            at = slot(B, z + r, x - 1)
            arrive(at)
            ready.append(at)

    def far(r):
        for at in {0: [slot(B, z, x + 2)], 4: [slot(B, z + 4, x + 2)]}.get(r, [slot(B, z - r, x + 2), slot(B, z + r, x + 2)]):
            arrive(at)
            ready.append(at)

    swap_q.wait_recv()
    lines_a(0, 1)
    work()
    lines_a(0, 3)
    work()
    lines_a(0, 2)
    work()
    lines_b(1)
    work()
    lines_a(1, 0)
    work()
    lines_a(1, 1)
    work()
    across(0)
    work()
    lines_b(2)
    work()
    lines_a(1, 3)
    work()
    lines_a(1, 2)
    work()
    across(1)
    work()
    far(0)
    work()
    lines_a(2, 0)
    work()
    lines_a(2, 1)
    work()
    lines_b(3)
    work()
    across(2)
    work()
    far(1)
    work()
    lines_a(2, 3)
    work()
    lines_a(2, 2)
    work()
    lines_b(4)
    work()
    lines_a(3, 0)
    work()
    lines_a(3, 1)
    work()
    across(3)
    work()
    far(2)
    work()
    lines_a(3, 3)
    work()
    lines_a(3, 2)
    work()
    across(4)
    work()
    far(3)
    work()
    lines_a(4, 0)
    work()
    lines_a(4, 1)
    work()
    far(4)
    work()
    lines_a(4, 3)
    work()
    lines_a(4, 2)
    work()
    while ready:
        work(1)

    def heads_of(which):
        cols = pl.ds(pl.multiple_of(which * 512, 512), 512)
        return (acc[:, cols] / l_ref[:, cols]).astype(jnp.bfloat16)

    theirs = heads_of(1 - core)
    obuf[2] = theirs
    own = heads_of(core)
    obuf[core] = own
    swap_o = pltpu.make_async_remote_copy(
        src_ref=obuf.at[2], dst_ref=obuf.at[core], send_sem=osem.at[0], recv_sem=osem.at[1], device_id=partner, device_id_type=MESH
    )
    swap_o.start()

    def stack_heads(g):
        for h in range(4):
            cols = pl.ds(pl.multiple_of(g * 512 + h * 128, 128), 128)
            heads[:, cols] = obuf[g, :, h * 128 : h * 128 + 128].T

    stack_heads(core)
    load.wait()
    swap_o.wait()
    stack_heads(1 - core)
    for cut in range(4):
        cols = slice(cut * 512, cut * 512 + 512)
        part = jnp.dot(heads[...], wo[:, cols], preferred_element_type=jnp.float32).astype(jnp.bfloat16)
        for owner in range(4):
            pbuf[owner, :, cols] = part[owner * 32 : owner * 32 + 32]
    gives = [
        pltpu.make_async_remote_copy(
            src_ref=pbuf.at[peer], dst_ref=pin.at[i], send_sem=psend.at[i], recv_sem=precv.at[i], device_id={"tp": peer},
            device_id_type=MESH,
        )
        for i, peer in enumerate(tp_peers)
    ]
    for give in gives:
        give.start()
    for i in range(3):
        done(asem.at[i])
    for i in range(4):
        done(bup.at[i])
        for j in range(4):
            if i < 3 or j in (0, 1):
                done(zup.at[i * 4 + j])
            if i < 3 or j in (2, 3):
                done(zdn.at[i * 4 + j])
    for i in range(3):
        done(bdn.at[i])
    for i in range(8):
        done(bxp.at[i])
        done(bxm.at[i])
        done(bfw.at[i])
    swap_kv.wait_send()
    swap_q.wait_send()
    for give in gives:
        give.wait()
    projected = pbuf[t].astype(jnp.float32)
    for i in range(3):
        projected = projected + pin[i].astype(jnp.float32)
    middle = residual_ref[...].astype(jnp.float32) + scale_rows(projected, mix_ref[...])
    middle_ref[...] = middle
    normed_ref[...] = scale_rows(middle, pre_ref[...]).astype(jnp.bfloat16)


GROUP_ORDER = (0, 1, 7, 2, 6, 3, 5, 4)
VIA_UP = (3, 6, 1, 0)
VIA_DN = (4, 5, 2, 7)


def experts_part(normed_ref, info_ref, middle_ref, gain_ref, loads, out_ref, others, column,
                 toks, infos, msgs, rows, act, part, mid, fin, ret, mixs, wg, wu, wd,
                   isend, irecv, tsend, trecv, msend, mrecv, gup, gdn, gfw, grecv, s_first, s_direct, s_mid, midrecv, finrecv,
                   rsend, rrecv, xsem):
    sp = lax.axis_index("sp")
    t = lax.axis_index("tp")
    core = lax.rem(sp, 2)
    chip = lax.div(sp, 2)
    x = lax.rem(chip, NX)
    z = lax.div(chip, NX)
    t_up, t_dn, t_far = lax.rem(t + 1, 4), lax.rem(t + 3, 4), lax.rem(t + 2, 4)

    def chip_at(dz, dx):
        return lax.rem(z + dz, NZ) * NX + lax.rem(x + dx, NX)

    def plane(which):
        return {"sp": which * 2 + core}

    partner = {"sp": chip * 2 + 1 - core}
    up, dn = {"tp": t_up}, {"tp": t_dn}

    toks[z, core] = normed_ref[...]
    infos[z, core] = info_ref[...]

    column = [{"sp": to} for to in column]

    def remote(src, dst, send_sem, recv_sem, to):
        return pltpu.make_async_remote_copy(
            src_ref=src, dst_ref=dst, send_sem=send_sem, recv_sem=recv_sem, device_id=to, device_id_type=MESH
        )

    z_up, z_dn = plane(chip_at(1, 0)), plane(chip_at(NZ - 1, 0))
    for i, to in enumerate((partner, z_up, z_dn)):
        remote(normed_ref, toks.at[z, core], tsend.at[i], trecv.at[z * 2 + core], to).start()
        if i == 0:
            remote(info_ref, infos.at[z, core], isend.at[0], irecv.at[z * 2 + core], partner).start()
    column += [plane(chip_at(dz, 0)) for dz in range(1, NZ)]
    for i, to in enumerate(column):
        remote(info_ref, infos.at[z, core], isend.at[1 + i], irecv.at[z * 2 + core], to).start()

    def wanted(count, first):
        row = lax.broadcasted_iota(jnp.int32, (count, 128), 0)
        lane = lax.broadcasted_iota(jnp.int32, (count, 128), 1)
        expert = (first + row // 8) * 2 + core
        slot_id = expert * 4 + row % 4
        return jnp.where((row // 4) % 2 == lane // 32, slot_id, -1).astype(jnp.float32)

    here = wanted(32, z * NX)

    def hop(dz, i, to):
        zz = lax.rem(z + NZ - dz, NZ)
        remote(toks.at[zz, core], toks.at[zz, core], tsend.at[i], trecv.at[zz * 2 + core], to).start()

    def tokens_of(dz):
        zz = lax.rem(z + NZ - dz, NZ)
        if dz:
            remote(normed_ref, toks.at[zz, core], tsend.at[0], trecv.at[zz * 2 + core], partner).wait_recv()
            if dz in (1, 2, 3):
                hop(dz, 2 + dz, z_up)
            if dz in (7, 6):
                hop(dz, dz, z_dn)
            hop(dz, 7 + dz, partner)
            remote(info_ref, infos.at[zz, core], isend.at[0], irecv.at[zz * 2 + core], partner).wait_recv()
        remote(info_ref, infos.at[zz, 1 - core], isend.at[0], irecv.at[zz * 2 + 1 - core], partner).wait_recv()
        remote(normed_ref, toks.at[zz, 1 - core], tsend.at[0], trecv.at[zz * 2 + 1 - core], partner).wait_recv()
        info = infos[zz, 0] + infos[zz, 1]
        disp = jnp.zeros((32, 128), jnp.float32)
        for k in range(4):
            disp = disp + jnp.where(info[k : k + 1] == here, 1.0, 0.0)
        disp = disp[:, :64].astype(jnp.bfloat16)
        data = jnp.concatenate([toks[zz, 0], toks[zz, 1]], axis=0)
        for cut in range(2):
            cols = slice(cut * 1024, cut * 1024 + 1024)
            msgs[zz, :, :, cols] = (
                jnp.dot(disp, data[:, cols], preferred_element_type=jnp.float32).astype(jnp.bfloat16).reshape(4, 8, 1024)
            )
        rows[t, zz * NX + x] = msgs[zz, x]
        for i, dx in enumerate((1, 3, 2)):
            to = lax.rem(x + dx, NX)
            remote(
                msgs.at[zz, to], rows.at[t, zz * NX + x], msend.at[dz * 3 + i], mrecv.at[zz * NX + x], plane(chip_at(0, dx))
            ).start()

    def chunk_at(which, dz):
        first = lax.rem(z + NZ - dz, NZ) * NX
        return rows.at[which, pl.ds(first, NX)]

    def give(dz, sem, to):
        ref = chunk_at(t, dz)
        return remote(ref, ref, sem, grecv.at[t * 8 + dz], to)

    def take(which, dz):
        ref = chunk_at(which, dz)
        remote(ref, ref, gup.at[0], grecv.at[which * 8 + dz], up).wait_recv()

    def hand(which, dz, to):
        ref = chunk_at(which, dz)
        return remote(ref, ref, gfw.at[dz], grecv.at[which * 8 + dz], to)

    def relay(dz):
        take(t_dn, dz)
        if dz in VIA_UP:
            hand(t_dn, dz, up).start()
        take(t_up, dz)
        if dz in VIA_DN:
            hand(t_up, dz, dn).start()

    def spread(dz):
        zz = lax.rem(z + NZ - dz, NZ)
        for dx in (1, 3, 2):
            source = zz * NX + lax.rem(x + dx, NX)
            remote(msgs.at[0, 0], rows.at[t, source], msend.at[0], mrecv.at[source], partner).wait_recv()
        give(dz, gup.at[dz], up).start()
        give(dz, gdn.at[dz], dn).start()

    for i in range(11):
        if i < 8:
            tokens_of(GROUP_ORDER[i])
        if 1 <= i < 9:
            spread(GROUP_ORDER[i - 1])
        if i >= 4:
            relay(GROUP_ORDER[i - 4])
    for load in loads:
        load.wait()

    def serve(which):
        data = rows[which].reshape(256, 2048)
        for f in range(2):
            cols = slice(f * 256, f * 256 + 256)
            gate = jnp.minimum(jnp.dot(data, wg[:, cols], preferred_element_type=jnp.float32), clamp_limit)
            lift = jnp.clip(jnp.dot(data, wu[:, cols], preferred_element_type=jnp.float32), -clamp_limit, clamp_limit)
            act[:, cols] = (gate * jax.nn.sigmoid(swish_alpha * gate) * (lift + 1.0)).astype(jnp.bfloat16)
        for cut in range(8):
            cols = slice(cut * 256, cut * 256 + 256)
            part[which, :, :, cols] = (
                jnp.dot(act[...], wd[:, cols], preferred_element_type=jnp.float32).astype(jnp.bfloat16).reshape(32, 8, 256)
            )

    def group(dz):
        return pl.ds(lax.rem(z + NZ - dz, NZ) * NX, NX)

    serve(t)
    relay(GROUP_ORDER[-1])

    def direct(k):
        a, b = group(VIA_DN[k]), group(VIA_UP[k])
        remote(part.at[t_up, a], fin.at[0, a], s_direct.at[k], finrecv.at[VIA_DN[k]], up).start()
        remote(part.at[t_dn, b], fin.at[1, b], s_direct.at[4 + k], finrecv.at[8 + VIA_UP[k]], dn).start()

    def first(k):
        a, b = group(VIA_UP[k]), group(VIA_DN[k])
        remote(part.at[t_far, a], mid.at[0, k], s_first.at[k], midrecv.at[k], up).start()
        remote(part.at[t_far, b], mid.at[1, k], s_first.at[4 + k], midrecv.at[4 + k], dn).start()

    def middle_sum(k):
        for way, (dzs, owner, to) in enumerate(((VIA_UP, t_up, up), (VIA_DN, t_dn, dn))):
            where = group(dzs[k])
            remote(part.at[owner, where], mid.at[way, k], s_first.at[0], midrecv.at[way * 4 + k], up).wait_recv()
            total = part[owner, where].astype(jnp.float32) + mid[way, k].astype(jnp.float32)
            part[owner, where] = total.astype(jnp.bfloat16)
            remote(part.at[owner, where], fin.at[way, where], s_mid.at[way * 4 + k], finrecv.at[way * 8 + dzs[k]], to).start()

    def settle(k):
        for dz in (VIA_UP[k], VIA_DN[k]):
            where = group(dz)
            for way in range(2):
                remote(part.at[t, where], fin.at[way, where], s_first.at[0], finrecv.at[way * 8 + dz], up).wait_recv()
            total = part[t, where].astype(jnp.float32) + fin[0, where].astype(jnp.float32) + fin[1, where].astype(jnp.float32)
            part[t, where] = total.astype(jnp.bfloat16)
            for dx in (2, 1, 3, 0):
                to = chip_at(NZ - dz, dx)
                if (dz, dx) != (0, 0):
                    remote(part.at[t, to], ret.at[chip], rsend.at[to], rrecv.at[chip], plane(to)).start()

    serve(t_up)
    serve(t_dn)
    direct(0)
    direct(1)
    for dz in GROUP_ORDER:
        take(t_far, dz)
    serve(t_far)
    first(0)
    first(1)
    middle_sum(0)
    first(2)
    middle_sum(1)
    direct(2)
    settle(0)
    first(3)
    middle_sum(2)
    direct(3)
    settle(1)
    middle_sum(3)
    settle(2)
    settle(3)
    ret[chip] = part[t, chip]
    for dz, dx in others:
        source = chip_at(dz, dx)
        remote(part.at[t, 0], ret.at[source], rsend.at[0], rrecv.at[source], partner).wait_recv()
    info = infos[z, 0] + infos[z, 1]
    everywhere = wanted(256, 0)
    weight = jnp.zeros((256, 128), jnp.float32)
    for k in range(4):
        weight = weight + jnp.where(info[k : k + 1] == everywhere, info[4 + k : 5 + k], 0.0)
    weight = weight.T[:64]
    coarse = weight.astype(jnp.bfloat16)
    fine = (weight - coarse.astype(jnp.float32)).astype(jnp.bfloat16)
    for cut in range(4):
        cols = slice(cut * 512, cut * 512 + 512)
        came = ret[:, :, cols].reshape(256, 512)
        mixed = jnp.dot(coarse, came, preferred_element_type=jnp.float32) + jnp.dot(
            fine, came, preferred_element_type=jnp.float32
        )
        mixs[0, :, cols] = mixed[:32]
        mixs[1, :, cols] = mixed[32:]
    swap_mix = remote(mixs.at[1 - core], mixs.at[2], xsem.at[0], xsem.at[1], partner)
    swap_mix.start()

    def sent(src, sem):
        remote(src, src, sem, xsem.at[1], partner).wait_send()

    for i in range(15):
        sent(toks.at[0, 0], tsend.at[i])
        sent(infos.at[0, 0], isend.at[i])
    for i in range(24):
        sent(msgs.at[0, 0], msend.at[i])

    for dz, dx in others:
        to = chip_at(dz, dx)
        sent(msgs.at[0, 0], rsend.at[to])
    for i in range(8):
        for sems in (gup, gdn, gfw, s_first, s_direct, s_mid):
            sent(mid.at[0, 0], sems.at[i])
    swap_mix.wait()
    mixture = mixs[core] + mixs[2]
    scale = lax.rsqrt(jnp.mean(mixture * mixture, axis=-1, keepdims=True) + norm_eps)
    out_ref[...] = (middle_ref[...] + mixture * scale * gain_ref[...]).astype(jnp.bfloat16)


ATTENTION_ITEMS = 25


def prepare(q_raw, k_raw, v_turned, table_ref, qgain_ref, kgain_ref, q_wide, k_wide, q_two, kv_two):
    cosine, sine = table_ref[0], table_ref[1]
    second = (lax.broadcasted_iota(jnp.int32, (128, 128), 1) // 32) % 2 == 1

    def turned(rows, gain):
        scaled = scale_rows(rows, gain)
        other = jnp.where(second, pltpu.roll(scaled, 32, 1), pltpu.roll(scaled, 96, 1))
        return scaled * cosine + other * sine

    k_wide[...] = k_raw[...].astype(jnp.float32)
    q_wide[...] = q_raw[...].astype(jnp.float32)
    for g in range(2):
        kv_two[g, 0] = turned(k_wide[pl.ds(g, 128, stride=2), :], kgain_ref[...]).astype(jnp.bfloat16)
        kv_two[g, 1] = v_turned[g]
        for h in range(4):
            rows = q_wide[pl.ds(g * 4 + h, 128, stride=8), :]
            q_two[g, h * 128 : h * 128 + 128, :] = (turned(rows, qgain_ref[...]) * 128 ** (-0.5)).astype(jnp.bfloat16)


def fill_info(routes_ref, lists_ref, info, core):
    chosen = routes_ref[...].astype(jnp.float32)
    lists = lists_ref[...]
    row = lax.broadcasted_iota(jnp.int32, (32, 128), 0)
    lane = lax.broadcasted_iota(jnp.int32, (32, 128), 1)
    before = row < lane
    slots = []
    for k in range(4):
        rank = jnp.zeros((1, 128), jnp.float32)
        for other in range(4):
            same = (chosen[:, other : other + 1] == lists[k : k + 1]) & before
            rank = rank + jnp.sum(jnp.where(same, 1.0, 0.0), axis=0, keepdims=True)
        slots.append(lists[k : k + 1] * 4.0 + rank)
    both = jnp.concatenate(slots + [lists[4:]], axis=0)
    both = jnp.where(lax.broadcasted_iota(jnp.int32, (8, 128), 1) < 32, both, 0.0)
    info[...] = jnp.where(core == 0, both, pltpu.roll(both, 32, 1))


def layer_kernel(q_raw, k_raw, v_turned, table_ref, qgain_ref, kgain_ref, routes_ref, lists_ref, wo_hbm, residual_ref, mix_ref,
                 pre_ref, gain_ref, wg_hbm, wu_hbm, wd_hbm, out_ref, *rest):
    middle, normed, wsem, q_wide, k_wide, q_ref, kv_ref, info_ref = rest[:8]
    attention_items = rest[8 : 8 + ATTENTION_ITEMS]
    expert_items = rest[8 + ATTENTION_ITEMS :]
    wg, wu, wd = expert_items[10:13]
    sp = lax.axis_index("sp")
    t = lax.axis_index("tp")
    core = lax.rem(sp, 2)
    chip = lax.div(sp, 2)
    x = lax.rem(chip, NX)
    z = lax.div(chip, NX)

    def chip_at(dz, dx):
        return lax.rem(z + dz, NZ) * NX + lax.rem(x + dx, NX)

    others = [(dz, dx) for dz in GROUP_ORDER for dx in (0, 1, 3, 2) if (dz, dx) != (0, 0)]
    column = [chip_at(dz, 0) * 2 + 1 - core for dz in range(1, NZ)]
    loads = [pltpu.make_async_copy(src, dst, wsem.at[i]) for i, (src, dst) in enumerate(((wg_hbm, wg), (wu_hbm, wu), (wd_hbm, wd)))]

    def meet():
        barrier = pltpu.get_barrier_semaphore()
        peers = [{"sp": chip * 2 + 1 - core}] + [{"tp": lax.rem(t + d, 4)} for d in (1, 2, 3)]
        peers += [{"sp": chip_at(dz, dx) * 2 + core} for dz, dx in others] + [{"sp": to} for to in column]
        for peer in peers:
            pl.semaphore_signal(barrier, inc=1, device_id=peer, device_id_type=MESH)
        pl.semaphore_wait(barrier, len(peers))

    for load in loads:
        load.start()
    prepare(q_raw, k_raw, v_turned, table_ref, qgain_ref, kgain_ref, q_wide, k_wide, q_ref, kv_ref)
    fill_info(routes_ref, lists_ref, info_ref, core)
    attention_part(q_ref, kv_ref, wo_hbm, residual_ref, mix_ref, pre_ref, middle, normed, meet, *attention_items)
    experts_part(normed, info_ref, middle, gain_ref, loads, out_ref, others, column, *expert_items)


def layer(queries, keys, values, tables, q_gain, k_gain, routes, lists, w_out, residual, gain_mix, gain_pre, gain_moe, w_gate, w_up, w_down):
    whole, apart = pl.BlockSpec(memory_space=pltpu.VMEM), pl.BlockSpec(memory_space=pltpu.MemorySpace.HBM)
    dma, bf16, f32 = pltpu.SemaphoreType.DMA, jnp.bfloat16, jnp.float32
    attention_scratch = [
        pltpu.VMEM((64, 2, PIECE, 128), bf16),
        pltpu.VMEM((1024, 128), bf16),
        pltpu.VMEM((1, 1024), f32),
        pltpu.VMEM((1, 1024), f32),
        pltpu.VMEM((128, 1024), f32),
        pltpu.VMEM((3, 128, 512), bf16),
        pltpu.VMEM((128, 1024), bf16),
        pltpu.VMEM((1024, 2048), bf16),
        pltpu.VMEM((4, 32, 2048), bf16),
        pltpu.VMEM((3, 32, 2048), bf16),
    ] + [dma((n,)) if n else dma for n in (64, 0, 3, 16, 16, 4, 4, 8, 8, 8, 2, 2, 3, 3, 0)]
    expert_scratch = [
        pltpu.VMEM((8, 2, 32, 2048), bf16),
        pltpu.VMEM((8, 2, 8, 128), f32),
        pltpu.VMEM((8, 4, 8, 2048), bf16),
        pltpu.VMEM((4, 32, 8, 2048), bf16),
        pltpu.VMEM((256, 512), bf16),
        pltpu.VMEM((4, 32, 8, 2048), bf16),
        pltpu.VMEM((2, 4, 4, 8, 2048), bf16),
        pltpu.VMEM((2, 32, 8, 2048), bf16),
        pltpu.VMEM((32, 8, 2048), bf16),
        pltpu.VMEM((3, 32, 2048), f32),
        pltpu.VMEM((2048, 512), bf16),
        pltpu.VMEM((2048, 512), bf16),
        pltpu.VMEM((512, 2048), bf16),
    ] + [dma((n,)) for n in (15, 16, 15, 16, 24, 32, 8, 8, 8, 32, 8, 8, 8, 8, 16, 32, 32, 2)]
    return pl.pallas_call(
        layer_kernel,
        out_shape=jax.ShapeDtypeStruct((32, 2048), bf16),
        in_specs=[whole] * 8 + [apart] + [whole] * 4 + [apart] * 3,
        out_specs=whole,
        scratch_shapes=[
            pltpu.VMEM((32, 2048), f32),
            pltpu.VMEM((32, 2048), bf16),
            dma((3,)),
            pltpu.VMEM((1024, 128), f32),
            pltpu.VMEM((256, 128), f32),
            pltpu.VMEM((2, 512, 128), bf16),
            pltpu.VMEM((2, 2, 128, 128), bf16),
            pltpu.VMEM((8, 128), f32),
        ]
        + attention_scratch
        + expert_scratch,
        compiler_params=pltpu.CompilerParams(collective_id=0, has_side_effects=True, vmem_limit_bytes=52 << 20),
        name="layer",
    )(queries, keys, values, tables, q_gain, k_gain, routes, lists, w_out, residual, gain_mix, gain_pre, gain_moe, w_gate, w_up, w_down)


def on_device(
    queries,
    keys,
    values,
    q_gain,
    k_gain,
    w_out,
    residual,
    gain_mix,
    gain_pre,
    routes,
    route_weights,
    w_gate,
    w_up,
    w_down,
    gain_moe,
):
    tok_rows, head_local, head_size = queries.shape
    kv_local = keys.shape[1]
    positions = lax.axis_index("sp") * tok_rows + jnp.arange(tok_rows, dtype=jnp.int32)
    cosine_table, sine_table = rope_tables(positions, head_size)
    cosines = jnp.stack([cosine_table, cosine_table], axis=2).reshape(tok_rows, head_size)
    sines = jnp.stack([-sine_table, sine_table], axis=2).reshape(tok_rows, head_size)
    width = residual.shape[1]
    lists = jnp.concatenate([routes.T.astype(jnp.float32), route_weights.T], axis=0)
    return layer(
        queries.reshape(tok_rows * head_local, head_size),
        keys.reshape(tok_rows * kv_local, head_size),
        values.transpose(1, 2, 0),
        jnp.stack([cosines, sines]),
        q_gain.reshape(1, head_size),
        k_gain.reshape(1, head_size),
        routes,
        jnp.pad(lists, ((0, 0), (0, 128 - lists.shape[1]))),
        w_out,
        residual,
        gain_mix.reshape(1, width),
        gain_pre.reshape(1, width),
        gain_moe.reshape(1, width),
        w_gate[0],
        w_up[0],
        w_down[0],
    )


def solution(mesh):
    placed = (
        P("sp", "tp", None),
        P("sp", "tp", None),
        P("sp", "tp", None),
        P(),
        P(),
        P("tp", None),
        P(("sp", "tp"), None),
        P(),
        P(),
        P(("sp", "tp"), None),
        P(("sp", "tp"), None),
        P("sp", None, "tp"),
        P("sp", None, "tp"),
        P("sp", "tp", None),
        P(),
    )
    return jax.shard_map(
        on_device, mesh=mesh, in_specs=placed, out_specs=P(("sp", "tp"), None), check_vma=False
    )
```

```python
import jax
import jax.numpy as jnp
from jax import lax
from jax.experimental import pallas as pl
from jax.experimental.pallas import tpu as pltpu
from jax.sharding import PartitionSpec as P

TOP = 4
GRID_W = 64


norm_eps = 1e-06
rope_theta = 10000.0
clamp_limit = 7.0
swish_alpha = 1.702


def rope_tables(positions, head_size):
    row_index = (positions // GRID_W).astype(jnp.float32)
    col_index = (positions % GRID_W).astype(jnp.float32)
    freq_count = head_size // 4
    inverse = rope_theta ** (-jnp.arange(freq_count, dtype=jnp.float32) / freq_count)
    angles = jnp.stack([row_index[:, None] * inverse, col_index[:, None] * inverse], axis=1)
    return (jnp.cos(angles), jnp.sin(angles))


def scale_rows(array_in, gain_vec):
    return (
        array_in
        * lax.rsqrt(jnp.mean(array_in * array_in, axis=-1, keepdims=True) + norm_eps)
        * gain_vec
    )


MESH = pl.DeviceIdType.MESH
NZ, NX = 8, 4
PIECE = 128


def attention_part(q_ref, kv_ref, wo_hbm, residual_ref, mix_ref, pre_ref, middle_ref, normed_ref, meet,
                     buf, qbuf, m_ref, l_ref, acc, obuf, heads, wo, pbuf, pin,
                     rsem, qsem, asem, zup, zdn, bup, bdn, bxp, bxm, bfw, dsem, osem, psend, precv, wsem):
    sp = lax.axis_index("sp")
    t = lax.axis_index("tp")
    load = pltpu.make_async_copy(wo_hbm, wo, wsem)
    load.start()
    core = lax.rem(sp, 2)
    chip = lax.div(sp, 2)
    x = lax.rem(chip, NX)
    z = lax.div(chip, NX)

    def dev(zz, xx, cc):
        return {"sp": (lax.rem(zz + 2 * NZ, NZ) * NX + lax.rem(xx + 2 * NX, NX)) * 2 + cc}

    def slot(kind, zz, xx):
        return kind * (NZ * NX) + lax.rem(zz + 2 * NZ, NZ) * NX + lax.rem(xx + 2 * NX, NX)

    partner = dev(z, x, 1 - core)
    z_up, z_dn = dev(z + 1, x, core), dev(z - 1, x, core)
    x_up, x_dn, x_far = dev(z, x + 1, core), dev(z, x - 1, core), dev(z, x + 2, core)

    mine = core * (NZ * NX) + chip
    buf[mine] = kv_ref[core]
    qbuf[pl.ds(pl.multiple_of(core * 512, 512), 512), :] = q_ref[core]
    m_ref[...] = jnp.full(m_ref.shape, -jnp.inf, jnp.float32)
    l_ref[...] = jnp.zeros(l_ref.shape, jnp.float32)
    acc[...] = jnp.zeros(acc.shape, jnp.float32)

    tp_peers = [lax.rem(t + d, 4) for d in (2, 1, 3)]
    meet()

    def move(at, sem, to):
        return pltpu.make_async_remote_copy(
            src_ref=buf.at[at], dst_ref=buf.at[at], send_sem=sem, recv_sem=rsem.at[at], device_id=to, device_id_type=MESH
        )

    def send(at, sem, to):
        move(at, sem, to).start()

    def arrive(at):
        move(at, dsem.at[0], partner).wait_recv()

    def done(sem):
        move(0, sem, partner).wait_send()

    swap_kv = pltpu.make_async_remote_copy(
        src_ref=kv_ref.at[1 - core], dst_ref=buf.at[(1 - core) * 0 + core * (NZ * NX) + chip], send_sem=dsem.at[0],
        recv_sem=rsem.at[core * (NZ * NX) + chip], device_id=partner, device_id_type=MESH,
    )
    swap_q = pltpu.make_async_remote_copy(
        src_ref=q_ref.at[1 - core], dst_ref=qbuf.at[pl.ds(pl.multiple_of(core * 512, 512), 512), :], send_sem=dsem.at[1],
        recv_sem=qsem, device_id=partner, device_id_type=MESH,
    )
    swap_kv.start()
    swap_q.start()
    arrive((1 - core) * (NZ * NX) + chip)

    def attend(slots):
        keys = jnp.concatenate([buf[s, 0] for s in slots], axis=0)
        vals = jnp.concatenate([buf[s, 1] for s in slots], axis=1)
        for tile in range(4):
            cols = slice(tile * 256, tile * 256 + 256)
            scores = lax.dot_general(keys, qbuf[cols, :], (((1,), (1,)), ((), ())), preferred_element_type=jnp.float32)
            before = m_ref[:, cols]
            now = jnp.maximum(before, jnp.max(scores, axis=0, keepdims=True))
            shrink = jnp.exp(before - now)
            unnorm = jnp.exp(scores - now)
            l_ref[:, cols] = l_ref[:, cols] * shrink + jnp.sum(unnorm, axis=0, keepdims=True)
            acc[:, cols] = acc[:, cols] * shrink + jnp.dot(
                vals, unnorm.astype(jnp.bfloat16), preferred_element_type=jnp.float32
            )
            m_ref[:, cols] = now

    A, B = 0, 1
    own_a, own_b = slot(A, z, x), slot(B, z, x)
    send(own_b, bup.at[0], z_up)
    send(own_b, bdn.at[0], z_dn)
    send(own_a, asem.at[0], x_up)
    send(own_a, asem.at[1], x_dn)
    send(own_a, zup.at[0], z_up)
    send(own_a, zdn.at[0], z_dn)
    send(own_a, asem.at[2], x_far)
    send(own_b, bxp.at[0], x_up)
    send(own_b, bxm.at[0], x_dn)
    ready = [own_a, own_b]

    def work(least=4):
        if len(ready) >= least:
            group = ready[:4]
            del ready[:4]
            attend(group)

    def lines_b(r):
        lo, hi = slot(B, z - r, x), slot(B, z + r, x)
        arrive(lo)
        if r < 4:
            send(lo, bup.at[r], z_up)
        send(lo, bxp.at[2 * r - 1], x_up)
        send(lo, bxm.at[2 * r - 1], x_dn)
        ready.append(lo)
        if r < 4:
            arrive(hi)
            if r < 3:
                send(hi, bdn.at[r], z_dn)
            send(hi, bxp.at[2 * r], x_up)
            send(hi, bxm.at[2 * r], x_dn)
            ready.append(hi)

    def lines_a(r, j):
        lo, hi = slot(A, z - r, x + j), slot(A, z + r, x + j)
        arrive(lo)
        if r < 3 or (r == 3 and j in (0, 1)):
            send(lo, zup.at[r * 4 + j], z_up)
        if 0 < r < 4:
            ready.append(lo)
            arrive(hi)
        if r < 3 or (r == 3 and j in (2, 3)):
            send(hi, zdn.at[r * 4 + j], z_dn)
        ready.append(hi)

    def across(r):
        if r > 0:
            at = slot(B, z - r, x - 1)
            arrive(at)
            send(at, bfw.at[2 * r - 1], x_up)
            ready.append(at)
        if r < 4:
            at = slot(B, z + r, x + 1)
            arrive(at)
            send(at, bfw.at[2 * r], x_dn)
            ready.append(at)
        if r > 0:
            at = slot(B, z - r, x + 1)
            arrive(at)
            ready.append(at)
        if r < 4:
            at = slot(B, z + r, x - 1)
            arrive(at)
            ready.append(at)

    def far(r):
        for at in {0: [slot(B, z, x + 2)], 4: [slot(B, z + 4, x + 2)]}.get(r, [slot(B, z - r, x + 2), slot(B, z + r, x + 2)]):
            arrive(at)
            ready.append(at)

    swap_q.wait_recv()
    lines_a(0, 1)
    work()
    lines_a(0, 3)
    work()
    lines_a(0, 2)
    work()
    lines_b(1)
    work()
    lines_a(1, 0)
    work()
    lines_a(1, 1)
    work()
    across(0)
    work()
    lines_b(2)
    work()
    lines_a(1, 3)
    work()
    lines_a(1, 2)
    work()
    across(1)
    work()
    far(0)
    work()
    lines_a(2, 0)
    work()
    lines_a(2, 1)
    work()
    lines_b(3)
    work()
    across(2)
    work()
    far(1)
    work()
    lines_a(2, 3)
    work()
    lines_a(2, 2)
    work()
    lines_b(4)
    work()
    lines_a(3, 0)
    work()
    lines_a(3, 1)
    work()
    across(3)
    work()
    far(2)
    work()
    lines_a(3, 3)
    work()
    lines_a(3, 2)
    work()
    across(4)
    work()
    far(3)
    work()
    lines_a(4, 0)
    work()
    lines_a(4, 1)
    work()
    far(4)
    work()
    lines_a(4, 3)
    work()
    lines_a(4, 2)
    work()
    while ready:
        work(1)

    def heads_of(which):
        cols = pl.ds(pl.multiple_of(which * 512, 512), 512)
        return (acc[:, cols] / l_ref[:, cols]).astype(jnp.bfloat16)

    theirs = heads_of(1 - core)
    obuf[2] = theirs
    own = heads_of(core)
    obuf[core] = own
    swap_o = pltpu.make_async_remote_copy(
        src_ref=obuf.at[2], dst_ref=obuf.at[core], send_sem=osem.at[0], recv_sem=osem.at[1], device_id=partner, device_id_type=MESH
    )
    swap_o.start()

    def stack_heads(g):
        for h in range(4):
            cols = pl.ds(pl.multiple_of(g * 512 + h * 128, 128), 128)
            heads[:, cols] = obuf[g, :, h * 128 : h * 128 + 128].T

    stack_heads(core)
    load.wait()
    swap_o.wait()
    stack_heads(1 - core)
    for cut in range(4):
        cols = slice(cut * 512, cut * 512 + 512)
        part = jnp.dot(heads[...], wo[:, cols], preferred_element_type=jnp.float32).astype(jnp.bfloat16)
        for owner in range(4):
            pbuf[owner, :, cols] = part[owner * 32 : owner * 32 + 32]
    gives = [
        pltpu.make_async_remote_copy(
            src_ref=pbuf.at[peer], dst_ref=pin.at[i], send_sem=psend.at[i], recv_sem=precv.at[i], device_id={"tp": peer},
            device_id_type=MESH,
        )
        for i, peer in enumerate(tp_peers)
    ]
    for give in gives:
        give.start()
    for i in range(3):
        done(asem.at[i])
    for i in range(4):
        done(bup.at[i])
        for j in range(4):
            if i < 3 or j in (0, 1):
                done(zup.at[i * 4 + j])
            if i < 3 or j in (2, 3):
                done(zdn.at[i * 4 + j])
    for i in range(3):
        done(bdn.at[i])
    for i in range(8):
        done(bxp.at[i])
        done(bxm.at[i])
        done(bfw.at[i])
    swap_kv.wait_send()
    swap_q.wait_send()
    for give in gives:
        give.wait()
    projected = pbuf[t].astype(jnp.float32)
    for i in range(3):
        projected = projected + pin[i].astype(jnp.float32)
    middle = residual_ref[...].astype(jnp.float32) + scale_rows(projected, mix_ref[...])
    middle_ref[...] = middle
    normed_ref[...] = scale_rows(middle, pre_ref[...]).astype(jnp.bfloat16)


GROUP_ORDER = (0, 1, 7, 2, 6, 3, 5, 4)
VIA_UP = (3, 6, 1, 0)
VIA_DN = (4, 5, 2, 7)


def experts_part(normed_ref, info_ref, middle_ref, gain_ref, loads, out_ref, others, column,
                 toks, infos, msgs, rows, act, part, mid, fin, ret, mixs, wg, wu, wd,
                   isend, irecv, tsend, trecv, msend, mrecv, gup, gdn, gfw, grecv, s_first, s_direct, s_mid, midrecv, finrecv,
                   rsend, rrecv, xsem):
    sp = lax.axis_index("sp")
    t = lax.axis_index("tp")
    core = lax.rem(sp, 2)
    chip = lax.div(sp, 2)
    x = lax.rem(chip, NX)
    z = lax.div(chip, NX)
    t_up, t_dn, t_far = lax.rem(t + 1, 4), lax.rem(t + 3, 4), lax.rem(t + 2, 4)

    def chip_at(dz, dx):
        return lax.rem(z + dz, NZ) * NX + lax.rem(x + dx, NX)

    def plane(which):
        return {"sp": which * 2 + core}

    partner = {"sp": chip * 2 + 1 - core}
    up, dn = {"tp": t_up}, {"tp": t_dn}

    toks[z, core] = normed_ref[...]
    infos[z, core] = info_ref[...]

    column = [{"sp": to} for to in column]

    def remote(src, dst, send_sem, recv_sem, to):
        return pltpu.make_async_remote_copy(
            src_ref=src, dst_ref=dst, send_sem=send_sem, recv_sem=recv_sem, device_id=to, device_id_type=MESH
        )

    z_up, z_dn = plane(chip_at(1, 0)), plane(chip_at(NZ - 1, 0))
    for i, to in enumerate((partner, z_up, z_dn)):
        remote(normed_ref, toks.at[z, core], tsend.at[i], trecv.at[z * 2 + core], to).start()
        if i == 0:
            remote(info_ref, infos.at[z, core], isend.at[0], irecv.at[z * 2 + core], partner).start()
    column += [plane(chip_at(dz, 0)) for dz in range(1, NZ)]
    for i, to in enumerate(column):
        remote(info_ref, infos.at[z, core], isend.at[1 + i], irecv.at[z * 2 + core], to).start()

    def wanted(count, first):
        row = lax.broadcasted_iota(jnp.int32, (count, 128), 0)
        lane = lax.broadcasted_iota(jnp.int32, (count, 128), 1)
        expert = (first + row // 8) * 2 + core
        slot_id = expert * 4 + row % 4
        return jnp.where((row // 4) % 2 == lane // 32, slot_id, -1).astype(jnp.float32)

    here = wanted(32, z * NX)

    def hop(dz, i, to):
        zz = lax.rem(z + NZ - dz, NZ)
        remote(toks.at[zz, core], toks.at[zz, core], tsend.at[i], trecv.at[zz * 2 + core], to).start()

    def tokens_of(dz):
        zz = lax.rem(z + NZ - dz, NZ)
        if dz:
            remote(normed_ref, toks.at[zz, core], tsend.at[0], trecv.at[zz * 2 + core], partner).wait_recv()
            if dz in (1, 2, 3):
                hop(dz, 2 + dz, z_up)
            if dz in (7, 6):
                hop(dz, dz, z_dn)
            hop(dz, 7 + dz, partner)
            remote(info_ref, infos.at[zz, core], isend.at[0], irecv.at[zz * 2 + core], partner).wait_recv()
        remote(info_ref, infos.at[zz, 1 - core], isend.at[0], irecv.at[zz * 2 + 1 - core], partner).wait_recv()
        remote(normed_ref, toks.at[zz, 1 - core], tsend.at[0], trecv.at[zz * 2 + 1 - core], partner).wait_recv()
        info = infos[zz, 0] + infos[zz, 1]
        disp = jnp.zeros((32, 128), jnp.float32)
        for k in range(4):
            disp = disp + jnp.where(info[k : k + 1] == here, 1.0, 0.0)
        disp = disp[:, :64].astype(jnp.bfloat16)
        data = jnp.concatenate([toks[zz, 0], toks[zz, 1]], axis=0)
        for cut in range(2):
            cols = slice(cut * 1024, cut * 1024 + 1024)
            msgs[zz, :, :, cols] = (
                jnp.dot(disp, data[:, cols], preferred_element_type=jnp.float32).astype(jnp.bfloat16).reshape(4, 8, 1024)
            )
        rows[t, zz * NX + x] = msgs[zz, x]
        for i, dx in enumerate((1, 3, 2)):
            to = lax.rem(x + dx, NX)
            remote(
                msgs.at[zz, to], rows.at[t, zz * NX + x], msend.at[dz * 3 + i], mrecv.at[zz * NX + x], plane(chip_at(0, dx))
            ).start()

    def chunk_at(which, dz):
        first = lax.rem(z + NZ - dz, NZ) * NX
        return rows.at[which, pl.ds(first, NX)]

    def give(dz, sem, to):
        ref = chunk_at(t, dz)
        return remote(ref, ref, sem, grecv.at[t * 8 + dz], to)

    def take(which, dz):
        ref = chunk_at(which, dz)
        remote(ref, ref, gup.at[0], grecv.at[which * 8 + dz], up).wait_recv()

    def hand(which, dz, to):
        ref = chunk_at(which, dz)
        return remote(ref, ref, gfw.at[dz], grecv.at[which * 8 + dz], to)

    def relay(dz):
        take(t_dn, dz)
        if dz in VIA_UP:
            hand(t_dn, dz, up).start()
        take(t_up, dz)
        if dz in VIA_DN:
            hand(t_up, dz, dn).start()

    def spread(dz):
        zz = lax.rem(z + NZ - dz, NZ)
        for dx in (1, 3, 2):
            source = zz * NX + lax.rem(x + dx, NX)
            remote(msgs.at[0, 0], rows.at[t, source], msend.at[0], mrecv.at[source], partner).wait_recv()
        give(dz, gup.at[dz], up).start()
        give(dz, gdn.at[dz], dn).start()

    for i in range(11):
        if i < 8:
            tokens_of(GROUP_ORDER[i])
        if 1 <= i < 9:
            spread(GROUP_ORDER[i - 1])
        if i >= 4:
            relay(GROUP_ORDER[i - 4])
    for load in loads:
        load.wait()

    def serve(which):
        data = rows[which].reshape(256, 2048)
        for f in range(2):
            cols = slice(f * 256, f * 256 + 256)
            gate = jnp.minimum(jnp.dot(data, wg[:, cols], preferred_element_type=jnp.float32), clamp_limit)
            lift = jnp.clip(jnp.dot(data, wu[:, cols], preferred_element_type=jnp.float32), -clamp_limit, clamp_limit)
            act[:, cols] = (gate * jax.nn.sigmoid(swish_alpha * gate) * (lift + 1.0)).astype(jnp.bfloat16)
        for cut in range(8):
            cols = slice(cut * 256, cut * 256 + 256)
            part[which, :, :, cols] = (
                jnp.dot(act[...], wd[:, cols], preferred_element_type=jnp.float32).astype(jnp.bfloat16).reshape(32, 8, 256)
            )

    def group(dz):
        return pl.ds(lax.rem(z + NZ - dz, NZ) * NX, NX)

    serve(t)
    relay(GROUP_ORDER[-1])

    def direct(k):
        a, b = group(VIA_DN[k]), group(VIA_UP[k])
        remote(part.at[t_up, a], fin.at[0, a], s_direct.at[k], finrecv.at[VIA_DN[k]], up).start()
        remote(part.at[t_dn, b], fin.at[1, b], s_direct.at[4 + k], finrecv.at[8 + VIA_UP[k]], dn).start()

    def first(k):
        a, b = group(VIA_UP[k]), group(VIA_DN[k])
        remote(part.at[t_far, a], mid.at[0, k], s_first.at[k], midrecv.at[k], up).start()
        remote(part.at[t_far, b], mid.at[1, k], s_first.at[4 + k], midrecv.at[4 + k], dn).start()

    def middle_sum(k):
        for way, (dzs, owner, to) in enumerate(((VIA_UP, t_up, up), (VIA_DN, t_dn, dn))):
            where = group(dzs[k])
            remote(part.at[owner, where], mid.at[way, k], s_first.at[0], midrecv.at[way * 4 + k], up).wait_recv()
            total = part[owner, where].astype(jnp.float32) + mid[way, k].astype(jnp.float32)
            part[owner, where] = total.astype(jnp.bfloat16)
            remote(part.at[owner, where], fin.at[way, where], s_mid.at[way * 4 + k], finrecv.at[way * 8 + dzs[k]], to).start()

    def settle(k):
        for dz in (VIA_UP[k], VIA_DN[k]):
            where = group(dz)
            for way in range(2):
                remote(part.at[t, where], fin.at[way, where], s_first.at[0], finrecv.at[way * 8 + dz], up).wait_recv()
            total = part[t, where].astype(jnp.float32) + fin[0, where].astype(jnp.float32) + fin[1, where].astype(jnp.float32)
            part[t, where] = total.astype(jnp.bfloat16)
            for dx in (2, 1, 3, 0):
                to = chip_at(NZ - dz, dx)
                if (dz, dx) != (0, 0):
                    remote(part.at[t, to], ret.at[chip], rsend.at[to], rrecv.at[chip], plane(to)).start()

    serve(t_up)
    serve(t_dn)
    direct(0)
    direct(1)
    for dz in GROUP_ORDER:
        take(t_far, dz)
    serve(t_far)
    first(0)
    first(1)
    middle_sum(0)
    first(2)
    middle_sum(1)
    direct(2)
    settle(0)
    first(3)
    middle_sum(2)
    direct(3)
    settle(1)
    middle_sum(3)
    settle(2)
    settle(3)
    ret[chip] = part[t, chip]
    for dz, dx in others:
        source = chip_at(dz, dx)
        remote(part.at[t, 0], ret.at[source], rsend.at[0], rrecv.at[source], partner).wait_recv()
    info = infos[z, 0] + infos[z, 1]
    everywhere = wanted(256, 0)
    weight = jnp.zeros((256, 128), jnp.float32)
    for k in range(4):
        weight = weight + jnp.where(info[k : k + 1] == everywhere, info[4 + k : 5 + k], 0.0)
    weight = weight.T[:64]
    coarse = weight.astype(jnp.bfloat16)
    fine = (weight - coarse.astype(jnp.float32)).astype(jnp.bfloat16)
    for cut in range(4):
        cols = slice(cut * 512, cut * 512 + 512)
        came = ret[:, :, cols].reshape(256, 512)
        mixed = jnp.dot(coarse, came, preferred_element_type=jnp.float32) + jnp.dot(
            fine, came, preferred_element_type=jnp.float32
        )
        mixs[0, :, cols] = mixed[:32]
        mixs[1, :, cols] = mixed[32:]
    swap_mix = remote(mixs.at[1 - core], mixs.at[2], xsem.at[0], xsem.at[1], partner)
    swap_mix.start()

    def sent(src, sem):
        remote(src, src, sem, xsem.at[1], partner).wait_send()

    for i in range(15):
        sent(toks.at[0, 0], tsend.at[i])
        sent(infos.at[0, 0], isend.at[i])
    for i in range(24):
        sent(msgs.at[0, 0], msend.at[i])

    for dz, dx in others:
        to = chip_at(dz, dx)
        sent(msgs.at[0, 0], rsend.at[to])
    for i in range(8):
        for sems in (gup, gdn, gfw, s_first, s_direct, s_mid):
            sent(mid.at[0, 0], sems.at[i])
    swap_mix.wait()
    mixture = mixs[core] + mixs[2]
    scale = lax.rsqrt(jnp.mean(mixture * mixture, axis=-1, keepdims=True) + norm_eps)
    out_ref[...] = (middle_ref[...] + mixture * scale * gain_ref[...]).astype(jnp.bfloat16)


ATTENTION_ITEMS = 25


def prepare(q_raw, k_raw, v_turned, table_ref, qgain_ref, kgain_ref, q_wide, k_wide, q_two, kv_two):
    cosine, sine = table_ref[0], table_ref[1]
    second = (lax.broadcasted_iota(jnp.int32, (128, 128), 1) // 32) % 2 == 1

    def turned(rows, gain):
        scaled = scale_rows(rows, gain)
        other = jnp.where(second, pltpu.roll(scaled, 32, 1), pltpu.roll(scaled, 96, 1))
        return scaled * cosine + other * sine

    k_wide[...] = k_raw[...].astype(jnp.float32)
    q_wide[...] = q_raw[...].astype(jnp.float32)
    for g in range(2):
        kv_two[g, 0] = turned(k_wide[pl.ds(g, 128, stride=2), :], kgain_ref[...]).astype(jnp.bfloat16)
        kv_two[g, 1] = v_turned[g]
        for h in range(4):
            rows = q_wide[pl.ds(g * 4 + h, 128, stride=8), :]
            q_two[g, h * 128 : h * 128 + 128, :] = (turned(rows, qgain_ref[...]) * 128 ** (-0.5)).astype(jnp.bfloat16)


def fill_info(routes_ref, lists_ref, info, core):
    chosen = routes_ref[...].astype(jnp.float32)
    lists = lists_ref[...]
    row = lax.broadcasted_iota(jnp.int32, (32, 128), 0)
    lane = lax.broadcasted_iota(jnp.int32, (32, 128), 1)
    before = row < lane
    slots = []
    for k in range(4):
        rank = jnp.zeros((1, 128), jnp.float32)
        for other in range(4):
            same = (chosen[:, other : other + 1] == lists[k : k + 1]) & before
            rank = rank + jnp.sum(jnp.where(same, 1.0, 0.0), axis=0, keepdims=True)
        slots.append(lists[k : k + 1] * 4.0 + rank)
    both = jnp.concatenate(slots + [lists[4:]], axis=0)
    both = jnp.where(lax.broadcasted_iota(jnp.int32, (8, 128), 1) < 32, both, 0.0)
    info[...] = jnp.where(core == 0, both, pltpu.roll(both, 32, 1))


def layer_kernel(q_raw, k_raw, v_turned, table_ref, qgain_ref, kgain_ref, routes_ref, lists_ref, wo_hbm, residual_ref, mix_ref,
                 pre_ref, gain_ref, wg_hbm, wu_hbm, wd_hbm, out_ref, *rest):
    middle, normed, wsem, q_wide, k_wide, q_ref, kv_ref, info_ref = rest[:8]
    attention_items = rest[8 : 8 + ATTENTION_ITEMS]
    expert_items = rest[8 + ATTENTION_ITEMS :]
    wg, wu, wd = expert_items[10:13]
    sp = lax.axis_index("sp")
    t = lax.axis_index("tp")
    core = lax.rem(sp, 2)
    chip = lax.div(sp, 2)
    x = lax.rem(chip, NX)
    z = lax.div(chip, NX)

    def chip_at(dz, dx):
        return lax.rem(z + dz, NZ) * NX + lax.rem(x + dx, NX)

    others = [(dz, dx) for dz in GROUP_ORDER for dx in (0, 1, 3, 2) if (dz, dx) != (0, 0)]
    column = [chip_at(dz, 0) * 2 + 1 - core for dz in range(1, NZ)]
    loads = [pltpu.make_async_copy(src, dst, wsem.at[i]) for i, (src, dst) in enumerate(((wg_hbm, wg), (wu_hbm, wu), (wd_hbm, wd)))]

    def meet():
        barrier = pltpu.get_barrier_semaphore()
        peers = [{"sp": chip * 2 + 1 - core}] + [{"tp": lax.rem(t + d, 4)} for d in (1, 2, 3)]
        peers += [{"sp": chip_at(dz, dx) * 2 + core} for dz, dx in others] + [{"sp": to} for to in column]
        for peer in peers:
            pl.semaphore_signal(barrier, inc=1, device_id=peer, device_id_type=MESH)
        pl.semaphore_wait(barrier, len(peers))

    for load in loads:
        load.start()
    prepare(q_raw, k_raw, v_turned, table_ref, qgain_ref, kgain_ref, q_wide, k_wide, q_ref, kv_ref)
    fill_info(routes_ref, lists_ref, info_ref, core)
    attention_part(q_ref, kv_ref, wo_hbm, residual_ref, mix_ref, pre_ref, middle, normed, meet, *attention_items)
    experts_part(normed, info_ref, middle, gain_ref, loads, out_ref, others, column, *expert_items)


def layer(queries, keys, values, tables, q_gain, k_gain, routes, lists, w_out, residual, gain_mix, gain_pre, gain_moe, w_gate, w_up, w_down):
    whole, apart = pl.BlockSpec(memory_space=pltpu.VMEM), pl.BlockSpec(memory_space=pltpu.MemorySpace.HBM)
    dma, bf16, f32 = pltpu.SemaphoreType.DMA, jnp.bfloat16, jnp.float32
    attention_scratch = [
        pltpu.VMEM((64, 2, PIECE, 128), bf16),
        pltpu.VMEM((1024, 128), bf16),
        pltpu.VMEM((1, 1024), f32),
        pltpu.VMEM((1, 1024), f32),
        pltpu.VMEM((128, 1024), f32),
        pltpu.VMEM((3, 128, 512), bf16),
        pltpu.VMEM((128, 1024), bf16),
        pltpu.VMEM((1024, 2048), bf16),
        pltpu.VMEM((4, 32, 2048), bf16),
        pltpu.VMEM((3, 32, 2048), bf16),
    ] + [dma((n,)) if n else dma for n in (64, 0, 3, 16, 16, 4, 4, 8, 8, 8, 2, 2, 3, 3, 0)]
    expert_scratch = [
        pltpu.VMEM((8, 2, 32, 2048), bf16),
        pltpu.VMEM((8, 2, 8, 128), f32),
        pltpu.VMEM((8, 4, 8, 2048), bf16),
        pltpu.VMEM((4, 32, 8, 2048), bf16),
        pltpu.VMEM((256, 512), bf16),
        pltpu.VMEM((4, 32, 8, 2048), bf16),
        pltpu.VMEM((2, 4, 4, 8, 2048), bf16),
        pltpu.VMEM((2, 32, 8, 2048), bf16),
        pltpu.VMEM((32, 8, 2048), bf16),
        pltpu.VMEM((3, 32, 2048), f32),
        pltpu.VMEM((2048, 512), bf16),
        pltpu.VMEM((2048, 512), bf16),
        pltpu.VMEM((512, 2048), bf16),
    ] + [dma((n,)) for n in (15, 16, 15, 16, 24, 32, 8, 8, 8, 32, 8, 8, 8, 8, 16, 32, 32, 2)]
    return pl.pallas_call(
        layer_kernel,
        out_shape=jax.ShapeDtypeStruct((32, 2048), bf16),
        in_specs=[whole] * 8 + [apart] + [whole] * 4 + [apart] * 3,
        out_specs=whole,
        scratch_shapes=[
            pltpu.VMEM((32, 2048), f32),
            pltpu.VMEM((32, 2048), bf16),
            dma((3,)),
            pltpu.VMEM((1024, 128), f32),
            pltpu.VMEM((256, 128), f32),
            pltpu.VMEM((2, 512, 128), bf16),
            pltpu.VMEM((2, 2, 128, 128), bf16),
            pltpu.VMEM((8, 128), f32),
        ]
        + attention_scratch
        + expert_scratch,
        compiler_params=pltpu.CompilerParams(collective_id=0, has_side_effects=True, vmem_limit_bytes=54 << 20),
        name="layer",
    )(queries, keys, values, tables, q_gain, k_gain, routes, lists, w_out, residual, gain_mix, gain_pre, gain_moe, w_gate, w_up, w_down)


def on_device(
    queries,
    keys,
    values,
    q_gain,
    k_gain,
    w_out,
    residual,
    gain_mix,
    gain_pre,
    routes,
    route_weights,
    w_gate,
    w_up,
    w_down,
    gain_moe,
):
    tok_rows, head_local, head_size = queries.shape
    kv_local = keys.shape[1]
    positions = lax.axis_index("sp") * tok_rows + jnp.arange(tok_rows, dtype=jnp.int32)
    cosine_table, sine_table = rope_tables(positions, head_size)
    cosines = jnp.stack([cosine_table, cosine_table], axis=2).reshape(tok_rows, head_size)
    sines = jnp.stack([-sine_table, sine_table], axis=2).reshape(tok_rows, head_size)
    width = residual.shape[1]
    lists = jnp.concatenate([routes.T.astype(jnp.float32), route_weights.T], axis=0)
    return layer(
        queries.reshape(tok_rows * head_local, head_size),
        keys.reshape(tok_rows * kv_local, head_size),
        values.transpose(1, 2, 0),
        jnp.stack([cosines, sines]),
        q_gain.reshape(1, head_size),
        k_gain.reshape(1, head_size),
        routes,
        jnp.pad(lists, ((0, 0), (0, 128 - lists.shape[1]))),
        w_out,
        residual,
        gain_mix.reshape(1, width),
        gain_pre.reshape(1, width),
        gain_moe.reshape(1, width),
        w_gate[0],
        w_up[0],
        w_down[0],
    )


def solution(mesh):
    placed = (
        P("sp", "tp", None),
        P("sp", "tp", None),
        P("sp", "tp", None),
        P(),
        P(),
        P("tp", None),
        P(("sp", "tp"), None),
        P(),
        P(),
        P(("sp", "tp"), None),
        P(("sp", "tp"), None),
        P("sp", None, "tp"),
        P("sp", None, "tp"),
        P("sp", "tp", None),
        P(),
    )
    return jax.shard_map(
        on_device, mesh=mesh, in_specs=placed, out_specs=P(("sp", "tp"), None), check_vma=False
    )
```
